512 devices in a mesh: sp: 128 (over z, y, core), tp: 4 (over x).
Axes of the slice: x: 4, y: 8, z: 8, core: 2. Of those that a mesh axis runs over, the one named last changes fastest.
Arguments:
- tokens: bfloat16 [65536, 2048], P(('sp', 'tp')), may hold values from -6 to 6
- pooling_input_weight: bfloat16 [2048, 1024], P('sp', 'tp'), may hold values from -0.125 to 0.125
- query_matrix: bfloat16 [2048, 512], P('sp', 'tp'), may hold values from -0.125 to 0.125
- key_matrix: bfloat16 [2048, 512], P('sp', 'tp'), may hold values from -0.125 to 0.125
- value_matrix: bfloat16 [2048, 1024], P('sp', 'tp'), may hold values from -0.125 to 0.125
- decay_inner_weight: bfloat16 [2048, 64], replicated, may hold values from -0.125 to 0.125
- decay_outer_weight: bfloat16 [2, 32, 512], replicated, may hold values from -1 to 1
- channel_decay_bias: float32 [2, 512], replicated, may hold values from -0.3 to 12
- spike_log_decay: float32 [8, 65536], P('tp', 'sp'), may hold values from -0.72 to 0
- starting_state: float32 [2, 8, 64, 128], P(None, 'tp'), may hold values from -1536 to 1536
- pooling_group_map: bfloat16 [4, 256, 256], replicated, may hold values from -0.375 to 0.375
- pooling_output_weight: bfloat16 [1024, 2048], P('tp', 'sp'), may hold values from -0.125 to 0.125
- attention_output_weight: bfloat16 [1024, 2048], P('tp', 'sp'), may hold values from -0.125 to 0.125
Outputs:
- mixed: bfloat16 [65536, 2048], P(('sp', 'tp'))
The draws below stay inside these ranges and needn't reach their ends.
All inputs are finite; a program needn't handle non-finite values.
Results may differ from the reference program's by a relative error of at most 0.015.
Values may be sent and summed in bfloat16 or wider, within the bound.
No kernel may reach another device: no remote copies, remote signals or barrier semaphores. Data moves between devices by JAX's collectives and lax.ppermute only.
A program may use at most 64 MiB of HBM per device.

```python
import math
import jax
import jax.numpy as jnp
from jax import lax

D = 2048
WINDOWS = 4
POOL_CH = 256
HEAD_COUNT = 8
KEY_CHANNELS = 64
DV = 128
RANK = 32
BLOCK = 64
TOKEN_COUNT = 65536
D_POOL = 1024
QK = 512
VW = 1024
N_SP = 128
N_TP = 4


def draw_tokens(key, part):
    noise_key, direction_key = jax.random.split(jax.random.fold_in(key, 37))
    noise = jax.random.normal(noise_key, (TOKEN_COUNT, D), jnp.float32)
    direction = jax.random.normal(direction_key, (D,), jnp.float32)
    ramp = -1.0 + 2.0 * jnp.arange(TOKEN_COUNT, dtype=jnp.float32) / jnp.float32(TOKEN_COUNT - 1)
    values = noise + 1.5 * ramp[:, None] * direction[None, :]
    return jnp.clip(values, -6.0, 6.0).astype(jnp.bfloat16)


def draw_channel_decay_bias(key, part):
    pick_key, jitter_key = jax.random.split(jax.random.fold_in(key, 11))
    chance = 0.5
    slower = jax.random.bernoulli(pick_key, chance, (2, HEAD_COUNT))
    slow_level = jnp.maximum(jnp.log(jnp.float32(TOKEN_COUNT) / 3.2), 3.0)
    jitter = jax.random.uniform(jitter_key, (2, HEAD_COUNT, KEY_CHANNELS), jnp.float32, -1.0, 1.0)
    levels = jnp.where(slower[:, :, None], slow_level, 0.7) + jitter
    return levels.reshape(2, HEAD_COUNT * KEY_CHANNELS).astype(jnp.float32)


def draw_spike_log_decay(key, part):
    factor_key, location_seed, depth_key = jax.random.split(jax.random.fold_in(key, 23), 3)
    low_factor = 0.5
    high_factor = 4.0
    block_count = TOKEN_COUNT // BLOCK
    factors = jnp.exp(jax.random.uniform(factor_key, (HEAD_COUNT, block_count), jnp.float32, math.log(low_factor), math.log(high_factor)))
    steady = -(0.2 / TOKEN_COUNT) * jnp.repeat(factors, BLOCK, axis=1)
    spike_locations = jax.random.randint(location_seed, (HEAD_COUNT, 2), 0, TOKEN_COUNT)
    spike_depth = jnp.log(jax.random.uniform(depth_key, (HEAD_COUNT, 2), jnp.float32, 0.5, 0.8))
    token_positions = jnp.arange(TOKEN_COUNT, dtype=jnp.int32)
    spike_events = token_positions[None, :, None] == spike_locations[:, None, :]
    abrupt_change = jnp.min(jnp.where(spike_events, spike_depth[:, None, :], 0.0), axis=2)
    return (steady + abrupt_change).astype(jnp.float32)


def level_of(key, dims, shards, smallest, largest):
    loudness, own = 1.0, jax.random.fold_in(key, 6)
    for dim, blocks in shards:
        draws = jnp.exp(jax.random.uniform(jax.random.fold_in(own, dim), (blocks,), jnp.float32, smallest / len(shards), largest / len(shards)))
        loudness = loudness * jnp.repeat(draws, dims[dim] // blocks).reshape([-1 if axis == dim else 1 for axis in range(len(dims))])
    return loudness


def scatter_about(rng, extent, scale, most, pieces=(), kind=jnp.bfloat16):
    result = scale * jax.random.normal(rng, extent, jnp.float32)
    if pieces:
        result = result * level_of(rng, extent, pieces, -0.22, 0.18)
    return jnp.clip(result, -most, most).astype(kind)


def setup_inputs(seed: int = 0) -> dict:
    keys = jax.random.split(jax.random.key(seed), 14)
    return {
        "tokens": draw_tokens(jax.random.fold_in(keys[13], 71), 0),
        "pooling_input_weight": scatter_about(keys[1], (D, D_POOL), D ** -0.5, 0.125, ((0, 128), (1, 4))),
        "query_matrix": scatter_about(keys[2], (D, QK), D ** -0.5, 0.125, ((0, 128), (1, 4))),
        "key_matrix": scatter_about(keys[3], (D, QK), D ** -0.5, 0.125, ((0, 128), (1, 4))),
        "value_matrix": scatter_about(keys[4], (D, VW), D ** -0.5, 0.125, ((0, 128), (1, 4))),
        "decay_inner_weight": scatter_about(keys[5], (D, 2 * RANK), D ** -0.5, 0.125),
        "decay_outer_weight": scatter_about(keys[6], (2, RANK, QK), RANK ** -0.5, 1.0),
        "channel_decay_bias": draw_channel_decay_bias(jax.random.fold_in(keys[13], 71), 0),
        "spike_log_decay": draw_spike_log_decay(jax.random.fold_in(keys[13], 71), 0),
        "starting_state": scatter_about(keys[9], (2, HEAD_COUNT, KEY_CHANNELS, DV), (2 * N_SP), 1536.0, ((1, 4),), jnp.float32),
        "pooling_group_map": scatter_about(keys[10], (WINDOWS, POOL_CH, POOL_CH), POOL_CH ** -0.5, 0.375),
        "pooling_output_weight": scatter_about(keys[11], (D_POOL, D), (D_POOL + VW) ** -0.5, 0.125, ((0, 4), (1, 128))),
        "attention_output_weight": scatter_about(keys[12], (VW, D), (D_POOL + VW) ** -0.5, 0.125, ((0, 4), (1, 128))),
    }


eps_value = 1e-06
gate_norm_factor = 16.0
highest = lax.Precision.HIGHEST
rim_width = 8

def normalize(token_rows):
    floats = token_rows.astype(jnp.float32)
    scaled = floats * lax.rsqrt(lax.optimization_barrier(jnp.mean(floats * floats, axis=-1, keepdims=True)) + eps_value)
    return scaled.astype(jnp.bfloat16)

def project(normed, weight):
    return jnp.dot(normed, weight, preferred_element_type=jnp.float32).astype(jnp.bfloat16)

def pooling(pool_input, pooling_group_map):
    sequence_length = pool_input.shape[0]
    floats = pool_input.astype(jnp.float32)
    padded = jnp.pad(floats, ((rim_width, rim_width), (0, 0)))
    position = jnp.arange(sequence_length, dtype=jnp.int32)
    outputs = []
    for group_id in range(WINDOWS):
        window = 2 ** (group_id + 1)
        half_width = window // 2
        columns = padded[:, group_id * POOL_CH:(group_id + 1) * POOL_CH]
        window_sum = jnp.zeros((sequence_length, POOL_CH), jnp.float32)
        for offset in range(-half_width, window - half_width):
            window_sum = window_sum + columns[rim_width + offset:rim_width + offset + sequence_length]
        low_end = jnp.clip(position - half_width, 0, sequence_length - 1)
        high_end = jnp.clip(position - half_width + window - 1, 0, sequence_length - 1)
        counted = (high_end - low_end + 1).astype(jnp.float32)[:, None]
        own_values = floats[:, group_id * POOL_CH:(group_id + 1) * POOL_CH]
        pooled = (window_sum / counted - own_values).astype(jnp.bfloat16)
        outputs.append(jnp.dot(pooled, pooling_group_map[group_id], preferred_element_type=jnp.float32).astype(jnp.bfloat16))
    return jnp.concatenate(outputs, axis=1)

def within_blocks(queries, cumulative, key_rows, value_rows, lower):
    row_ids = lax.broadcasted_iota(jnp.int32, (BLOCK, BLOCK), 0)
    col_ids = lax.broadcasted_iota(jnp.int32, (BLOCK, BLOCK), 1)
    allowed = col_ids <= row_ids if lower else col_ids > row_ids
    scaled_q = queries * jnp.exp(cumulative)
    scaled_k = key_rows * jnp.exp(-cumulative)
    scores = jnp.einsum('hnid,hnjd->hnij', scaled_q, scaled_k, precision=highest)
    scores = jnp.where(allowed, scores, 0.0)
    return (scaled_q, jnp.einsum('hnij,hnjv->hniv', scores, value_rows, precision=highest))

def block_updates(key_rows, value_rows, cumulative, edge):
    weighted = key_rows * jnp.exp(edge[:, :, None, :] - cumulative)
    return jnp.einsum('hncd,hncv->hndv', weighted, value_rows, precision=highest)

def run_states(edge, updates, start_memory, backward):

    def advance(memory, element):
        decay_now, update_now = element
        return (jnp.exp(decay_now)[..., None] * memory + update_now, memory)
    _, before = lax.scan(advance, start_memory, (jnp.moveaxis(edge, 1, 0), jnp.moveaxis(updates, 1, 0)), reverse=backward)
    return before

def reference(tokens, pooling_input_weight, query_matrix, key_matrix, value_matrix, decay_inner_weight, decay_outer_weight, channel_decay_bias, spike_log_decay, starting_state, pooling_group_map, pooling_output_weight, attention_output_weight):
    normed = normalize(tokens)
    sequence_length = tokens.shape[0]
    blocks = sequence_length // BLOCK
    pool_output = pooling(project(normed, pooling_input_weight), pooling_group_map)

    def split_heads(token_level, width):
        return token_level.astype(jnp.float32).reshape(blocks, BLOCK, HEAD_COUNT, width).transpose(2, 0, 1, 3)
    queries = split_heads(project(normed, query_matrix), KEY_CHANNELS) * KEY_CHANNELS ** (-0.5)
    key_rows = split_heads(project(normed, key_matrix), KEY_CHANNELS)
    value_rows = split_heads(project(normed, value_matrix), DV)
    low_rank = project(normed, decay_inner_weight)
    spike_amounts = spike_log_decay.T[:, :, None]

    def log_decay(direction):
        preactivation = jnp.dot(low_rank[:, direction * RANK:(direction + 1) * RANK], decay_outer_weight[direction], preferred_element_type=jnp.float32) + channel_decay_bias[direction]
        token_level = (jax.nn.log_sigmoid(preactivation) / gate_norm_factor).reshape(sequence_length, HEAD_COUNT, KEY_CHANNELS) + spike_amounts
        return token_level.reshape(blocks, BLOCK, HEAD_COUNT, KEY_CHANNELS).transpose(2, 0, 1, 3)
    cum_fwd = jnp.cumsum(log_decay(0), axis=2)
    cum_bwd = jnp.flip(jnp.cumsum(jnp.flip(log_decay(1), 2), axis=2), 2)
    scaled_fwd, inner_fwd = within_blocks(queries, cum_fwd, key_rows, value_rows, True)
    scaled_bwd, inner_bwd = within_blocks(queries, cum_bwd, key_rows, value_rows, False)
    edge_fwd = cum_fwd[:, :, -1, :]
    edge_bwd = cum_bwd[:, :, 0, :]
    before_fwd = run_states(edge_fwd, block_updates(key_rows, value_rows, cum_fwd, edge_fwd), starting_state[0], False)
    before_bwd = run_states(edge_bwd, block_updates(key_rows, value_rows, cum_bwd, edge_bwd), starting_state[1], True)
    out_fwd = inner_fwd + jnp.einsum('hnid,nhdv->hniv', scaled_fwd, before_fwd, precision=highest)
    out_bwd = inner_bwd + jnp.einsum('hnid,nhdv->hniv', scaled_bwd, before_bwd, precision=highest)
    joined = out_fwd + out_bwd
    normal_scale = lax.rsqrt(lax.optimization_barrier(jnp.mean(joined * joined, axis=-1, keepdims=True)) + eps_value)
    attention_output = (joined * normal_scale).astype(jnp.bfloat16).transpose(1, 2, 0, 3).reshape(sequence_length, HEAD_COUNT * DV)
    pool_rows = D_POOL // N_TP
    attention_rows = VW // N_TP
    mixed = jnp.zeros((sequence_length, D), jnp.float32)
    for group_id in range(N_TP):
        part_one = jnp.dot(pool_output[:, group_id * pool_rows:(group_id + 1) * pool_rows], pooling_output_weight[group_id * pool_rows:(group_id + 1) * pool_rows], preferred_element_type=jnp.float32)
        part_two = jnp.dot(attention_output[:, group_id * attention_rows:(group_id + 1) * attention_rows], attention_output_weight[group_id * attention_rows:(group_id + 1) * attention_rows], preferred_element_type=jnp.float32)
        rounded = lax.optimization_barrier((part_one + part_two).astype(jnp.bfloat16))
        mixed = mixed + rounded.astype(jnp.float32)
    return mixed.astype(jnp.bfloat16)
```

```python
import jax
import jax.numpy as jnp
from jax import lax
from jax.experimental import pallas as pl
from jax.experimental.pallas import tpu as pltpu
from jax.sharding import Mesh
from jax.sharding import PartitionSpec as P

KEY_CHANNELS = 64
DV = 128
RANK = 32
BLOCK = 64
SP = ("sp_0", "sp_1", "sp_2")
SP_TP = ("sp_0", "sp_1", "sp_2", "tp")


eps_value = 1e-06
gate_norm_factor = 16.0
rim_width = 8
LANES = 128


def from_everyone(value, axis):
    copies = jnp.broadcast_to(value, (lax.axis_size(axis), *value.shape))
    return lax.all_to_all(copies, axis, split_axis=0, concat_axis=0, tiled=True)


def laid_out(tiles, dim):
    tiles = jnp.moveaxis(tiles, 0, dim)
    lengths = tiles.shape
    return tiles.reshape(*lengths[:dim], lengths[dim] * lengths[dim + 1], *lengths[dim + 2 :])


def gathered_copies(value, axis, dim):
    tiles = from_everyone(value, axis)
    return laid_out(tiles, dim)


def extended(value, sides, width):
    for axis, dim in sides:
        devices, length = (lax.axis_size(axis), value.shape[dim])
        up = [(i, (i + 1) % devices) for i in range(devices - 1)]
        down = [(j, i) for i, j in up]
        last = lax.slice_in_dim(value, length - width, length, axis=dim)
        leading = lax.slice_in_dim(value, 0, width, axis=dim)
        before = lax.ppermute(last, axis, up)
        after = lax.ppermute(leading, axis, down)
        value = jnp.concatenate([before, value, after], axis=dim)
    return value


def scan_kernel(place_ref, received_ref, start_ref, out_ref):
    place = place_ref[0]
    devices = received_ref.shape[0]
    packed = received_ref[:, 2, :].astype(jnp.float32)
    logs = packed + pltpu.roll(packed, LANES - 2, 1)
    row = lax.broadcasted_iota(jnp.int32, (devices, devices), 0)
    col = lax.broadcasted_iota(jnp.int32, (devices, devices), 1)
    earlier = (col < row).astype(jnp.float32)
    later = (row < col).astype(jnp.float32)
    exact = lax.Precision.HIGHEST
    before_col = jnp.dot(earlier, logs, precision=exact, preferred_element_type=jnp.float32)
    dims = (((0,), (0,)), ((), ()))
    before_row = lax.dot_general(
        logs, later, dims, precision=exact, preferred_element_type=jnp.float32
    )
    own_row = lax.dot_general(
        logs,
        (row == col).astype(jnp.float32),
        dims,
        precision=exact,
        preferred_element_type=jnp.float32,
    )
    total = jnp.sum(logs, axis=0, keepdims=True)
    forward = place < devices // 2
    for r in range(2):
        at_col = before_col[:, r : r + 1]
        past_col = at_col + logs[:, r : r + 1]
        at_row = before_row[r : r + 1, :]
        past_row = at_row + own_row[r : r + 1, :]
        between = jnp.where(forward, at_col - past_row, at_row - past_col)
        allowed = jnp.where(forward, row - col, col - row) > 0
        weights = jnp.where(allowed, jnp.exp(jnp.minimum(between, 0.0)), 0.0)
        outside = jnp.where(forward, at_col, total[:, r : r + 1] - past_col)
        updates = received_ref[:, r, :].astype(jnp.float32)
        first = start_ref[pl.ds(2 * place + r, 1), :]
        entering = jnp.dot(
            weights, updates, precision=exact, preferred_element_type=jnp.float32
        ) + jnp.exp(jnp.minimum(outside, 0.0)) * first
        out_ref[:, r, :] = entering.astype(out_ref.dtype)


def entering_states(total_fwd, total_bwd, starting_state, place):
    logs = jnp.stack([total_fwd[0], total_bwd[0]])
    updates = jnp.stack([total_fwd[1], total_bwd[1]])
    devices = logs.size // 2
    high = logs.astype(jnp.bfloat16)
    low = (logs - high.astype(jnp.float32)).astype(jnp.bfloat16)
    edge = jnp.concatenate([high.reshape(devices, 2), low.reshape(devices, 2)], axis=1)
    edge = jnp.pad(edge, ((0, 0), (0, LANES - 4)))
    packed = jnp.concatenate(
        [updates.astype(jnp.bfloat16).reshape(devices, 2, DV), edge[:, None]], axis=1
    )
    received = lax.all_to_all(packed, SP, 0, 0, tiled=True)
    entering = pl.pallas_call(
        scan_kernel,
        in_specs=[
            pl.BlockSpec(memory_space=pltpu.SMEM),
            pl.BlockSpec(memory_space=pltpu.VMEM),
            pl.BlockSpec(memory_space=pltpu.VMEM),
        ],
        out_specs=pl.BlockSpec(memory_space=pltpu.VMEM),
        out_shape=jax.ShapeDtypeStruct((devices, 2, DV), jnp.bfloat16),
        name="scan_states",
    )(place.reshape(1).astype(jnp.int32), received, starting_state.reshape(2 * devices, DV))
    entering = lax.all_to_all(entering, SP, 0, 0, tiled=True)
    return entering.reshape(starting_state.shape).astype(jnp.float32)


def spread(value, axes):
    for axis in axes:
        copies = jnp.broadcast_to(value, (lax.axis_size(axis), *value.shape))
        value = lax.all_to_all(copies, axis, split_axis=0, concat_axis=0, tiled=True)
    return value


def in_order(tiles):
    whole = tiles.transpose(1, 2, 0, 3, 4)
    return whole.reshape(-1, tiles.shape[-1])


def cut_along(value, dim, devices):
    lengths = value.shape
    tiles = value.reshape(*lengths[:dim], devices, lengths[dim] // devices, *lengths[dim + 1 :])
    return jnp.moveaxis(tiles, dim, 0)


def sum_at_owner(value, axis, dim):
    devices = lax.axis_size(axis)
    tiles = lax.all_to_all(cut_along(value, dim, devices), axis, 0, 0, tiled=True)
    return jnp.sum(tiles.astype(jnp.float32), axis=0)


def normalize(token_rows):
    floats = token_rows.astype(jnp.float32)
    scaled = floats * lax.rsqrt(jnp.mean(floats * floats, axis=-1, keepdims=True) + eps_value)
    return scaled.astype(jnp.bfloat16)


def local_chain(decays, updates, backward):

    def advance(carried, element):
        log_total, memory = carried
        decay_now, update_now = element
        return (
            (log_total + decay_now, jnp.exp(decay_now)[..., None] * memory + update_now),
            (log_total, memory),
        )

    begin = (jnp.zeros_like(decays[0]), jnp.zeros_like(updates[0]))
    return lax.scan(advance, begin, (decays, updates), reverse=backward)


def within_blocks(queries, cumulative, key_rows, value_rows, lower):
    row_ids = lax.broadcasted_iota(jnp.int32, (BLOCK, BLOCK), 0)
    col_ids = lax.broadcasted_iota(jnp.int32, (BLOCK, BLOCK), 1)
    allowed = col_ids <= row_ids if lower else col_ids > row_ids
    scaled_q = queries * jnp.exp(cumulative)
    scaled_k = key_rows * jnp.exp(-cumulative)
    scores = jnp.einsum("hnid,hnjd->hnij", scaled_q, scaled_k)
    scores = jnp.where(allowed, scores, 0.0)
    return (scaled_q, jnp.einsum("hnij,hnjv->hniv", scores, value_rows))


def block_updates(key_rows, value_rows, cumulative, edge):
    weighted = key_rows * jnp.exp(edge[:, :, None, :] - cumulative)
    return jnp.einsum("hncd,hncv->hndv", weighted, value_rows)


def carried_term(scaled_q, before, entering):
    log_before, memory_before = before
    block_memory = jnp.exp(log_before)[..., None] * entering[None] + memory_before
    return jnp.einsum("hnid,nhdv->hniv", scaled_q, block_memory)


def shards(
    tokens,
    pooling_input_weight,
    query_matrix,
    key_matrix,
    value_matrix,
    decay_inner_weight,
    decay_outer_weight,
    channel_decay_bias,
    spike_log_decay,
    starting_state,
    pooling_group_map,
    pooling_output_weight,
    attention_output_weight,
):
    sp_index = lax.axis_index(SP)
    tp_index = lax.axis_index("tp")
    normed = normalize(tokens)
    pool_cols = pooling_input_weight.shape[1]
    qk_cols = query_matrix.shape[1]
    value_cols = value_matrix.shape[1]
    local_weight = jnp.concatenate(
        [pooling_input_weight, query_matrix, key_matrix, value_matrix], axis=1
    )
    local_out = jnp.concatenate([pooling_output_weight, attention_output_weight], axis=0).T
    some = spread(jnp.concatenate([local_weight, local_out], axis=1), ("sp_1",))
    in_cols = local_weight.shape[1]
    whole_in = in_order(spread(some[..., :in_cols], ("sp_0", "sp_2")))
    whole_out = in_order(spread(some[..., in_cols:], ("sp_0", "sp_2")))
    all_rows = gathered_copies(normed, "tp", 0)
    summed = jnp.dot(
        all_rows,
        whole_in,
        preferred_element_type=jnp.float32,
    )
    rank_part = jnp.dot(all_rows, decay_inner_weight, preferred_element_type=jnp.float32).astype(
        jnp.bfloat16
    )
    projected = jnp.concatenate([summed.astype(jnp.bfloat16), rank_part], axis=1)
    sequence_length = projected.shape[0]
    blocks = sequence_length // BLOCK
    heads_here = qk_cols // KEY_CHANNELS
    pool_input = projected[:, :pool_cols]
    query_part = projected[:, pool_cols : pool_cols + qk_cols]
    key_part = projected[:, pool_cols + qk_cols : pool_cols + 2 * qk_cols]
    value_part = projected[:, pool_cols + 2 * qk_cols : pool_cols + 2 * qk_cols + value_cols]
    low_rank = projected[:, pool_cols + 2 * qk_cols + value_cols :]
    window = jnp.left_shift(jnp.int32(2), tp_index)
    half_width = window // 2
    padded = extended(pool_input, ((SP, 0),), rim_width)
    floats = padded.astype(jnp.float32)
    window_sum = jnp.zeros((sequence_length, pool_cols), jnp.float32)
    for offset in range(-rim_width, rim_width):
        inside = ((offset >= -half_width) & (offset < window - half_width)).astype(jnp.float32)
        window_sum = (
            window_sum + inside * floats[rim_width + offset : rim_width + offset + sequence_length]
        )
    seq_length = sequence_length * lax.axis_size(SP)
    position = sp_index * sequence_length + jnp.arange(sequence_length, dtype=jnp.int32)
    low_end = jnp.clip(position - half_width, 0, seq_length - 1)
    high_end = jnp.clip(position - half_width + window - 1, 0, seq_length - 1)
    counted = (high_end - low_end + 1).astype(jnp.float32)[:, None]
    pooled = (window_sum / counted - floats[rim_width : rim_width + sequence_length]).astype(
        jnp.bfloat16
    )
    mix_here = lax.dynamic_index_in_dim(pooling_group_map, tp_index, 0, keepdims=False)
    pool_output = jnp.dot(pooled, mix_here, preferred_element_type=jnp.float32).astype(jnp.bfloat16)

    def split_heads(token_level, width):
        return (
            token_level.astype(jnp.float32)
            .reshape(blocks, BLOCK, heads_here, width)
            .transpose(2, 0, 1, 3)
        )

    queries = split_heads(query_part, KEY_CHANNELS) * KEY_CHANNELS ** (-0.5)
    key_rows = split_heads(key_part, KEY_CHANNELS)
    value_rows = split_heads(value_part, DV)
    up_here = lax.dynamic_slice_in_dim(decay_outer_weight, tp_index * qk_cols, qk_cols, 2)
    bias_here = lax.dynamic_slice_in_dim(channel_decay_bias, tp_index * qk_cols, qk_cols, 1)
    spike_amounts = spike_log_decay.T[:, :, None]

    def log_decay(direction):
        preactivation = (
            jnp.dot(
                low_rank[:, direction * RANK : (direction + 1) * RANK],
                up_here[direction],
                preferred_element_type=jnp.float32,
            )
            + bias_here[direction]
        )
        token_level = (jax.nn.log_sigmoid(preactivation) / gate_norm_factor).reshape(
            sequence_length, heads_here, KEY_CHANNELS
        ) + spike_amounts
        return token_level.reshape(blocks, BLOCK, heads_here, KEY_CHANNELS).transpose(2, 0, 1, 3)

    cum_fwd = jnp.cumsum(log_decay(0), axis=2)
    cum_bwd = jnp.flip(jnp.cumsum(jnp.flip(log_decay(1), 2), axis=2), 2)
    scaled_fwd, inner_fwd = within_blocks(queries, cum_fwd, key_rows, value_rows, True)
    scaled_bwd, inner_bwd = within_blocks(queries, cum_bwd, key_rows, value_rows, False)
    edge_fwd = cum_fwd[:, :, -1, :]
    edge_bwd = cum_bwd[:, :, 0, :]
    updates_fwd = block_updates(key_rows, value_rows, cum_fwd, edge_fwd)
    updates_bwd = block_updates(key_rows, value_rows, cum_bwd, edge_bwd)
    total_fwd, before_fwd = local_chain(
        jnp.moveaxis(edge_fwd, 1, 0), jnp.moveaxis(updates_fwd, 1, 0), False
    )
    total_bwd, before_bwd = local_chain(
        jnp.moveaxis(edge_bwd, 1, 0), jnp.moveaxis(updates_bwd, 1, 0), True
    )
    entering = entering_states(total_fwd, total_bwd, starting_state, sp_index)
    entering_fwd, entering_bwd = entering[0], entering[1]
    out_fwd = inner_fwd + carried_term(scaled_fwd, before_fwd, entering_fwd)
    out_bwd = inner_bwd + carried_term(scaled_bwd, before_bwd, entering_bwd)
    joined = out_fwd + out_bwd
    normal_scale = lax.rsqrt(jnp.mean(joined * joined, axis=-1, keepdims=True) + eps_value)
    attention_output = (
        (joined * normal_scale)
        .astype(jnp.bfloat16)
        .transpose(1, 2, 0, 3)
        .reshape(sequence_length, heads_here * DV)
    )
    activations = jnp.concatenate([pool_output, attention_output], axis=1)
    partial = lax.dot_general(
        activations, whole_out, (((1,), (1,)), ((), ())), preferred_element_type=jnp.float32
    )
    mixed = sum_at_owner(partial.astype(jnp.bfloat16), "tp", 0)
    return mixed.astype(jnp.bfloat16)


def solution(mesh):
    split = Mesh(mesh.devices.reshape(8, 8, 2, mesh.shape["tp"]), ("sp_0", "sp_1", "sp_2", "tp"))
    in_specs = (
        P(SP_TP, None),
        P(SP, "tp"),
        P(SP, "tp"),
        P(SP, "tp"),
        P(SP, "tp"),
        P(),
        P(),
        P(),
        P("tp", SP),
        P(None, "tp", None, None),
        P(),
        P("tp", SP),
        P("tp", SP),
    )
    out_specs = P(SP_TP, None)
    return jax.shard_map(
        shards, mesh=split, in_specs=in_specs, out_specs=out_specs, check_vma=False
    )
```

```python
import jax
import jax.numpy as jnp
from jax import lax
from jax.experimental import pallas as pl
from jax.experimental.pallas import tpu as pltpu
from jax.sharding import Mesh
from jax.sharding import PartitionSpec as P


KEY_CHANNELS = 64
DV = 128
RANK = 32
BLOCK = 64
LANES = 128
SP = ("sp_0", "sp_1", "sp_2")
CHIPS = ("sp_0", "sp_1")
SP_TP = ("sp_0", "sp_1", "sp_2", "tp")

eps_value = 1e-06
gate_norm_factor = 16.0
rim_width = 8
interpreted = False

bf16 = jnp.bfloat16
f32 = jnp.float32
exact = lax.Precision.HIGHEST


def matmul(a, b, dims=((1,), (0,)), precision=None):
    return lax.dot_general(a, b, (dims, ((), ())), precision=precision, preferred_element_type=f32)


def call(kernel, out_shapes, operands, scalars=1, scratch=(), flops=0, moved=0):
    smem = pl.BlockSpec(memory_space=pltpu.SMEM)
    vmem = pl.BlockSpec(memory_space=pltpu.VMEM)
    return pl.pallas_call(
        kernel,
        in_specs=[smem if i < scalars else vmem for i in range(len(operands))],
        out_specs=jax.tree.map(lambda _: vmem, out_shapes),
        out_shape=out_shapes,
        scratch_shapes=list(scratch),
        cost_estimate=pl.CostEstimate(flops=flops, bytes_accessed=moved, transcendentals=0),
        interpret=interpreted,
    )(*operands)


def shifted(value, axis, step):
    devices = lax.axis_size(axis)
    return lax.ppermute(value, axis, [(i, (i + step) % devices) for i in range(devices)])


def neighbours(value, axes, step):
    devices = lax.axis_size(axes)
    pairs = [(i, i + step) for i in range(devices) if 0 <= i + step < devices]
    return lax.ppermute(value, axes, pairs)


def normalize(token_rows):
    floats = token_rows.astype(f32)
    scaled = floats * lax.rsqrt(jnp.mean(floats * floats, axis=-1, keepdims=True) + eps_value)
    return scaled.astype(bf16)


def place_tokens(tp, pieces, whole_ref, first):
    own, before, after, far_top, far_end = pieces
    rows = own.shape[0]
    half = rows // 2

    def at(step):
        return pl.multiple_of(first + lax.rem(tp + step, 4) * rows, 8)

    whole_ref[pl.ds(at(0), rows), :] = own[...]
    whole_ref[pl.ds(at(3), rows), :] = before[...]
    whole_ref[pl.ds(at(1), rows), :] = after[...]
    far = at(2)
    whole_ref[pl.ds(far, half), :] = far_top[...]
    whole_ref[pl.ds(pl.multiple_of(far + half, 8), half), :] = far_end[...]


def split_dot(ones, values):
    high = values.astype(bf16)
    low = (values - high.astype(f32)).astype(bf16)
    return matmul(ones, high) + matmul(ones, low)


def project_kernel(
    place,
    own,
    before,
    after,
    far_top,
    far_end,
    weight_own,
    weight_other,
    inner,
    outer,
    bias,
    spike,
    qkv_out,
    pool_out,
    logs_out,
    packed_out,
    tokens_ref,
    weight_ref,
):
    tp, core = (place[0], place[1])
    place_tokens(tp, (own, before, after, far_top, far_end), tokens_ref, 0)
    weight_ref[:, pl.ds(core, 1)] = weight_own[...][:, None]
    weight_ref[:, pl.ds(1 - core, 1)] = weight_other[...][:, None]
    rows, width = tokens_ref.shape
    tokens = tokens_ref[...]
    low_rank = matmul(tokens, inner[...]).astype(bf16)
    projected = matmul(tokens, weight_ref[...].reshape(width, -1)).astype(bf16)
    qkv = projected[:, : 4 * LANES]
    qkv_out[...] = qkv
    pool_out[...] = projected[:, 4 * LANES :]
    here = pl.ds(pl.multiple_of(tp * LANES, LANES), LANES)
    blank = jnp.zeros((RANK, LANES), bf16)
    outer_both = jnp.concatenate(
        [
            jnp.concatenate([outer[0, :, here], blank], axis=1),
            jnp.concatenate([blank, outer[1, :, here]], axis=1),
        ],
        axis=0,
    )
    bias_both = jnp.concatenate([bias[0:1, here], bias[1:2, here]], axis=1)
    pre = matmul(low_rank, outer_both) + bias_both
    gate = jnp.minimum(pre, 0.0) - jnp.log1p(jnp.exp(-jnp.abs(pre)))
    lane = lax.broadcasted_iota(jnp.int32, (rows, LANES), 1)
    spikes = jnp.where(lane < KEY_CHANNELS, spike[:, 0:1], spike[:, 1:2])
    decay = gate * (1.0 / gate_norm_factor) + jnp.concatenate([spikes, spikes], axis=1)
    size = LANES
    row_ids = lax.broadcasted_iota(jnp.int32, (size, size), 0)
    col_ids = lax.broadcasted_iota(jnp.int32, (size, size), 1)
    upto = (col_ids <= row_ids).astype(bf16)
    onward = (col_ids >= row_ids).astype(bf16)
    tiles = rows // size
    carry = jnp.zeros((1, LANES), f32)
    for n in range(tiles):
        found = split_dot(upto, decay[n * size : (n + 1) * size, :LANES]) + carry
        logs_out[0, n * size : (n + 1) * size, :] = found
        carry = found[size - 1 : size, :]
    total_fwd = carry
    carry = jnp.zeros((1, LANES), f32)
    for n in reversed(range(tiles)):
        found = split_dot(onward, decay[n * size : (n + 1) * size, LANES:]) + carry
        logs_out[1, n * size : (n + 1) * size, :] = found
        carry = found[0:1, :]
    total_bwd = carry
    keys = qkv[:, LANES : 2 * LANES].astype(f32)
    weighted = jnp.concatenate(
        [
            (keys * jnp.exp(total_fwd - logs_out[0])).astype(bf16),
            (keys * jnp.exp(total_bwd - logs_out[1])).astype(bf16),
        ],
        axis=1,
    )
    updates = matmul(weighted, qkv[:, 2 * LANES :], ((0,), (0,)))
    first = lax.broadcasted_iota(jnp.int32, (LANES, LANES), 0) < KEY_CHANNELS
    for d in range(2):
        mine = updates[d * LANES : (d + 1) * LANES]
        packed_out[:, 0, d * LANES : (d + 1) * LANES] = jnp.where(
            first, mine[:, :LANES], mine[:, LANES:]
        )
    totals = jnp.concatenate([total_fwd, total_bwd], axis=0)
    stacked = jnp.concatenate([totals, jnp.zeros((LANES - 2, LANES), f32)], axis=0)
    packed_out[:, 0, 2 * LANES :] = stacked.T


def scan_kernel(place, received, start, out):
    devices = received.shape[0]
    here = place[0]
    logs = received[:, 0, 2 * LANES :]
    row = lax.broadcasted_iota(jnp.int32, (devices, devices), 0)
    col = lax.broadcasted_iota(jnp.int32, (devices, devices), 1)
    earlier = (col < row).astype(f32)
    upto = (row <= col).astype(f32)
    strictly = (row < col).astype(f32)
    before_col = matmul(earlier, logs, precision=exact)
    before_row = matmul(logs, strictly, ((0,), (0,)), precision=exact)
    past_row = matmul(logs, upto, ((0,), (0,)), precision=exact)
    past_col = before_col + logs
    total = jnp.sum(logs, axis=0, keepdims=True)
    for r in range(2):
        if r == 0:
            between = before_col[:, 0:1] - past_row[0:1, :]
            allowed = col < row
            outside = before_col[:, 0:1]
        else:
            between = before_row[1:2, :] - past_col[:, 1:2]
            allowed = col > row
            outside = total[:, 1:2] - past_col[:, 1:2]
        weights = jnp.where(allowed, jnp.exp(jnp.minimum(between, 0.0)), 0.0)
        high = weights.astype(bf16)
        low = (weights - high.astype(f32)).astype(bf16)
        updates = received[:, 0, r * LANES : (r + 1) * LANES].astype(bf16)
        first = start[r, pl.ds(here, 1), :]
        entering = matmul(high, updates) + matmul(low, updates)
        entering = entering + jnp.exp(jnp.minimum(outside, 0.0)) * first
        out[:, 0, r * LANES : (r + 1) * LANES] = entering


def inner_kernel(qkv, logs, part_out, query_out):
    rows = qkv.shape[0]
    blocks = rows // BLOCK
    lane = lax.broadcasted_iota(jnp.int32, (BLOCK, LANES), 1)
    row = lax.broadcasted_iota(jnp.int32, (BLOCK, LANES), 0)
    head_one = lane < KEY_CHANNELS
    lower = lax.rem(lane, KEY_CHANNELS) <= row
    value_lane = lax.broadcasted_iota(jnp.int32, (BLOCK, 2 * DV), 1)
    value_one = value_lane < DV
    diagonal = (
        lax.rem(lax.broadcasted_iota(jnp.int32, (4 * KEY_CHANNELS, 2 * DV), 0), LANES)
        < KEY_CHANNELS
    ) == (lax.broadcasted_iota(jnp.int32, (4 * KEY_CHANNELS, 2 * DV), 1) < DV)
    zero = jnp.zeros((), bf16)
    scale = KEY_CHANNELS ** (-0.5)
    edges, updates, scaled, scored = [], [], [], []
    nothing = jnp.zeros((1, LANES), f32)
    for n in range(blocks):
        at = slice(n * BLOCK, (n + 1) * BLOCK)
        base_fwd = logs[0, n * BLOCK - 1 : n * BLOCK, :] if n else nothing
        base_bwd = logs[1, (n + 1) * BLOCK : (n + 1) * BLOCK + 1, :] if n + 1 < blocks else nothing
        cum_fwd = logs[0, at, :] - base_fwd
        cum_bwd = logs[1, at, :] - base_bwd
        edge_fwd = cum_fwd[BLOCK - 1 : BLOCK, :]
        edge_bwd = cum_bwd[0:1, :]
        queries = qkv[at, :LANES].astype(f32) * scale
        keys = qkv[at, LANES : 2 * LANES].astype(f32)
        values = qkv[at, 2 * LANES :]
        query_out[at, :LANES] = (queries * jnp.exp(logs[0, at, :])).astype(bf16)
        query_out[at, LANES:] = (queries * jnp.exp(logs[1, at, :])).astype(bf16)
        query_fwd = (queries * jnp.exp(cum_fwd)).astype(bf16)
        query_bwd = (queries * jnp.exp(cum_bwd)).astype(bf16)
        key_fwd = (keys * jnp.exp(-cum_fwd)).astype(bf16)
        key_bwd = (keys * jnp.exp(-cum_bwd)).astype(bf16)

        def by_head(key):
            return jnp.concatenate(
                [jnp.where(head_one, key, zero), jnp.where(head_one, zero, key)], axis=0
            )

        across = ((1,), (1,))
        scores = jnp.where(
            lower,
            matmul(query_fwd, by_head(key_fwd), across),
            matmul(query_bwd, by_head(key_bwd), across),
        ).astype(bf16)
        spread = jnp.concatenate(
            [jnp.where(value_one, values, zero), jnp.where(value_one, zero, values)], axis=0
        )
        scored.append(matmul(scores, spread))
        scaled.append(jnp.concatenate([query_fwd, query_bwd], axis=1))
        weighted = jnp.concatenate(
            [
                (keys * jnp.exp(edge_fwd - cum_fwd)).astype(bf16),
                (keys * jnp.exp(edge_bwd - cum_bwd)).astype(bf16),
            ],
            axis=1,
        )
        update = matmul(weighted, values, ((0,), (0,)))
        updates.append(jnp.where(diagonal, update, 0.0))
        edges.append((edge_fwd, edge_bwd))
    stacked = jnp.concatenate(
        [e[0] for e in edges]
        + [e[1] for e in edges]
        + [jnp.zeros((LANES - 2 * blocks, LANES), f32)],
        axis=0,
    )
    factors = jnp.exp(stacked.T)
    start_fwd, start_bwd = [None] * blocks, [None] * blocks
    memory = jnp.zeros((LANES, 2 * DV), f32)
    for n in range(blocks):
        start_fwd[n] = memory.astype(bf16)
        memory = factors[:, n : n + 1] * memory + updates[n][:LANES]
    memory = jnp.zeros((LANES, 2 * DV), f32)
    for n in reversed(range(blocks)):
        start_bwd[n] = memory.astype(bf16)
        memory = factors[:, blocks + n : blocks + n + 1] * memory + updates[n][LANES:]
    for n in range(blocks):
        entering = jnp.concatenate([start_fwd[n], start_bwd[n]], axis=0)
        part_out[n * BLOCK : (n + 1) * BLOCK, :] = scored[n] + matmul(scaled[n], entering)


def pool_kernel(place, pool_input, rim_before, rim_after, group_map, out):
    tp, here = (place[0], place[2])
    rows = out.shape[0]
    padded = rows + 2 * rim_width
    values = jnp.concatenate([rim_before[...], pool_input[...], rim_after[...]], axis=0).astype(f32)
    sums = values + pltpu.roll(values, 1, 0)
    chosen = sums
    for level in (1, 2, 3):
        step = 2 ** (level - 1)
        sums = pltpu.roll(sums, step, 0) + pltpu.roll(sums, padded - step, 0)
        chosen = jnp.where(tp >= level, sums, chosen)
    half = jnp.left_shift(1, tp)
    position = here * rows + lax.broadcasted_iota(jnp.int32, (rows, LANES), 0)
    last = place[3] * rows - 1
    low_end = jnp.maximum(position - half, 0)
    high_end = jnp.minimum(position + half - 1, last)
    counted = (high_end - low_end + 1).astype(f32)[:, 0:1]
    inside = slice(rim_width, rim_width + rows)
    pooled = (chosen[inside] / counted - values[inside]).astype(bf16)
    out[...] = matmul(pooled, group_map[tp]).astype(bf16)


def finish_kernel(part, query, entering, pooled, out):
    channel_one = lax.broadcasted_iota(jnp.int32, (LANES, DV), 0) < KEY_CHANNELS
    zero = jnp.zeros((), bf16)
    sides = []
    for d in range(2):
        state = entering[:, 0, d * LANES : (d + 1) * LANES].astype(bf16)
        sides.append(
            jnp.concatenate(
                [jnp.where(channel_one, state, zero), jnp.where(channel_one, zero, state)], axis=1
            )
        )
    joined = part[...] + matmul(query[...], jnp.concatenate(sides, axis=0))
    rows = joined.shape[0]
    ready = [pooled[...]]
    for h in range(2):
        mine = joined[:, h * DV : (h + 1) * DV]
        scale = lax.rsqrt(jnp.mean(mine * mine, axis=1, keepdims=True) + eps_value)
        ready.append((mine * scale).astype(bf16))
    owners = out.shape[0]
    for j in range(owners):
        at = slice(j * rows // owners, (j + 1) * rows // owners)
        start = 0
        for piece in ready:
            out[j, :, start : start + piece.shape[1]] = piece[at]
            start += piece.shape[1]


def output_kernel(place, activations, weight, out):
    tp = place[0]
    groups, _, width = activations.shape
    total = None
    for s in range(groups):
        source = lax.rem(tp + groups - s, groups)
        partial = matmul(
            activations[source], weight[:, s * width : (s + 1) * width], ((1,), (1,))
        )
        partial = partial.astype(bf16).astype(f32)
        total = partial if total is None else total + partial
    out[...] = total.astype(bf16)


def output_projection(place, activations, weights):
    groups, rows, width = activations.shape
    model = weights.shape[0]
    tile = 256
    return pl.pallas_call(
        output_kernel,
        grid=(model // tile,),
        in_specs=[
            pl.BlockSpec(memory_space=pltpu.SMEM),
            pl.BlockSpec((groups, rows, width), lambda n: (0, 0, 0)),
            pl.BlockSpec((tile, groups * width), lambda n: (n, 0)),
        ],
        out_specs=pl.BlockSpec((rows, tile), lambda n: (0, n)),
        out_shape=jax.ShapeDtypeStruct((rows, model), bf16),
        interpret=interpreted,
        name="output_kernel",
    )(place, activations, weights)


def shape_of(*lengths, kind=bf16):
    return jax.ShapeDtypeStruct(lengths, kind)


def shards(
    tokens,
    pooling_input_weight,
    query_matrix,
    key_matrix,
    value_matrix,
    decay_inner_weight,
    decay_outer_weight,
    channel_decay_bias,
    spike_log_decay,
    starting_state,
    pooling_group_map,
    pooling_output_weight,
    attention_output_weight,
):
    sp_index = lax.axis_index(SP)
    tp_index = lax.axis_index("tp")
    core = lax.axis_index("sp_2")
    positions = lax.axis_size(SP)
    place = jnp.stack([tp_index, core, sp_index, jnp.int32(positions)]).astype(jnp.int32)
    groups = lax.axis_size("tp")
    rows = tokens.shape[0] * groups
    model = tokens.shape[1]

    local_in = jnp.concatenate(
        [query_matrix, key_matrix, value_matrix, pooling_input_weight], axis=1
    )
    chips = lax.axis_size(CHIPS)
    copies = jnp.broadcast_to(local_in, (chips, *local_in.shape))
    weight_own = lax.all_to_all(copies, CHIPS, 0, 0, tiled=True)
    local_out = jnp.concatenate([pooling_output_weight, attention_output_weight], axis=0).T
    outs = [local_out] + [shifted(local_out, "tp", k) for k in range(1, groups)]
    normed = normalize(tokens)
    half = normed.shape[0] // 2
    before = shifted(normed, "tp", 1)
    after = shifted(normed, "tp", -1)
    top, end = (before[:half], after[half:])
    far_top = shifted(top, "tp", 1)
    far_end = shifted(end, "tp", -1)
    weight_other = shifted(weight_own, "sp_2", 1)
    whole_out = lax.all_gather(jnp.concatenate(outs, axis=1), SP, axis=0, tiled=True)

    qkv, pool_input, logs, packed = call(
        project_kernel,
        (
            shape_of(rows, 4 * LANES),
            shape_of(rows, 2 * LANES),
            shape_of(2, rows, LANES, kind=f32),
            shape_of(LANES, 1, 3 * LANES, kind=f32),
        ),
        (
            place,
            normed,
            before,
            after,
            far_top,
            far_end,
            weight_own,
            weight_other,
            decay_inner_weight,
            decay_outer_weight,
            channel_decay_bias,
            spike_log_decay.T,
        ),
        scratch=(
            pltpu.VMEM((rows, model), bf16),
            pltpu.VMEM((chips, 2, model // (2 * chips), 6 * LANES), bf16),
        ),
        flops=2 * rows * model * 7 * LANES,
        moved=10_000_000,
    )
    received = lax.all_to_all(packed, SP, 0, 0, tiled=True)
    rim_before = neighbours(pool_input[rows - rim_width :], SP, 1)
    rim_after = neighbours(pool_input[:rim_width], SP, -1)
    part, query = call(
        inner_kernel,
        (shape_of(rows, 2 * DV, kind=f32), shape_of(rows, 2 * LANES)),
        (qkv, logs),
        scalars=0,
        flops=2 * rows * model * 2 * LANES,
        moved=3_000_000,
    )
    states = call(
        scan_kernel,
        shape_of(positions, 1, 2 * LANES, kind=f32),
        (place[2:3], received, starting_state.reshape(2, -1, DV)),
        flops=40_000_000,
    )
    entering = lax.all_to_all(states, SP, 0, 0, tiled=True)
    pooled = call(
        pool_kernel,
        shape_of(rows, 2 * LANES),
        (place, pool_input, rim_before, rim_after, pooling_group_map),
        flops=2 * rows * 4 * LANES * LANES,
        moved=1_000_000,
    )
    activations = call(
        finish_kernel,
        shape_of(groups, rows // groups, 4 * LANES),
        (part, query, entering, pooled),
        scalars=0,
        flops=100_000_000,
        moved=2_000_000,
    )
    gathered = lax.all_to_all(activations, "tp", 0, 0, tiled=True)
    return output_projection(place, gathered, whole_out)


def solution(mesh):
    split = Mesh(mesh.devices.reshape(8, 8, 2, mesh.shape["tp"]), ("sp_0", "sp_1", "sp_2", "tp"))
    in_specs = (
        P(SP_TP, None),
        P(SP, "tp"),
        P(SP, "tp"),
        P(SP, "tp"),
        P(SP, "tp"),
        P(),
        P(),
        P(),
        P("tp", SP),
        P(None, "tp", None, None),
        P(),
        P("tp", SP),
        P("tp", SP),
    )
    out_specs = P(SP_TP, None)
    return jax.shard_map(
        shards, mesh=split, in_specs=in_specs, out_specs=out_specs, check_vma=False
    )
```

```python
import jax
import jax.numpy as jnp
from jax import lax
from jax.experimental import pallas as pl
from jax.experimental.pallas import tpu as pltpu
from jax.sharding import Mesh
from jax.sharding import PartitionSpec as P


KEY_CHANNELS = 64
DV = 128
RANK = 32
BLOCK = 64
LANES = 128
SP = ("sp_0", "sp_1", "sp_2")
CHIPS = ("sp_0", "sp_1")
SP_TP = ("sp_0", "sp_1", "sp_2", "tp")

eps_value = 1e-06
gate_norm_factor = 16.0
rim_width = 8
interpreted = False

bf16 = jnp.bfloat16
f32 = jnp.float32
exact = lax.Precision.HIGHEST


def matmul(a, b, dims=((1,), (0,)), precision=None):
    return lax.dot_general(a, b, (dims, ((), ())), precision=precision, preferred_element_type=f32)


def call(kernel, out_shapes, operands, scalars=1, far=0, scratch=(), flops=0, moved=0):
    smem = pl.BlockSpec(memory_space=pltpu.SMEM)
    vmem = pl.BlockSpec(memory_space=pltpu.VMEM)
    anywhere = pl.BlockSpec(memory_space=pl.ANY)
    near = len(operands) - scalars - far
    return pl.pallas_call(
        kernel,
        in_specs=[smem] * scalars + [anywhere] * far + [vmem] * near,
        out_specs=jax.tree.map(lambda _: vmem, out_shapes),
        out_shape=out_shapes,
        scratch_shapes=list(scratch),
        cost_estimate=pl.CostEstimate(flops=flops, bytes_accessed=moved, transcendentals=0),
        interpret=interpreted,
    )(*operands)


def shifted(value, axis, step):
    devices = lax.axis_size(axis)
    return lax.ppermute(value, axis, [(i, (i + step) % devices) for i in range(devices)])


def neighbours(value, axes, step):
    devices = lax.axis_size(axes)
    pairs = [(i, i + step) for i in range(devices) if 0 <= i + step < devices]
    return lax.ppermute(value, axes, pairs)


def normalize(token_rows):
    floats = token_rows.astype(f32)
    scaled = floats * lax.rsqrt(jnp.mean(floats * floats, axis=-1, keepdims=True) + eps_value)
    return scaled.astype(bf16)


def split_dot(ones, values):
    high = values.astype(bf16)
    low = (values - high.astype(f32)).astype(bf16)
    return matmul(ones, high) + matmul(ones, low)


def project_kernel(
    place,
    tokens_in,
    weight_own,
    weight_other,
    inner,
    outer,
    bias,
    spike,
    qkv_out,
    pool_out,
    logs_out,
    packed_out,
    tokens_ref,
    weight_ref,
    sems,
):
    tp, core = (place[0], place[1])
    rows, width = tokens_ref.shape
    load_tokens = pltpu.make_async_copy(tokens_in, tokens_ref, sems.at[0])
    load_own = pltpu.make_async_copy(weight_own, weight_ref.at[:, core], sems.at[1])
    load_other = pltpu.make_async_copy(weight_other, weight_ref.at[:, 1 - core], sems.at[2])
    load_tokens.start()
    load_own.start()
    load_other.start()
    load_tokens.wait()
    tokens = tokens_ref[...]
    low_rank = matmul(tokens, inner[...]).astype(bf16)
    here = pl.ds(pl.multiple_of(tp * LANES, LANES), LANES)
    blank = jnp.zeros((RANK, LANES), bf16)
    outer_both = jnp.concatenate(
        [
            jnp.concatenate([outer[0, :, here], blank], axis=1),
            jnp.concatenate([blank, outer[1, :, here]], axis=1),
        ],
        axis=0,
    )
    bias_both = jnp.concatenate([bias[0:1, here], bias[1:2, here]], axis=1)
    pre = matmul(low_rank, outer_both) + bias_both
    gate = jnp.minimum(pre, 0.0) - jnp.log1p(jnp.exp(-jnp.abs(pre)))
    lane = lax.broadcasted_iota(jnp.int32, (rows, LANES), 1)
    spikes = jnp.where(lane < KEY_CHANNELS, spike[:, 0:1], spike[:, 1:2])
    decay = gate * (1.0 / gate_norm_factor) + jnp.concatenate([spikes, spikes], axis=1)
    size = LANES
    row_ids = lax.broadcasted_iota(jnp.int32, (size, size), 0)
    col_ids = lax.broadcasted_iota(jnp.int32, (size, size), 1)
    upto = (col_ids <= row_ids).astype(bf16)
    onward = (col_ids >= row_ids).astype(bf16)
    tiles = rows // size
    carry = jnp.zeros((1, LANES), f32)
    for n in range(tiles):
        found = split_dot(upto, decay[n * size : (n + 1) * size, :LANES]) + carry
        logs_out[0, n * size : (n + 1) * size, :] = found
        carry = found[size - 1 : size, :]
    total_fwd = carry
    carry = jnp.zeros((1, LANES), f32)
    for n in reversed(range(tiles)):
        found = split_dot(onward, decay[n * size : (n + 1) * size, LANES:]) + carry
        logs_out[1, n * size : (n + 1) * size, :] = found
        carry = found[0:1, :]
    total_bwd = carry
    load_own.wait()
    load_other.wait()
    projected = matmul(tokens_ref[...], weight_ref[...].reshape(width, -1)).astype(bf16)
    qkv = projected[:, : 4 * LANES]
    qkv_out[...] = qkv
    pool_out[...] = projected[:, 4 * LANES :]
    keys = qkv[:, LANES : 2 * LANES].astype(f32)
    weighted = jnp.concatenate(
        [
            (keys * jnp.exp(total_fwd - logs_out[0])).astype(bf16),
            (keys * jnp.exp(total_bwd - logs_out[1])).astype(bf16),
        ],
        axis=1,
    )
    updates = matmul(weighted, qkv[:, 2 * LANES :], ((0,), (0,)))
    first = lax.broadcasted_iota(jnp.int32, (LANES, LANES), 0) < KEY_CHANNELS
    for d in range(2):
        mine = updates[d * LANES : (d + 1) * LANES]
        packed_out[:, 0, d * LANES : (d + 1) * LANES] = jnp.where(
            first, mine[:, :LANES], mine[:, LANES:]
        )
    totals = jnp.concatenate([total_fwd, total_bwd], axis=0)
    stacked = jnp.concatenate([totals, jnp.zeros((LANES - 2, LANES), f32)], axis=0)
    packed_out[:, 0, 2 * LANES :] = stacked.T


def scan_kernel(place, received, start, out):
    devices = received.shape[0]
    here = place[0]
    logs = received[:, 0, 2 * LANES :]
    row = lax.broadcasted_iota(jnp.int32, (devices, devices), 0)
    col = lax.broadcasted_iota(jnp.int32, (devices, devices), 1)
    earlier = (col < row).astype(f32)
    upto = (row <= col).astype(f32)
    strictly = (row < col).astype(f32)
    before_col = matmul(earlier, logs, precision=exact)
    before_row = matmul(logs, strictly, ((0,), (0,)), precision=exact)
    past_row = matmul(logs, upto, ((0,), (0,)), precision=exact)
    past_col = before_col + logs
    total = jnp.sum(logs, axis=0, keepdims=True)
    for r in range(2):
        if r == 0:
            between = before_col[:, 0:1] - past_row[0:1, :]
            allowed = col < row
            outside = before_col[:, 0:1]
        else:
            between = before_row[1:2, :] - past_col[:, 1:2]
            allowed = col > row
            outside = total[:, 1:2] - past_col[:, 1:2]
        weights = jnp.where(allowed, jnp.exp(jnp.minimum(between, 0.0)), 0.0)
        high = weights.astype(bf16)
        low = (weights - high.astype(f32)).astype(bf16)
        updates = received[:, 0, r * LANES : (r + 1) * LANES].astype(bf16)
        first = start[r, pl.ds(here, 1), :]
        entering = matmul(high, updates) + matmul(low, updates)
        entering = entering + jnp.exp(jnp.minimum(outside, 0.0)) * first
        out[:, 0, r * LANES : (r + 1) * LANES] = entering


def inner_kernel(qkv, logs, part_out, query_out):
    rows = qkv.shape[0]
    blocks = rows // BLOCK
    lane = lax.broadcasted_iota(jnp.int32, (BLOCK, LANES), 1)
    row = lax.broadcasted_iota(jnp.int32, (BLOCK, LANES), 0)
    head_one = lane < KEY_CHANNELS
    lower = lax.rem(lane, KEY_CHANNELS) <= row
    value_lane = lax.broadcasted_iota(jnp.int32, (BLOCK, 2 * DV), 1)
    value_one = value_lane < DV
    diagonal = (
        lax.rem(lax.broadcasted_iota(jnp.int32, (4 * KEY_CHANNELS, 2 * DV), 0), LANES)
        < KEY_CHANNELS
    ) == (lax.broadcasted_iota(jnp.int32, (4 * KEY_CHANNELS, 2 * DV), 1) < DV)
    zero = jnp.zeros((), bf16)
    scale = KEY_CHANNELS ** (-0.5)
    edges, updates, scaled, scored = [], [], [], []
    nothing = jnp.zeros((1, LANES), f32)
    for n in range(blocks):
        at = slice(n * BLOCK, (n + 1) * BLOCK)
        base_fwd = logs[0, n * BLOCK - 1 : n * BLOCK, :] if n else nothing
        base_bwd = logs[1, (n + 1) * BLOCK : (n + 1) * BLOCK + 1, :] if n + 1 < blocks else nothing
        cum_fwd = logs[0, at, :] - base_fwd
        cum_bwd = logs[1, at, :] - base_bwd
        edge_fwd = cum_fwd[BLOCK - 1 : BLOCK, :]
        edge_bwd = cum_bwd[0:1, :]
        queries = qkv[at, :LANES].astype(f32) * scale
        keys = qkv[at, LANES : 2 * LANES].astype(f32)
        values = qkv[at, 2 * LANES :]
        query_out[at, :LANES] = (queries * jnp.exp(logs[0, at, :])).astype(bf16)
        query_out[at, LANES:] = (queries * jnp.exp(logs[1, at, :])).astype(bf16)
        query_fwd = (queries * jnp.exp(cum_fwd)).astype(bf16)
        query_bwd = (queries * jnp.exp(cum_bwd)).astype(bf16)
        key_fwd = (keys * jnp.exp(-cum_fwd)).astype(bf16)
        key_bwd = (keys * jnp.exp(-cum_bwd)).astype(bf16)

        def by_head(key):
            return jnp.concatenate(
                [jnp.where(head_one, key, zero), jnp.where(head_one, zero, key)], axis=0
            )

        across = ((1,), (1,))
        scores = jnp.where(
            lower,
            matmul(query_fwd, by_head(key_fwd), across),
            matmul(query_bwd, by_head(key_bwd), across),
        ).astype(bf16)
        spread = jnp.concatenate(
            [jnp.where(value_one, values, zero), jnp.where(value_one, zero, values)], axis=0
        )
        scored.append(matmul(scores, spread))
        scaled.append(jnp.concatenate([query_fwd, query_bwd], axis=1))
        weighted = jnp.concatenate(
            [
                (keys * jnp.exp(edge_fwd - cum_fwd)).astype(bf16),
                (keys * jnp.exp(edge_bwd - cum_bwd)).astype(bf16),
            ],
            axis=1,
        )
        update = matmul(weighted, values, ((0,), (0,)))
        updates.append(jnp.where(diagonal, update, 0.0))
        edges.append((edge_fwd, edge_bwd))
    stacked = jnp.concatenate(
        [e[0] for e in edges]
        + [e[1] for e in edges]
        + [jnp.zeros((LANES - 2 * blocks, LANES), f32)],
        axis=0,
    )
    factors = jnp.exp(stacked.T)
    start_fwd, start_bwd = [None] * blocks, [None] * blocks
    memory = jnp.zeros((LANES, 2 * DV), f32)
    for n in range(blocks):
        start_fwd[n] = memory.astype(bf16)
        memory = factors[:, n : n + 1] * memory + updates[n][:LANES]
    memory = jnp.zeros((LANES, 2 * DV), f32)
    for n in reversed(range(blocks)):
        start_bwd[n] = memory.astype(bf16)
        memory = factors[:, blocks + n : blocks + n + 1] * memory + updates[n][LANES:]
    for n in range(blocks):
        entering = jnp.concatenate([start_fwd[n], start_bwd[n]], axis=0)
        part_out[n * BLOCK : (n + 1) * BLOCK, :] = scored[n] + matmul(scaled[n], entering)


def pool_kernel(place, pool_input, rim_before, rim_after, group_map, out):
    tp, here = (place[0], place[2])
    rows = out.shape[0]
    padded = rows + 2 * rim_width
    values = jnp.concatenate([rim_before[...], pool_input[...], rim_after[...]], axis=0).astype(f32)
    sums = values + pltpu.roll(values, 1, 0)
    chosen = sums
    for level in (1, 2, 3):
        step = 2 ** (level - 1)
        sums = pltpu.roll(sums, step, 0) + pltpu.roll(sums, padded - step, 0)
        chosen = jnp.where(tp >= level, sums, chosen)
    half = jnp.left_shift(1, tp)
    position = here * rows + lax.broadcasted_iota(jnp.int32, (rows, LANES), 0)
    last = place[3] * rows - 1
    low_end = jnp.maximum(position - half, 0)
    high_end = jnp.minimum(position + half - 1, last)
    counted = (high_end - low_end + 1).astype(f32)[:, 0:1]
    inside = slice(rim_width, rim_width + rows)
    pooled = (chosen[inside] / counted - values[inside]).astype(bf16)
    out[...] = matmul(pooled, group_map[tp]).astype(bf16)


def finish_kernel(part, query, entering, pooled, out):
    channel_one = lax.broadcasted_iota(jnp.int32, (LANES, DV), 0) < KEY_CHANNELS
    zero = jnp.zeros((), bf16)
    sides = []
    for d in range(2):
        state = entering[:, 0, d * LANES : (d + 1) * LANES].astype(bf16)
        sides.append(
            jnp.concatenate(
                [jnp.where(channel_one, state, zero), jnp.where(channel_one, zero, state)], axis=1
            )
        )
    joined = part[...] + matmul(query[...], jnp.concatenate(sides, axis=0))
    rows = joined.shape[0]
    ready = [pooled[...]]
    for h in range(2):
        mine = joined[:, h * DV : (h + 1) * DV]
        scale = lax.rsqrt(jnp.mean(mine * mine, axis=1, keepdims=True) + eps_value)
        ready.append((mine * scale).astype(bf16))
    owners = out.shape[0]
    for j in range(owners):
        at = slice(j * rows // owners, (j + 1) * rows // owners)
        start = 0
        for piece in ready:
            out[j, :, start : start + piece.shape[1]] = piece[at]
            start += piece.shape[1]


def output_kernel(place, activations, weight, out, turned):
    tp = place[0]
    groups, _, width = activations.shape

    @pl.when(pl.program_id(0) == 0)
    def _():
        for s in range(groups):
            source = lax.rem(tp + groups - s, groups)
            turned[s] = activations[source].astype(f32).T.astype(bf16)

    total = None
    for s in range(groups):
        partial = matmul(weight[:, s * width : (s + 1) * width], turned[s])
        partial = partial.astype(bf16).astype(f32)
        total = partial if total is None else total + partial
    out[...] = total.T.astype(bf16)


def output_projection(place, activations, weights):
    groups, rows, width = activations.shape
    model = weights.shape[0]
    tile = 256
    return pl.pallas_call(
        output_kernel,
        grid=(model // tile,),
        in_specs=[
            pl.BlockSpec(memory_space=pltpu.SMEM),
            pl.BlockSpec((groups, rows, width), lambda n: (0, 0, 0)),
            pl.BlockSpec((tile, groups * width), lambda n: (n, 0)),
        ],
        out_specs=pl.BlockSpec((rows, tile), lambda n: (0, n)),
        out_shape=jax.ShapeDtypeStruct((rows, model), bf16),
        scratch_shapes=[pltpu.VMEM((groups, width, rows), bf16)],
        interpret=interpreted,
        name="output_kernel",
    )(place, activations, weights)


def shape_of(*lengths, kind=bf16):
    return jax.ShapeDtypeStruct(lengths, kind)


def shards(
    tokens,
    pooling_input_weight,
    query_matrix,
    key_matrix,
    value_matrix,
    decay_inner_weight,
    decay_outer_weight,
    channel_decay_bias,
    spike_log_decay,
    starting_state,
    pooling_group_map,
    pooling_output_weight,
    attention_output_weight,
):
    sp_index = lax.axis_index(SP)
    tp_index = lax.axis_index("tp")
    core = lax.axis_index("sp_2")
    positions = lax.axis_size(SP)
    place = jnp.stack([tp_index, core, sp_index, jnp.int32(positions)]).astype(jnp.int32)
    groups = lax.axis_size("tp")
    rows = tokens.shape[0] * groups
    model = tokens.shape[1]

    local_in = jnp.concatenate(
        [query_matrix, key_matrix, value_matrix, pooling_input_weight], axis=1
    )
    chips = lax.axis_size(CHIPS)
    copies = jnp.broadcast_to(local_in, (chips, *local_in.shape))
    weight_own = lax.all_to_all(copies, CHIPS, 0, 0, tiled=True)
    local_out = jnp.concatenate([pooling_output_weight, attention_output_weight], axis=0).T
    outs = [local_out] + [shifted(local_out, "tp", k) for k in range(1, groups)]
    weight_other = shifted(weight_own, "sp_2", 1)
    all_tokens = lax.all_gather(normalize(tokens), "tp", axis=0, tiled=True)
    whole_out = lax.all_gather(jnp.concatenate(outs, axis=1), SP, axis=0, tiled=True)

    qkv, pool_input, logs, packed = call(
        project_kernel,
        (
            shape_of(rows, 4 * LANES),
            shape_of(rows, 2 * LANES),
            shape_of(2, rows, LANES, kind=f32),
            shape_of(LANES, 1, 3 * LANES, kind=f32),
        ),
        (
            place,
            all_tokens,
            weight_own,
            weight_other,
            decay_inner_weight,
            decay_outer_weight,
            channel_decay_bias,
            spike_log_decay.T,
        ),
        far=3,
        scratch=(
            pltpu.VMEM((rows, model), bf16),
            pltpu.VMEM((chips, 2, model // (2 * chips), 6 * LANES), bf16),
            pltpu.SemaphoreType.DMA((3,)),
        ),
        flops=2 * rows * model * 7 * LANES,
        moved=10_000_000,
    )
    received = lax.all_to_all(packed, SP, 0, 0, tiled=True)
    rim_before = neighbours(pool_input[rows - rim_width :], SP, 1)
    rim_after = neighbours(pool_input[:rim_width], SP, -1)
    part, query = call(
        inner_kernel,
        (shape_of(rows, 2 * DV, kind=f32), shape_of(rows, 2 * LANES)),
        (qkv, logs),
        scalars=0,
        flops=2 * rows * model * 2 * LANES,
        moved=3_000_000,
    )
    states = call(
        scan_kernel,
        shape_of(positions, 1, 2 * LANES, kind=f32),
        (place[2:3], received, starting_state.reshape(2, -1, DV)),
        flops=40_000_000,
    )
    entering = lax.all_to_all(states, SP, 0, 0, tiled=True)
    pooled = call(
        pool_kernel,
        shape_of(rows, 2 * LANES),
        (place, pool_input, rim_before, rim_after, pooling_group_map),
        flops=2 * rows * 4 * LANES * LANES,
        moved=1_000_000,
    )
    activations = call(
        finish_kernel,
        shape_of(groups, rows // groups, 4 * LANES),
        (part, query, entering, pooled),
        scalars=0,
        flops=100_000_000,
        moved=2_000_000,
    )
    gathered = lax.all_to_all(activations, "tp", 0, 0, tiled=True)
    return output_projection(place, gathered, whole_out)


def solution(mesh):
    split = Mesh(mesh.devices.reshape(8, 8, 2, mesh.shape["tp"]), ("sp_0", "sp_1", "sp_2", "tp"))
    in_specs = (
        P(SP_TP, None),
        P(SP, "tp"),
        P(SP, "tp"),
        P(SP, "tp"),
        P(SP, "tp"),
        P(),
        P(),
        P(),
        P("tp", SP),
        P(None, "tp", None, None),
        P(),
        P("tp", SP),
        P("tp", SP),
    )
    out_specs = P(SP_TP, None)
    return jax.shard_map(
        shards, mesh=split, in_specs=in_specs, out_specs=out_specs, check_vma=False
    )
```

```python
import jax
import jax.numpy as jnp
from jax import lax
from jax.experimental import pallas as pl
from jax.experimental.pallas import tpu as pltpu
from jax.sharding import Mesh
from jax.sharding import PartitionSpec as P


KEY_CHANNELS = 64
DV = 128
RANK = 32
BLOCK = 64
LANES = 128
SP = ("sp_0", "sp_1", "sp_2")
CHIPS = ("sp_0", "sp_1")
SP_TP = ("sp_0", "sp_1", "sp_2", "tp")

eps_value = 1e-06
gate_norm_factor = 16.0
rim_width = 8
interpreted = False

bf16 = jnp.bfloat16
f32 = jnp.float32
exact = lax.Precision.HIGHEST


def matmul(a, b, dims=((1,), (0,)), precision=None):
    return lax.dot_general(a, b, (dims, ((), ())), precision=precision, preferred_element_type=f32)


def call(kernel, out_shapes, operands, scalars=1, far=0, scratch=(), flops=0, moved=0):
    smem = pl.BlockSpec(memory_space=pltpu.SMEM)
    vmem = pl.BlockSpec(memory_space=pltpu.VMEM)
    anywhere = pl.BlockSpec(memory_space=pl.ANY)
    near = len(operands) - scalars - far
    return pl.pallas_call(
        kernel,
        in_specs=[smem] * scalars + [anywhere] * far + [vmem] * near,
        out_specs=jax.tree.map(lambda _: vmem, out_shapes),
        out_shape=out_shapes,
        scratch_shapes=list(scratch),
        cost_estimate=pl.CostEstimate(flops=flops, bytes_accessed=moved, transcendentals=0),
        interpret=interpreted,
    )(*operands)


def shifted(value, axis, step):
    devices = lax.axis_size(axis)
    return lax.ppermute(value, axis, [(i, (i + step) % devices) for i in range(devices)])


def neighbours(value, axes, step):
    devices = lax.axis_size(axes)
    pairs = [(i, i + step) for i in range(devices) if 0 <= i + step < devices]
    return lax.ppermute(value, axes, pairs)


def normalize(token_rows):
    floats = token_rows.astype(f32)
    scaled = floats * lax.rsqrt(jnp.mean(floats * floats, axis=-1, keepdims=True) + eps_value)
    return scaled.astype(bf16)


def place_tokens(tp, pieces, whole_ref, first):
    own, before, after, far_top, far_end = pieces
    rows = own.shape[0]
    half = rows // 2

    def at(step):
        return pl.multiple_of(first + lax.rem(tp + step, 4) * rows, 8)

    whole_ref[pl.ds(at(0), rows), :] = own[...]
    whole_ref[pl.ds(at(3), rows), :] = before[...]
    whole_ref[pl.ds(at(1), rows), :] = after[...]
    far = at(2)
    whole_ref[pl.ds(far, half), :] = far_top[...]
    whole_ref[pl.ds(pl.multiple_of(far + half, 8), half), :] = far_end[...]


def split_dot(ones, values):
    high = values.astype(bf16)
    low = (values - high.astype(f32)).astype(bf16)
    return matmul(ones, high) + matmul(ones, low)


def decay_kernel(
    place,
    own,
    before,
    after,
    far_top,
    far_end,
    inner,
    outer,
    bias,
    spike,
    tokens_out,
    logs_out,
):
    tp = place[0]
    place_tokens(tp, (own, before, after, far_top, far_end), tokens_out, 0)
    rows = tokens_out.shape[0]
    low_rank = matmul(tokens_out[...], inner[...]).astype(bf16)
    here = pl.ds(pl.multiple_of(tp * LANES, LANES), LANES)
    blank = jnp.zeros((RANK, LANES), bf16)
    outer_both = jnp.concatenate(
        [
            jnp.concatenate([outer[0, :, here], blank], axis=1),
            jnp.concatenate([blank, outer[1, :, here]], axis=1),
        ],
        axis=0,
    )
    bias_both = jnp.concatenate([bias[0:1, here], bias[1:2, here]], axis=1)
    pre = matmul(low_rank, outer_both) + bias_both
    gate = jnp.minimum(pre, 0.0) - jnp.log1p(jnp.exp(-jnp.abs(pre)))
    lane = lax.broadcasted_iota(jnp.int32, (rows, LANES), 1)
    spikes = jnp.where(lane < KEY_CHANNELS, spike[:, 0:1], spike[:, 1:2])
    decay = gate * (1.0 / gate_norm_factor) + jnp.concatenate([spikes, spikes], axis=1)
    size = LANES
    row_ids = lax.broadcasted_iota(jnp.int32, (size, size), 0)
    col_ids = lax.broadcasted_iota(jnp.int32, (size, size), 1)
    upto = (col_ids <= row_ids).astype(bf16)
    onward = (col_ids >= row_ids).astype(bf16)
    tiles = rows // size
    carry = jnp.zeros((1, LANES), f32)
    for n in range(tiles):
        found = split_dot(upto, decay[n * size : (n + 1) * size, :LANES]) + carry
        logs_out[0, n * size : (n + 1) * size, :] = found
        carry = found[size - 1 : size, :]
    carry = jnp.zeros((1, LANES), f32)
    for n in reversed(range(tiles)):
        found = split_dot(onward, decay[n * size : (n + 1) * size, LANES:]) + carry
        logs_out[1, n * size : (n + 1) * size, :] = found
        carry = found[0:1, :]


def project_kernel(
    place,
    weight_own,
    weight_other,
    tokens,
    logs,
    qkv_out,
    pool_out,
    packed_out,
    weight_ref,
    sems,
):
    core = place[1]
    load_own = pltpu.make_async_copy(weight_own, weight_ref.at[:, core], sems.at[0])
    load_other = pltpu.make_async_copy(weight_other, weight_ref.at[:, 1 - core], sems.at[1])
    load_own.start()
    load_other.start()
    rows, width = tokens.shape
    total_fwd = logs[0, rows - 1 : rows, :]
    total_bwd = logs[1, 0:1, :]
    load_own.wait()
    load_other.wait()
    projected = matmul(tokens[...], weight_ref[...].reshape(width, -1)).astype(bf16)
    qkv = projected[:, : 4 * LANES]
    qkv_out[...] = qkv
    pool_out[...] = projected[:, 4 * LANES :]
    keys = qkv[:, LANES : 2 * LANES].astype(f32)
    weighted = jnp.concatenate(
        [
            (keys * jnp.exp(total_fwd - logs[0])).astype(bf16),
            (keys * jnp.exp(total_bwd - logs[1])).astype(bf16),
        ],
        axis=1,
    )
    updates = matmul(weighted, qkv[:, 2 * LANES :], ((0,), (0,)))
    first = lax.broadcasted_iota(jnp.int32, (LANES, LANES), 0) < KEY_CHANNELS
    for d in range(2):
        mine = updates[d * LANES : (d + 1) * LANES]
        packed_out[:, 0, d * LANES : (d + 1) * LANES] = jnp.where(
            first, mine[:, :LANES], mine[:, LANES:]
        )
    totals = jnp.concatenate([total_fwd, total_bwd], axis=0)
    stacked = jnp.concatenate([totals, jnp.zeros((LANES - 2, LANES), f32)], axis=0)
    packed_out[:, 0, 2 * LANES :] = stacked.T


def scan_kernel(place, received, start, out):
    devices = received.shape[0]
    here = place[0]
    logs = received[:, 0, 2 * LANES :]
    row = lax.broadcasted_iota(jnp.int32, (devices, devices), 0)
    col = lax.broadcasted_iota(jnp.int32, (devices, devices), 1)
    earlier = (col < row).astype(f32)
    upto = (row <= col).astype(f32)
    strictly = (row < col).astype(f32)
    before_col = matmul(earlier, logs, precision=exact)
    before_row = matmul(logs, strictly, ((0,), (0,)), precision=exact)
    past_row = matmul(logs, upto, ((0,), (0,)), precision=exact)
    past_col = before_col + logs
    total = jnp.sum(logs, axis=0, keepdims=True)
    for r in range(2):
        if r == 0:
            between = before_col[:, 0:1] - past_row[0:1, :]
            allowed = col < row
            outside = before_col[:, 0:1]
        else:
            between = before_row[1:2, :] - past_col[:, 1:2]
            allowed = col > row
            outside = total[:, 1:2] - past_col[:, 1:2]
        weights = jnp.where(allowed, jnp.exp(jnp.minimum(between, 0.0)), 0.0)
        high = weights.astype(bf16)
        low = (weights - high.astype(f32)).astype(bf16)
        updates = received[:, 0, r * LANES : (r + 1) * LANES].astype(bf16)
        first = start[r, pl.ds(here, 1), :]
        entering = matmul(high, updates) + matmul(low, updates)
        entering = entering + jnp.exp(jnp.minimum(outside, 0.0)) * first
        out[:, 0, r * LANES : (r + 1) * LANES] = entering


def inner_kernel(qkv, logs, part_out, query_out):
    rows = qkv.shape[0]
    blocks = rows // BLOCK
    lane = lax.broadcasted_iota(jnp.int32, (BLOCK, LANES), 1)
    row = lax.broadcasted_iota(jnp.int32, (BLOCK, LANES), 0)
    head_one = lane < KEY_CHANNELS
    lower = lax.rem(lane, KEY_CHANNELS) <= row
    value_lane = lax.broadcasted_iota(jnp.int32, (BLOCK, 2 * DV), 1)
    value_one = value_lane < DV
    diagonal = (
        lax.rem(lax.broadcasted_iota(jnp.int32, (4 * KEY_CHANNELS, 2 * DV), 0), LANES)
        < KEY_CHANNELS
    ) == (lax.broadcasted_iota(jnp.int32, (4 * KEY_CHANNELS, 2 * DV), 1) < DV)
    zero = jnp.zeros((), bf16)
    scale = KEY_CHANNELS ** (-0.5)
    edges, updates, scaled, scored = [], [], [], []
    nothing = jnp.zeros((1, LANES), f32)
    for n in range(blocks):
        at = slice(n * BLOCK, (n + 1) * BLOCK)
        base_fwd = logs[0, n * BLOCK - 1 : n * BLOCK, :] if n else nothing
        base_bwd = logs[1, (n + 1) * BLOCK : (n + 1) * BLOCK + 1, :] if n + 1 < blocks else nothing
        cum_fwd = logs[0, at, :] - base_fwd
        cum_bwd = logs[1, at, :] - base_bwd
        edge_fwd = cum_fwd[BLOCK - 1 : BLOCK, :]
        edge_bwd = cum_bwd[0:1, :]
        queries = qkv[at, :LANES].astype(f32) * scale
        keys = qkv[at, LANES : 2 * LANES].astype(f32)
        values = qkv[at, 2 * LANES :]
        query_out[at, :LANES] = (queries * jnp.exp(logs[0, at, :])).astype(bf16)
        query_out[at, LANES:] = (queries * jnp.exp(logs[1, at, :])).astype(bf16)
        query_fwd = (queries * jnp.exp(cum_fwd)).astype(bf16)
        query_bwd = (queries * jnp.exp(cum_bwd)).astype(bf16)
        key_fwd = (keys * jnp.exp(-cum_fwd)).astype(bf16)
        key_bwd = (keys * jnp.exp(-cum_bwd)).astype(bf16)

        def by_head(key):
            return jnp.concatenate(
                [jnp.where(head_one, key, zero), jnp.where(head_one, zero, key)], axis=0
            )

        across = ((1,), (1,))
        scores = jnp.where(
            lower,
            matmul(query_fwd, by_head(key_fwd), across),
            matmul(query_bwd, by_head(key_bwd), across),
        ).astype(bf16)
        spread = jnp.concatenate(
            [jnp.where(value_one, values, zero), jnp.where(value_one, zero, values)], axis=0
        )
        scored.append(matmul(scores, spread))
        scaled.append(jnp.concatenate([query_fwd, query_bwd], axis=1))
        weighted = jnp.concatenate(
            [
                (keys * jnp.exp(edge_fwd - cum_fwd)).astype(bf16),
                (keys * jnp.exp(edge_bwd - cum_bwd)).astype(bf16),
            ],
            axis=1,
        )
        update = matmul(weighted, values, ((0,), (0,)))
        updates.append(jnp.where(diagonal, update, 0.0))
        edges.append((edge_fwd, edge_bwd))
    stacked = jnp.concatenate(
        [e[0] for e in edges]
        + [e[1] for e in edges]
        + [jnp.zeros((LANES - 2 * blocks, LANES), f32)],
        axis=0,
    )
    factors = jnp.exp(stacked.T)
    start_fwd, start_bwd = [None] * blocks, [None] * blocks
    memory = jnp.zeros((LANES, 2 * DV), f32)
    for n in range(blocks):
        start_fwd[n] = memory.astype(bf16)
        memory = factors[:, n : n + 1] * memory + updates[n][:LANES]
    memory = jnp.zeros((LANES, 2 * DV), f32)
    for n in reversed(range(blocks)):
        start_bwd[n] = memory.astype(bf16)
        memory = factors[:, blocks + n : blocks + n + 1] * memory + updates[n][LANES:]
    for n in range(blocks):
        entering = jnp.concatenate([start_fwd[n], start_bwd[n]], axis=0)
        part_out[n * BLOCK : (n + 1) * BLOCK, :] = scored[n] + matmul(scaled[n], entering)


def pool_kernel(place, pool_input, rim_before, rim_after, group_map, out):
    tp, here = (place[0], place[2])
    rows = out.shape[0]
    padded = rows + 2 * rim_width
    values = jnp.concatenate([rim_before[...], pool_input[...], rim_after[...]], axis=0).astype(f32)
    sums = values + pltpu.roll(values, 1, 0)
    chosen = sums
    for level in (1, 2, 3):
        step = 2 ** (level - 1)
        sums = pltpu.roll(sums, step, 0) + pltpu.roll(sums, padded - step, 0)
        chosen = jnp.where(tp >= level, sums, chosen)
    half = jnp.left_shift(1, tp)
    position = here * rows + lax.broadcasted_iota(jnp.int32, (rows, LANES), 0)
    last = place[3] * rows - 1
    low_end = jnp.maximum(position - half, 0)
    high_end = jnp.minimum(position + half - 1, last)
    counted = (high_end - low_end + 1).astype(f32)[:, 0:1]
    inside = slice(rim_width, rim_width + rows)
    pooled = (chosen[inside] / counted - values[inside]).astype(bf16)
    out[...] = matmul(pooled, group_map[tp]).astype(bf16)


def finish_kernel(part, query, entering, pooled, out):
    channel_one = lax.broadcasted_iota(jnp.int32, (LANES, DV), 0) < KEY_CHANNELS
    zero = jnp.zeros((), bf16)
    sides = []
    for d in range(2):
        state = entering[:, 0, d * LANES : (d + 1) * LANES].astype(bf16)
        sides.append(
            jnp.concatenate(
                [jnp.where(channel_one, state, zero), jnp.where(channel_one, zero, state)], axis=1
            )
        )
    joined = part[...] + matmul(query[...], jnp.concatenate(sides, axis=0))
    rows = joined.shape[0]
    ready = [pooled[...]]
    for h in range(2):
        mine = joined[:, h * DV : (h + 1) * DV]
        scale = lax.rsqrt(jnp.mean(mine * mine, axis=1, keepdims=True) + eps_value)
        ready.append((mine * scale).astype(bf16))
    owners = out.shape[0]
    for j in range(owners):
        at = slice(j * rows // owners, (j + 1) * rows // owners)
        start = 0
        for piece in ready:
            out[j, :, start : start + piece.shape[1]] = piece[at]
            start += piece.shape[1]


def output_kernel(place, activations, weight, out, total):
    groups = activations.shape[0]
    step, part = (pl.program_id(0), pl.program_id(1))
    tile = weight.shape[0]
    here = pl.ds(pl.multiple_of(part * tile, tile), tile)
    source = lax.rem(place[0] + groups - step, groups)
    partial = matmul(weight[...], activations[source], ((1,), (1,))).astype(bf16).astype(f32)

    @pl.when(step == 0)
    def _():
        total[here, :] = partial

    @pl.when(step > 0)
    def _():
        total[here, :] += partial

    @pl.when(step == groups - 1)
    def _():
        out[:, here] = total[here, :].T.astype(bf16)


def output_projection(place, activations, weights):
    groups, rows, width = activations.shape
    model = weights.shape[0]
    parts = 2
    return pl.pallas_call(
        output_kernel,
        grid=(groups, parts),
        in_specs=[
            pl.BlockSpec(memory_space=pltpu.SMEM),
            pl.BlockSpec((groups, rows, width), lambda s, n: (0, 0, 0)),
            pl.BlockSpec((model // parts, width), lambda s, n: (n, s)),
        ],
        out_specs=pl.BlockSpec((rows, model), lambda s, n: (0, 0)),
        out_shape=jax.ShapeDtypeStruct((rows, model), bf16),
        scratch_shapes=[pltpu.VMEM((model, rows), f32)],
        interpret=interpreted,
        name="output_kernel",
    )(place, activations, weights)


def shape_of(*lengths, kind=bf16):
    return jax.ShapeDtypeStruct(lengths, kind)


def shards(
    tokens,
    pooling_input_weight,
    query_matrix,
    key_matrix,
    value_matrix,
    decay_inner_weight,
    decay_outer_weight,
    channel_decay_bias,
    spike_log_decay,
    starting_state,
    pooling_group_map,
    pooling_output_weight,
    attention_output_weight,
):
    sp_index = lax.axis_index(SP)
    tp_index = lax.axis_index("tp")
    core = lax.axis_index("sp_2")
    positions = lax.axis_size(SP)
    place = jnp.stack([tp_index, core, sp_index, jnp.int32(positions)]).astype(jnp.int32)
    groups = lax.axis_size("tp")
    rows = tokens.shape[0] * groups
    model = tokens.shape[1]

    local_in = jnp.concatenate(
        [query_matrix, key_matrix, value_matrix, pooling_input_weight], axis=1
    )
    chips = lax.axis_size(CHIPS)
    copies = jnp.broadcast_to(local_in, (chips, *local_in.shape))
    weight_own = lax.all_to_all(copies, CHIPS, 0, 0, tiled=True)
    local_out = jnp.concatenate([pooling_output_weight, attention_output_weight], axis=0).T
    outs = [local_out] + [shifted(local_out, "tp", k) for k in range(1, groups)]
    normed = normalize(tokens)
    half = normed.shape[0] // 2
    before = shifted(normed, "tp", 1)
    after = shifted(normed, "tp", -1)
    top, end = (before[:half], after[half:])
    far_top = shifted(top, "tp", 1)
    far_end = shifted(end, "tp", -1)
    weight_other = shifted(weight_own, "sp_2", 1)
    whole_out = lax.all_gather(jnp.concatenate(outs, axis=1), SP, axis=0, tiled=True)

    all_tokens, logs = call(
        decay_kernel,
        (shape_of(rows, model), shape_of(2, rows, LANES, kind=f32)),
        (
            place,
            normed,
            before,
            after,
            far_top,
            far_end,
            decay_inner_weight,
            decay_outer_weight,
            channel_decay_bias,
            spike_log_decay.T,
        ),
        flops=2 * rows * model * 4 * LANES,
        moved=5_000_000,
    )
    qkv, pool_input, packed = call(
        project_kernel,
        (
            shape_of(rows, 4 * LANES),
            shape_of(rows, 2 * LANES),
            shape_of(LANES, 1, 3 * LANES, kind=f32),
        ),
        (place, weight_own, weight_other, all_tokens, logs),
        far=2,
        scratch=(
            pltpu.VMEM((chips, 2, model // (2 * chips), 6 * LANES), bf16),
            pltpu.SemaphoreType.DMA((2,)),
        ),
        flops=2 * rows * model * 7 * LANES,
        moved=8_000_000,
    )
    received = lax.all_to_all(packed, SP, 0, 0, tiled=True)
    rim_before = neighbours(pool_input[rows - rim_width :], SP, 1)
    rim_after = neighbours(pool_input[:rim_width], SP, -1)
    part, query = call(
        inner_kernel,
        (shape_of(rows, 2 * DV, kind=f32), shape_of(rows, 2 * LANES)),
        (qkv, logs),
        scalars=0,
        flops=2 * rows * model * 2 * LANES,
        moved=3_000_000,
    )
    states = call(
        scan_kernel,
        shape_of(positions, 1, 2 * LANES, kind=f32),
        (place[2:3], received, starting_state.reshape(2, -1, DV)),
        flops=40_000_000,
    )
    entering = lax.all_to_all(states, SP, 0, 0, tiled=True)
    pooled = call(
        pool_kernel,
        shape_of(rows, 2 * LANES),
        (place, pool_input, rim_before, rim_after, pooling_group_map),
        flops=2 * rows * 4 * LANES * LANES,
        moved=1_000_000,
    )
    activations = call(
        finish_kernel,
        shape_of(groups, rows // groups, 4 * LANES),
        (part, query, entering, pooled),
        scalars=0,
        flops=100_000_000,
        moved=2_000_000,
    )
    gathered = lax.all_to_all(activations, "tp", 0, 0, tiled=True)
    return output_projection(place, gathered, whole_out)


def solution(mesh):
    split = Mesh(mesh.devices.reshape(8, 8, 2, mesh.shape["tp"]), ("sp_0", "sp_1", "sp_2", "tp"))
    in_specs = (
        P(SP_TP, None),
        P(SP, "tp"),
        P(SP, "tp"),
        P(SP, "tp"),
        P(SP, "tp"),
        P(),
        P(),
        P(),
        P("tp", SP),
        P(None, "tp", None, None),
        P(),
        P("tp", SP),
        P("tp", SP),
    )
    out_specs = P(SP_TP, None)
    return jax.shard_map(
        shards, mesh=split, in_specs=in_specs, out_specs=out_specs, check_vma=False
    )
```

```python
import jax
import jax.numpy as jnp
from jax import lax
from jax.experimental import pallas as pl
from jax.experimental.pallas import tpu as pltpu
from jax.sharding import Mesh
from jax.sharding import PartitionSpec as P


KEY_CHANNELS = 64
DV = 128
RANK = 32
BLOCK = 64
LANES = 128
SP = ("sp_0", "sp_1", "sp_2")
CHIPS = ("sp_0", "sp_1")
SP_TP = ("sp_0", "sp_1", "sp_2", "tp")

eps_value = 1e-06
gate_norm_factor = 16.0
rim_width = 8
interpreted = False

bf16 = jnp.bfloat16
f32 = jnp.float32


def matmul(a, b, dims=((1,), (0,)), precision=None):
    return lax.dot_general(a, b, (dims, ((), ())), precision=precision, preferred_element_type=f32)


def call(kernel, out_shapes, operands, scalars=1, far=0, scratch=(), flops=0, moved=0):
    smem = pl.BlockSpec(memory_space=pltpu.SMEM)
    vmem = pl.BlockSpec(memory_space=pltpu.VMEM)
    anywhere = pl.BlockSpec(memory_space=pl.ANY)
    near = len(operands) - scalars - far
    return pl.pallas_call(
        kernel,
        in_specs=[smem] * scalars + [anywhere] * far + [vmem] * near,
        out_specs=jax.tree.map(lambda _: vmem, out_shapes),
        out_shape=out_shapes,
        scratch_shapes=list(scratch),
        cost_estimate=pl.CostEstimate(flops=flops, bytes_accessed=moved, transcendentals=0),
        interpret=interpreted,
    )(*operands)


def shifted(value, axis, step):
    devices = lax.axis_size(axis)
    return lax.ppermute(value, axis, [(i, (i + step) % devices) for i in range(devices)])


def neighbours(value, axes, step):
    devices = lax.axis_size(axes)
    pairs = [(i, i + step) for i in range(devices) if 0 <= i + step < devices]
    return lax.ppermute(value, axes, pairs)


def normalize(token_rows):
    floats = token_rows.astype(f32)
    scaled = floats * lax.rsqrt(jnp.mean(floats * floats, axis=-1, keepdims=True) + eps_value)
    return scaled.astype(bf16)


def place_tokens(tp, pieces, whole_ref, first):
    own, before, after, far_top, far_end = pieces
    rows = own.shape[0]
    half = rows // 2

    def at(step):
        return pl.multiple_of(first + lax.rem(tp + step, 4) * rows, 8)

    whole_ref[pl.ds(at(0), rows), :] = own[...]
    whole_ref[pl.ds(at(3), rows), :] = before[...]
    whole_ref[pl.ds(at(1), rows), :] = after[...]
    far = at(2)
    whole_ref[pl.ds(far, half), :] = far_top[...]
    whole_ref[pl.ds(pl.multiple_of(far + half, 8), half), :] = far_end[...]


def split_dot(ones, values):
    high = values.astype(bf16)
    low = (values - high.astype(f32)).astype(bf16)
    return matmul(ones, high) + matmul(ones, low)


def decay_kernel(
    place,
    own,
    before,
    after,
    far_top,
    far_end,
    inner,
    outer,
    bias,
    spike,
    tokens_out,
    logs_out,
):
    tp = place[0]
    place_tokens(tp, (own, before, after, far_top, far_end), tokens_out, 0)
    rows = tokens_out.shape[0]
    low_rank = matmul(tokens_out[...], inner[...], ((1,), (1,))).astype(bf16)
    here = pl.ds(pl.multiple_of(tp * LANES, LANES), LANES)
    blank = jnp.zeros((RANK, LANES), bf16)
    outer_both = jnp.concatenate(
        [
            jnp.concatenate([outer[0, :, here], blank], axis=1),
            jnp.concatenate([blank, outer[1, :, here]], axis=1),
        ],
        axis=0,
    )
    bias_both = jnp.concatenate([bias[0:1, here], bias[1:2, here]], axis=1)
    pre = matmul(low_rank, outer_both) + bias_both
    gate = jnp.minimum(pre, 0.0) - jnp.log1p(jnp.exp(-jnp.abs(pre)))
    lane = lax.broadcasted_iota(jnp.int32, (rows, LANES), 1)
    spike_rows = jnp.concatenate([spike[...], jnp.zeros((6, rows), f32)], axis=0).T
    spikes = jnp.where(lane < KEY_CHANNELS, spike_rows[:, 0:1], spike_rows[:, 1:2])
    decay = gate * (1.0 / gate_norm_factor) + jnp.concatenate([spikes, spikes], axis=1)
    size = LANES
    row_ids = lax.broadcasted_iota(jnp.int32, (size, size), 0)
    col_ids = lax.broadcasted_iota(jnp.int32, (size, size), 1)
    upto = (col_ids <= row_ids).astype(bf16)
    onward = (col_ids >= row_ids).astype(bf16)
    tiles = rows // size
    carry = jnp.zeros((1, LANES), f32)
    for n in range(tiles):
        found = split_dot(upto, decay[n * size : (n + 1) * size, :LANES]) + carry
        logs_out[0, n * size : (n + 1) * size, :] = found
        carry = found[size - 1 : size, :]
    carry = jnp.zeros((1, LANES), f32)
    for n in reversed(range(tiles)):
        found = split_dot(onward, decay[n * size : (n + 1) * size, LANES:]) + carry
        logs_out[1, n * size : (n + 1) * size, :] = found
        carry = found[0:1, :]


def load_weights(core, start, weight_own, weight_other, weight_ref, sems):
    columns = slice(start, start + weight_ref.shape[-1])
    for n, (side, source) in enumerate(((core, weight_own), (1 - core, weight_other))):
        yield pltpu.make_async_copy(
            source.at[:, :, columns], weight_ref.at[:, side], sems.at[n]
        )


def project_kernel(
    place, weight_own, weight_other, tokens, logs, keys_values, packed_out, tokens_ref, weight_ref, sems
):
    loads = list(load_weights(place[1], 0, weight_own, weight_other, weight_ref, sems))
    loads.append(pltpu.make_async_copy(tokens, tokens_ref, sems.at[2]))
    for load in loads:
        load.start()
    rows, width = tokens_ref.shape
    total_fwd = logs[0, rows - 1 : rows, :]
    total_bwd = logs[1, 0:1, :]
    far_fwd = jnp.exp(total_fwd - logs[0])
    far_bwd = jnp.exp(total_bwd - logs[1])
    for load in loads:
        load.wait()
    found = matmul(tokens_ref[...], weight_ref[...].reshape(width, -1)).astype(bf16)
    keys_values[...] = found
    keys = found[:, :LANES].astype(f32)
    weighted = jnp.concatenate(
        [(keys * far_fwd).astype(bf16), (keys * far_bwd).astype(bf16)], axis=1
    )
    updates = matmul(weighted, found[:, LANES:], ((0,), (0,)))
    first = lax.broadcasted_iota(jnp.int32, (LANES, LANES), 0) < KEY_CHANNELS
    for d in range(2):
        mine = updates[d * LANES : (d + 1) * LANES]
        packed_out[:, 0, d * LANES : (d + 1) * LANES] = jnp.where(
            first, mine[:, :LANES], mine[:, LANES:]
        )
    totals = jnp.concatenate([total_fwd, total_bwd], axis=0)
    stacked = jnp.concatenate([totals, jnp.zeros((LANES - 2, LANES), f32)], axis=0)
    packed_out[:, 0, 2 * LANES :] = stacked.T


def late_kernel(
    place, weight_own, weight_other, tokens, query_out, pool_out, tokens_ref, weight_ref, sems
):
    loads = list(load_weights(place[1], 3 * LANES, weight_own, weight_other, weight_ref, sems))
    loads.append(pltpu.make_async_copy(tokens, tokens_ref, sems.at[2]))
    for load in loads:
        load.start()
    for load in loads:
        load.wait()
    width = tokens_ref.shape[1]
    found = matmul(tokens_ref[...], weight_ref[...].reshape(width, -1)).astype(bf16)
    query_out[...] = found[:, :LANES]
    pool_out[...] = found[:, LANES:]


def scan_kernel(place, received, start, out):
    devices = received.shape[0]
    here = place[0]
    logs = received[:, 0, 2 * LANES :]
    row = lax.broadcasted_iota(jnp.int32, (devices, devices), 0)
    col = lax.broadcasted_iota(jnp.int32, (devices, devices), 1)
    high = logs.astype(bf16)
    low = (logs - high.astype(f32)).astype(bf16)
    turn = ((0,), (0,))
    earlier = (col < row).astype(bf16)
    strictly = (row < col).astype(bf16)
    upto = (row <= col).astype(bf16)
    before_col = matmul(earlier, high) + matmul(earlier, low)
    before_row = matmul(high, strictly, turn) + matmul(low, strictly, turn)
    past_row = matmul(high, upto, turn) + matmul(low, upto, turn)
    logs = high.astype(f32) + low.astype(f32)
    past_col = before_col + logs
    total = jnp.sum(logs, axis=0, keepdims=True)
    for r in range(2):
        if r == 0:
            between = before_col[:, 0:1] - past_row[0:1, :]
            allowed = col < row
            outside = before_col[:, 0:1]
        else:
            between = before_row[1:2, :] - past_col[:, 1:2]
            allowed = col > row
            outside = total[:, 1:2] - past_col[:, 1:2]
        weights = jnp.where(allowed, jnp.exp(jnp.minimum(between, 0.0)), 0.0)
        high = weights.astype(bf16)
        low = (weights - high.astype(f32)).astype(bf16)
        updates = received[:, 0, r * LANES : (r + 1) * LANES].astype(bf16)
        first = start[r, pl.ds(here, 1), :]
        entering = matmul(high, updates) + matmul(low, updates)
        entering = entering + jnp.exp(jnp.minimum(outside, 0.0)) * first
        out[:, 0, r * LANES : (r + 1) * LANES] = entering


def inner_kernel(query, keys_values, logs, part_out, query_out):
    rows = query.shape[0]
    blocks = rows // BLOCK
    lane = lax.broadcasted_iota(jnp.int32, (BLOCK, LANES), 1)
    row = lax.broadcasted_iota(jnp.int32, (BLOCK, LANES), 0)
    head_one = lane < KEY_CHANNELS
    lower = lax.rem(lane, KEY_CHANNELS) <= row
    value_lane = lax.broadcasted_iota(jnp.int32, (BLOCK, 2 * DV), 1)
    value_one = value_lane < DV
    diagonal = (
        lax.rem(lax.broadcasted_iota(jnp.int32, (4 * KEY_CHANNELS, 2 * DV), 0), LANES)
        < KEY_CHANNELS
    ) == (lax.broadcasted_iota(jnp.int32, (4 * KEY_CHANNELS, 2 * DV), 1) < DV)
    zero = jnp.zeros((), bf16)
    scale = KEY_CHANNELS ** (-0.5)
    edges, updates, scaled, scored = [], [], [], []
    nothing = jnp.zeros((1, LANES), f32)
    for n in range(blocks):
        at = slice(n * BLOCK, (n + 1) * BLOCK)
        base_fwd = logs[0, n * BLOCK - 1 : n * BLOCK, :] if n else nothing
        base_bwd = logs[1, (n + 1) * BLOCK : (n + 1) * BLOCK + 1, :] if n + 1 < blocks else nothing
        cum_fwd = logs[0, at, :] - base_fwd
        cum_bwd = logs[1, at, :] - base_bwd
        edge_fwd = cum_fwd[BLOCK - 1 : BLOCK, :]
        edge_bwd = cum_bwd[0:1, :]
        queries = query[at, :].astype(f32) * scale
        keys = keys_values[at, :LANES].astype(f32)
        values = keys_values[at, LANES:]
        query_out[at, :LANES] = (queries * jnp.exp(logs[0, at, :])).astype(bf16)
        query_out[at, LANES:] = (queries * jnp.exp(logs[1, at, :])).astype(bf16)
        query_fwd = (queries * jnp.exp(cum_fwd)).astype(bf16)
        query_bwd = (queries * jnp.exp(cum_bwd)).astype(bf16)
        key_fwd = (keys * jnp.exp(-cum_fwd)).astype(bf16)
        key_bwd = (keys * jnp.exp(-cum_bwd)).astype(bf16)

        def by_head(key):
            return jnp.concatenate(
                [jnp.where(head_one, key, zero), jnp.where(head_one, zero, key)], axis=0
            )

        across = ((1,), (1,))
        scores = jnp.where(
            lower,
            matmul(query_fwd, by_head(key_fwd), across),
            matmul(query_bwd, by_head(key_bwd), across),
        ).astype(bf16)
        spread = jnp.concatenate(
            [jnp.where(value_one, values, zero), jnp.where(value_one, zero, values)], axis=0
        )
        scored.append(matmul(scores, spread))
        scaled.append(jnp.concatenate([query_fwd, query_bwd], axis=1))
        weighted = jnp.concatenate(
            [
                (keys * jnp.exp(edge_fwd - cum_fwd)).astype(bf16),
                (keys * jnp.exp(edge_bwd - cum_bwd)).astype(bf16),
            ],
            axis=1,
        )
        update = matmul(weighted, values, ((0,), (0,)))
        updates.append(jnp.where(diagonal, update, 0.0))
        edges.append((edge_fwd, edge_bwd))
    stacked = jnp.concatenate(
        [e[0] for e in edges]
        + [e[1] for e in edges]
        + [jnp.zeros((LANES - 2 * blocks, LANES), f32)],
        axis=0,
    )
    factors = jnp.exp(stacked.T)
    start_fwd, start_bwd = [None] * blocks, [None] * blocks
    memory = jnp.zeros((LANES, 2 * DV), f32)
    for n in range(blocks):
        start_fwd[n] = memory.astype(bf16)
        memory = factors[:, n : n + 1] * memory + updates[n][:LANES]
    memory = jnp.zeros((LANES, 2 * DV), f32)
    for n in reversed(range(blocks)):
        start_bwd[n] = memory.astype(bf16)
        memory = factors[:, blocks + n : blocks + n + 1] * memory + updates[n][LANES:]
    for n in range(blocks):
        entering = jnp.concatenate([start_fwd[n], start_bwd[n]], axis=0)
        part_out[n * BLOCK : (n + 1) * BLOCK, :] = scored[n] + matmul(scaled[n], entering)


def pool_kernel(place, pool_input, rim_before, rim_after, group_map, out):
    tp, here = (place[0], place[2])
    rows = out.shape[0]
    padded = rows + 2 * rim_width
    values = jnp.concatenate([rim_before[...], pool_input[...], rim_after[...]], axis=0).astype(f32)
    sums = values + pltpu.roll(values, 1, 0)
    chosen = sums
    for level in (1, 2, 3):
        step = 2 ** (level - 1)
        sums = pltpu.roll(sums, step, 0) + pltpu.roll(sums, padded - step, 0)
        chosen = jnp.where(tp >= level, sums, chosen)
    half = jnp.left_shift(1, tp)
    position = here * rows + lax.broadcasted_iota(jnp.int32, (rows, LANES), 0)
    last = place[3] * rows - 1
    low_end = jnp.maximum(position - half, 0)
    high_end = jnp.minimum(position + half - 1, last)
    counted = (high_end - low_end + 1).astype(f32)[:, 0:1]
    inside = slice(rim_width, rim_width + rows)
    pooled = (chosen[inside] / counted - values[inside]).astype(bf16)
    out[...] = matmul(pooled, group_map[tp]).astype(bf16)


def finish_kernel(part, query, entering, pooled, out):
    channel_one = lax.broadcasted_iota(jnp.int32, (LANES, DV), 0) < KEY_CHANNELS
    zero = jnp.zeros((), bf16)
    sides = []
    for d in range(2):
        state = entering[:, 0, d * LANES : (d + 1) * LANES].astype(bf16)
        sides.append(
            jnp.concatenate(
                [jnp.where(channel_one, state, zero), jnp.where(channel_one, zero, state)], axis=1
            )
        )
    joined = part[...] + matmul(query[...], jnp.concatenate(sides, axis=0))
    rows = joined.shape[0]
    ready = [pooled[...]]
    for h in range(2):
        mine = joined[:, h * DV : (h + 1) * DV]
        scale = lax.rsqrt(jnp.mean(mine * mine, axis=1, keepdims=True) + eps_value)
        ready.append((mine * scale).astype(bf16))
    owners = out.shape[0]
    for j in range(owners):
        at = slice(j * rows // owners, (j + 1) * rows // owners)
        start = 0
        for piece in ready:
            out[j, :, start : start + piece.shape[1]] = piece[at]
            start += piece.shape[1]


def output_kernel(place, weights, activations, out, weight_ref, total, sems):
    groups, _, width = activations.shape
    parts, tile = weight_ref.shape[1:3]
    loads = {}
    for s in range(groups):
        for n in range(parts):
            loads[s, n] = pltpu.make_async_copy(
                weights.at[n * tile : (n + 1) * tile, s * width : (s + 1) * width],
                weight_ref.at[s, n],
                sems.at[s * parts + n],
            )
            loads[s, n].start()
    for s in range(groups):
        mine = activations[lax.rem(place[0] + groups - s, groups)]
        for n in range(parts):
            here = slice(n * tile, (n + 1) * tile)
            loads[s, n].wait()
            partial = matmul(weight_ref[s, n], mine, ((1,), (1,))).astype(bf16).astype(f32)
            if s == 0:
                total[here, :] = partial
            elif s + 1 < groups:
                total[here, :] += partial
            else:
                out[:, here] = (total[here, :] + partial).T.astype(bf16)


def output_projection(place, activations, weights):
    groups, rows, width = activations.shape
    model = weights.shape[0]
    parts = 2
    return call(
        output_kernel,
        shape_of(rows, model),
        (place, weights, activations),
        far=1,
        scratch=(
            pltpu.VMEM((groups, parts, model // parts, width), bf16),
            pltpu.VMEM((model, rows), f32),
            pltpu.SemaphoreType.DMA((groups * parts,)),
        ),
        flops=2 * rows * model * groups * width,
        moved=2 * model * groups * width,
    )


def shape_of(*lengths, kind=bf16):
    return jax.ShapeDtypeStruct(lengths, kind)


def shards(
    tokens,
    pooling_input_weight,
    query_matrix,
    key_matrix,
    value_matrix,
    decay_inner_weight,
    decay_outer_weight,
    channel_decay_bias,
    spike_log_decay,
    starting_state,
    pooling_group_map,
    pooling_output_weight,
    attention_output_weight,
):
    sp_index = lax.axis_index(SP)
    tp_index = lax.axis_index("tp")
    core = lax.axis_index("sp_2")
    positions = lax.axis_size(SP)
    place = jnp.stack([tp_index, core, sp_index, jnp.int32(positions)]).astype(jnp.int32)
    groups = lax.axis_size("tp")
    rows = tokens.shape[0] * groups
    model = tokens.shape[1]

    local_in = jnp.concatenate(
        [key_matrix, value_matrix, query_matrix, pooling_input_weight], axis=1
    )
    chips = lax.axis_size(CHIPS)
    copies = jnp.broadcast_to(local_in, (chips, *local_in.shape))
    weight_own = lax.all_to_all(copies, CHIPS, 0, 0, tiled=True)
    local_out = jnp.concatenate([pooling_output_weight, attention_output_weight], axis=0).T
    outs = [local_out] + [shifted(local_out, "tp", k) for k in range(1, groups)]
    normed = normalize(tokens)
    half = normed.shape[0] // 2
    before = shifted(normed, "tp", 1)
    after = shifted(normed, "tp", -1)
    top, end = (before[:half], after[half:])
    far_top = shifted(top, "tp", 1)
    far_end = shifted(end, "tp", -1)
    weight_other = shifted(weight_own, "sp_2", 1)
    whole_out = lax.all_gather(jnp.concatenate(outs, axis=1), SP, axis=0, tiled=True)

    all_tokens, logs = call(
        decay_kernel,
        (shape_of(rows, model), shape_of(2, rows, LANES, kind=f32)),
        (
            place,
            normed,
            before,
            after,
            far_top,
            far_end,
            decay_inner_weight.T,
            decay_outer_weight,
            channel_decay_bias,
            spike_log_decay,
        ),
        flops=2 * rows * model * 4 * LANES,
        moved=5_000_000,
    )
    project_scratch = (
        pltpu.VMEM((rows, model), bf16),
        pltpu.VMEM((chips, 2, model // (2 * chips), 3 * LANES), bf16),
        pltpu.SemaphoreType.DMA((3,)),
    )
    keys_values, packed = call(
        project_kernel,
        (shape_of(rows, 3 * LANES), shape_of(LANES, 1, 3 * LANES, kind=f32)),
        (place, weight_own, weight_other, all_tokens, logs),
        far=3,
        scratch=project_scratch,
        flops=2 * rows * model * 4 * LANES,
        moved=4_000_000,
    )
    received = lax.all_to_all(packed, SP, 0, 0, tiled=True)
    query, pool_input = call(
        late_kernel,
        (shape_of(rows, LANES), shape_of(rows, 2 * LANES)),
        (place, weight_own, weight_other, all_tokens),
        far=3,
        scratch=project_scratch,
        flops=2 * rows * model * 3 * LANES,
        moved=4_000_000,
    )
    part, query = call(
        inner_kernel,
        (shape_of(rows, 2 * DV, kind=f32), shape_of(rows, 2 * LANES)),
        (query, keys_values, logs),
        scalars=0,
        flops=2 * rows * model * 2 * LANES,
        moved=3_000_000,
    )
    rim_before = neighbours(pool_input[rows - rim_width :], SP, 1)
    rim_after = neighbours(pool_input[:rim_width], SP, -1)
    states = call(
        scan_kernel,
        shape_of(positions, 1, 2 * LANES, kind=f32),
        (place[2:3], received, starting_state.reshape(2, -1, DV)),
        flops=40_000_000,
    )
    entering = lax.all_to_all(states, SP, 0, 0, tiled=True)
    pooled = call(
        pool_kernel,
        shape_of(rows, 2 * LANES),
        (place, pool_input, rim_before, rim_after, pooling_group_map),
        flops=2 * rows * 4 * LANES * LANES,
        moved=1_000_000,
    )
    activations = call(
        finish_kernel,
        shape_of(groups, rows // groups, 4 * LANES),
        (part, query, entering, pooled),
        scalars=0,
        flops=100_000_000,
        moved=2_000_000,
    )
    gathered = lax.all_to_all(activations, "tp", 0, 0, tiled=True)
    return output_projection(place, gathered, whole_out)


def solution(mesh):
    split = Mesh(mesh.devices.reshape(8, 8, 2, mesh.shape["tp"]), ("sp_0", "sp_1", "sp_2", "tp"))
    in_specs = (
        P(SP_TP, None),
        P(SP, "tp"),
        P(SP, "tp"),
        P(SP, "tp"),
        P(SP, "tp"),
        P(),
        P(),
        P(),
        P("tp", SP),
        P(None, "tp", None, None),
        P(),
        P("tp", SP),
        P("tp", SP),
    )
    out_specs = P(SP_TP, None)
    return jax.shard_map(
        shards, mesh=split, in_specs=in_specs, out_specs=out_specs, check_vma=False
    )
```

```python
import jax
import jax.numpy as jnp
from jax import lax
from jax.experimental import pallas as pl
from jax.experimental.pallas import tpu as pltpu
from jax.sharding import Mesh
from jax.sharding import PartitionSpec as P


KEY_CHANNELS = 64
DV = 128
RANK = 32
BLOCK = 64
LANES = 128
SP = ("sp_0", "sp_1", "sp_2")
CHIPS = ("sp_0", "sp_1")
GROUP = ("sp_1", "sp_2")
SP_TP = ("sp_0", "sp_1", "sp_2", "tp")

eps_value = 1e-06
gate_norm_factor = 16.0
rim_width = 8
interpreted = False

bf16 = jnp.bfloat16
f32 = jnp.float32


def matmul(a, b, dims=((1,), (0,)), precision=None):
    return lax.dot_general(a, b, (dims, ((), ())), precision=precision, preferred_element_type=f32)


def call(kernel, out_shapes, operands, scalars=1, far=0, scratch=(), flops=0, moved=0):
    smem = pl.BlockSpec(memory_space=pltpu.SMEM)
    vmem = pl.BlockSpec(memory_space=pltpu.VMEM)
    anywhere = pl.BlockSpec(memory_space=pl.ANY)
    near = len(operands) - scalars - far
    return pl.pallas_call(
        kernel,
        in_specs=[smem] * scalars + [anywhere] * far + [vmem] * near,
        out_specs=jax.tree.map(lambda _: vmem, out_shapes),
        out_shape=out_shapes,
        scratch_shapes=list(scratch),
        cost_estimate=pl.CostEstimate(flops=flops, bytes_accessed=moved, transcendentals=0),
        interpret=interpreted,
    )(*operands)


def shifted(value, axis, step):
    devices = lax.axis_size(axis)
    return lax.ppermute(value, axis, [(i, (i + step) % devices) for i in range(devices)])


def neighbours(value, axes, step):
    devices = lax.axis_size(axes)
    pairs = [(i, i + step) for i in range(devices) if 0 <= i + step < devices]
    return lax.ppermute(value, axes, pairs)


def normalize(token_rows):
    floats = token_rows.astype(f32)
    scaled = floats * lax.rsqrt(jnp.mean(floats * floats, axis=-1, keepdims=True) + eps_value)
    return scaled.astype(bf16)


def place_tokens(tp, pieces, whole_ref, first):
    own, before, after, far_top, far_end = pieces
    rows = own.shape[0]
    half = rows // 2

    def at(step):
        return pl.multiple_of(first + lax.rem(tp + step, 4) * rows, 8)

    whole_ref[pl.ds(at(0), rows), :] = own[...]
    whole_ref[pl.ds(at(3), rows), :] = before[...]
    whole_ref[pl.ds(at(1), rows), :] = after[...]
    far = at(2)
    whole_ref[pl.ds(far, half), :] = far_top[...]
    whole_ref[pl.ds(pl.multiple_of(far + half, 8), half), :] = far_end[...]


def split_dot(ones, values):
    high = values.astype(bf16)
    low = (values - high.astype(f32)).astype(bf16)
    return matmul(ones, high) + matmul(ones, low)


def decay_kernel(
    place,
    own,
    before,
    after,
    far_top,
    far_end,
    inner,
    outer,
    bias,
    spike,
    tokens_out,
    logs_out,
):
    tp = place[0]
    place_tokens(tp, (own, before, after, far_top, far_end), tokens_out, 0)
    rows = tokens_out.shape[0]
    low_rank = matmul(tokens_out[...], inner[...], ((1,), (1,))).astype(bf16)
    here = pl.ds(pl.multiple_of(tp * LANES, LANES), LANES)
    blank = jnp.zeros((RANK, LANES), bf16)
    outer_both = jnp.concatenate(
        [
            jnp.concatenate([outer[0, :, here], blank], axis=1),
            jnp.concatenate([blank, outer[1, :, here]], axis=1),
        ],
        axis=0,
    )
    bias_both = jnp.concatenate([bias[0:1, here], bias[1:2, here]], axis=1)
    pre = matmul(low_rank, outer_both) + bias_both
    gate = jnp.minimum(pre, 0.0) - jnp.log1p(jnp.exp(-jnp.abs(pre)))
    lane = lax.broadcasted_iota(jnp.int32, (rows, LANES), 1)
    spike_rows = jnp.concatenate([spike[...], jnp.zeros((6, rows), f32)], axis=0).T
    spikes = jnp.where(lane < KEY_CHANNELS, spike_rows[:, 0:1], spike_rows[:, 1:2])
    decay = gate * (1.0 / gate_norm_factor) + jnp.concatenate([spikes, spikes], axis=1)
    size = LANES
    row_ids = lax.broadcasted_iota(jnp.int32, (size, size), 0)
    col_ids = lax.broadcasted_iota(jnp.int32, (size, size), 1)
    upto = (col_ids <= row_ids).astype(bf16)
    onward = (col_ids >= row_ids).astype(bf16)
    tiles = rows // size
    carry = jnp.zeros((1, LANES), f32)
    for n in range(tiles):
        found = split_dot(upto, decay[n * size : (n + 1) * size, :LANES]) + carry
        logs_out[0, n * size : (n + 1) * size, :] = found
        carry = found[size - 1 : size, :]
    carry = jnp.zeros((1, LANES), f32)
    for n in reversed(range(tiles)):
        found = split_dot(onward, decay[n * size : (n + 1) * size, LANES:]) + carry
        logs_out[1, n * size : (n + 1) * size, :] = found
        carry = found[0:1, :]


def project_kernel(
    place,
    weight_own,
    weight_other,
    tokens,
    logs,
    qkv_out,
    pool_out,
    packed_out,
    tokens_ref,
    weight_ref,
    sems,
):
    core = place[1]
    loads = (
        pltpu.make_async_copy(tokens, tokens_ref, sems.at[0]),
        pltpu.make_async_copy(weight_own, weight_ref.at[:, core], sems.at[1]),
        pltpu.make_async_copy(weight_other, weight_ref.at[:, 1 - core], sems.at[2]),
    )
    for load in loads:
        load.start()
    rows, width = tokens_ref.shape
    total_fwd = logs[0, rows - 1 : rows, :]
    total_bwd = logs[1, 0:1, :]
    far_fwd = jnp.exp(total_fwd - logs[0])
    far_bwd = jnp.exp(total_bwd - logs[1])
    totals = jnp.concatenate([total_fwd, total_bwd], axis=0)
    high = totals.astype(bf16).astype(f32)
    stacked = jnp.concatenate([high, totals - high, jnp.zeros((LANES - 4, LANES), f32)], axis=0)
    packed_out[:, 2 * LANES :] = stacked.T.astype(bf16)
    for load in loads:
        load.wait()
    projected = matmul(tokens_ref[...], weight_ref[...].reshape(width, -1)).astype(bf16)
    qkv = projected[:, : 4 * LANES]
    qkv_out[...] = qkv
    pool_out[...] = projected[:, 4 * LANES :]
    keys = qkv[:, LANES : 2 * LANES].astype(f32)
    weighted = jnp.concatenate(
        [(keys * far_fwd).astype(bf16), (keys * far_bwd).astype(bf16)], axis=1
    )
    updates = matmul(weighted, qkv[:, 2 * LANES :], ((0,), (0,)))
    first = lax.broadcasted_iota(jnp.int32, (LANES, LANES), 0) < KEY_CHANNELS
    for d in range(2):
        mine = updates[d * LANES : (d + 1) * LANES]
        packed_out[:, d * LANES : (d + 1) * LANES] = jnp.where(
            first, mine[:, :LANES], mine[:, LANES:]
        ).astype(bf16)


def decays_of(tile):
    edge = tile[:, 2 * LANES :].astype(f32)
    return [edge[:, d : d + 1] + edge[:, d + 2 : d + 3] for d in range(2)]


def updates_of(tile):
    return [tile[:, d * LANES : (d + 1) * LANES].astype(f32) for d in range(2)]


def total_kernel(received, out):
    members, rows = received.shape[:2]
    orders = (range(members), reversed(range(members)))
    lane = lax.broadcasted_iota(jnp.int32, (rows, LANES), 1)
    edge = jnp.zeros((rows, LANES), f32)
    for d, order in enumerate(orders):
        state = jnp.zeros((rows, LANES), f32)
        total = jnp.zeros((rows, 1), f32)
        for n in order:
            tile = received[n]
            log = decays_of(tile)[d]
            state = jnp.exp(log) * state + updates_of(tile)[d]
            total = total + log
        high = total.astype(bf16).astype(f32)
        edge = jnp.where(lane == d, high, jnp.where(lane == d + 2, total - high, edge))
        out[:, d * LANES : (d + 1) * LANES] = state.astype(bf16)
    out[:, 2 * LANES :] = edge.astype(bf16)


def scan_kernel(place, received, totals, start, out):
    layer, member = (place[4], place[5])
    members, rows = received.shape[:2]
    layers = totals.shape[0]
    here = pl.ds(pl.multiple_of(member * rows, rows), rows)
    for d in range(2):
        turn = list if d == 0 else (lambda r: list(reversed(r)))
        state = start[d, here, :]
        for n in turn(range(layers)):
            tile = totals[n]
            passed = (n < layer) if d == 0 else (n > layer)
            moved = jnp.exp(decays_of(tile)[d]) * state + updates_of(tile)[d]
            state = jnp.where(passed, moved, state)
        for n in turn(range(members)):
            out[n, :, d * LANES : (d + 1) * LANES] = state.astype(bf16)
            tile = received[n]
            state = jnp.exp(decays_of(tile)[d]) * state + updates_of(tile)[d]


def inner_kernel(qkv, logs, part_out, query_out):
    rows = qkv.shape[0]
    blocks = rows // BLOCK
    lane = lax.broadcasted_iota(jnp.int32, (BLOCK, LANES), 1)
    row = lax.broadcasted_iota(jnp.int32, (BLOCK, LANES), 0)
    head_one = lane < KEY_CHANNELS
    lower = lax.rem(lane, KEY_CHANNELS) <= row
    value_lane = lax.broadcasted_iota(jnp.int32, (BLOCK, 2 * DV), 1)
    value_one = value_lane < DV
    diagonal = (
        lax.rem(lax.broadcasted_iota(jnp.int32, (4 * KEY_CHANNELS, 2 * DV), 0), LANES)
        < KEY_CHANNELS
    ) == (lax.broadcasted_iota(jnp.int32, (4 * KEY_CHANNELS, 2 * DV), 1) < DV)
    zero = jnp.zeros((), bf16)
    scale = KEY_CHANNELS ** (-0.5)
    edges, updates, scaled, scored = [], [], [], []
    nothing = jnp.zeros((1, LANES), f32)
    for n in range(blocks):
        at = slice(n * BLOCK, (n + 1) * BLOCK)
        base_fwd = logs[0, n * BLOCK - 1 : n * BLOCK, :] if n else nothing
        base_bwd = logs[1, (n + 1) * BLOCK : (n + 1) * BLOCK + 1, :] if n + 1 < blocks else nothing
        cum_fwd = logs[0, at, :] - base_fwd
        cum_bwd = logs[1, at, :] - base_bwd
        edge_fwd = cum_fwd[BLOCK - 1 : BLOCK, :]
        edge_bwd = cum_bwd[0:1, :]
        queries = qkv[at, :LANES].astype(f32) * scale
        keys = qkv[at, LANES : 2 * LANES].astype(f32)
        values = qkv[at, 2 * LANES :]
        query_out[at, :LANES] = (queries * jnp.exp(logs[0, at, :])).astype(bf16)
        query_out[at, LANES:] = (queries * jnp.exp(logs[1, at, :])).astype(bf16)
        query_fwd = (queries * jnp.exp(cum_fwd)).astype(bf16)
        query_bwd = (queries * jnp.exp(cum_bwd)).astype(bf16)
        key_fwd = (keys * jnp.exp(-cum_fwd)).astype(bf16)
        key_bwd = (keys * jnp.exp(-cum_bwd)).astype(bf16)

        def by_head(key):
            return jnp.concatenate(
                [jnp.where(head_one, key, zero), jnp.where(head_one, zero, key)], axis=0
            )

        across = ((1,), (1,))
        scores = jnp.where(
            lower,
            matmul(query_fwd, by_head(key_fwd), across),
            matmul(query_bwd, by_head(key_bwd), across),
        ).astype(bf16)
        spread = jnp.concatenate(
            [jnp.where(value_one, values, zero), jnp.where(value_one, zero, values)], axis=0
        )
        scored.append(matmul(scores, spread))
        scaled.append(jnp.concatenate([query_fwd, query_bwd], axis=1))
        weighted = jnp.concatenate(
            [
                (keys * jnp.exp(edge_fwd - cum_fwd)).astype(bf16),
                (keys * jnp.exp(edge_bwd - cum_bwd)).astype(bf16),
            ],
            axis=1,
        )
        update = matmul(weighted, values, ((0,), (0,)))
        updates.append(jnp.where(diagonal, update, 0.0))
        edges.append((edge_fwd, edge_bwd))
    stacked = jnp.concatenate(
        [e[0] for e in edges]
        + [e[1] for e in edges]
        + [jnp.zeros((LANES - 2 * blocks, LANES), f32)],
        axis=0,
    )
    factors = jnp.exp(stacked.T)
    start_fwd, start_bwd = [None] * blocks, [None] * blocks
    memory = jnp.zeros((LANES, 2 * DV), f32)
    for n in range(blocks):
        start_fwd[n] = memory.astype(bf16)
        memory = factors[:, n : n + 1] * memory + updates[n][:LANES]
    memory = jnp.zeros((LANES, 2 * DV), f32)
    for n in reversed(range(blocks)):
        start_bwd[n] = memory.astype(bf16)
        memory = factors[:, blocks + n : blocks + n + 1] * memory + updates[n][LANES:]
    for n in range(blocks):
        entering = jnp.concatenate([start_fwd[n], start_bwd[n]], axis=0)
        part_out[n * BLOCK : (n + 1) * BLOCK, :] = scored[n] + matmul(scaled[n], entering)


def pool_kernel(place, pool_input, rim_before, rim_after, group_map, out):
    tp, here = (place[0], place[2])
    rows = out.shape[0]
    padded = rows + 2 * rim_width
    values = jnp.concatenate([rim_before[...], pool_input[...], rim_after[...]], axis=0).astype(f32)
    sums = values + pltpu.roll(values, 1, 0)
    chosen = sums
    for level in (1, 2, 3):
        step = 2 ** (level - 1)
        sums = pltpu.roll(sums, step, 0) + pltpu.roll(sums, padded - step, 0)
        chosen = jnp.where(tp >= level, sums, chosen)
    half = jnp.left_shift(1, tp)
    position = here * rows + lax.broadcasted_iota(jnp.int32, (rows, LANES), 0)
    last = place[3] * rows - 1
    low_end = jnp.maximum(position - half, 0)
    high_end = jnp.minimum(position + half - 1, last)
    counted = (high_end - low_end + 1).astype(f32)[:, 0:1]
    inside = slice(rim_width, rim_width + rows)
    pooled = (chosen[inside] / counted - values[inside]).astype(bf16)
    out[...] = matmul(pooled, group_map[tp]).astype(bf16)


def finish_kernel(part, query, entering, pooled, out):
    channel_one = lax.broadcasted_iota(jnp.int32, (LANES, DV), 0) < KEY_CHANNELS
    zero = jnp.zeros((), bf16)
    sides = []
    for d in range(2):
        state = entering[:, d * LANES : (d + 1) * LANES]
        sides.append(
            jnp.concatenate(
                [jnp.where(channel_one, state, zero), jnp.where(channel_one, zero, state)], axis=1
            )
        )
    joined = part[...] + matmul(query[...], jnp.concatenate(sides, axis=0))
    rows = joined.shape[0]
    ready = [pooled[...]]
    for h in range(2):
        mine = joined[:, h * DV : (h + 1) * DV]
        scale = lax.rsqrt(jnp.mean(mine * mine, axis=1, keepdims=True) + eps_value)
        ready.append((mine * scale).astype(bf16))
    owners = out.shape[0]
    for j in range(owners):
        at = slice(j * rows // owners, (j + 1) * rows // owners)
        start = 0
        for piece in ready:
            out[j, :, start : start + piece.shape[1]] = piece[at]
            start += piece.shape[1]


def output_kernel(place, weights, activations, out, weight_ref, sems):
    groups, _, width = activations.shape
    pieces = sems.shape[0]
    tile = weights.shape[0] // pieces
    loads = []
    for n in range(pieces):
        here = slice(n * tile, (n + 1) * tile)
        loads.append(pltpu.make_async_copy(weights.at[here], weight_ref.at[here], sems.at[n]))
        loads[n].start()
    mine = [activations[lax.rem(place[0] + groups - s, groups)] for s in range(groups)]
    for n in range(pieces):
        here = slice(n * tile, (n + 1) * tile)
        loads[n].wait()
        total = None
        for s in range(groups):
            block = weight_ref[here, s * width : (s + 1) * width]
            partial = matmul(mine[s], block, ((1,), (1,))).astype(bf16).astype(f32)
            total = partial if total is None else total + partial
        out[:, here] = total.astype(bf16)


def output_projection(place, activations, weights):
    groups, rows, width = activations.shape
    model = weights.shape[0]
    pieces = 8
    return call(
        output_kernel,
        shape_of(rows, model),
        (place, weights, activations),
        far=1,
        scratch=(pltpu.VMEM((model, groups * width), bf16), pltpu.SemaphoreType.DMA((pieces,))),
        flops=2 * rows * model * groups * width,
        moved=2 * model * groups * width,
    )


def shape_of(*lengths, kind=bf16):
    return jax.ShapeDtypeStruct(lengths, kind)


def shards(
    tokens,
    pooling_input_weight,
    query_matrix,
    key_matrix,
    value_matrix,
    decay_inner_weight,
    decay_outer_weight,
    channel_decay_bias,
    spike_log_decay,
    starting_state,
    pooling_group_map,
    pooling_output_weight,
    attention_output_weight,
):
    sp_index = lax.axis_index(SP)
    tp_index = lax.axis_index("tp")
    core = lax.axis_index("sp_2")
    positions = lax.axis_size(SP)
    layer, member = (lax.axis_index("sp_0"), lax.axis_index(GROUP))
    layers, members = (lax.axis_size("sp_0"), lax.axis_size(GROUP))
    place = jnp.stack([tp_index, core, sp_index, jnp.int32(positions), layer, member])
    place = place.astype(jnp.int32)
    groups = lax.axis_size("tp")
    rows = tokens.shape[0] * groups
    model = tokens.shape[1]

    local_in = jnp.concatenate(
        [query_matrix, key_matrix, value_matrix, pooling_input_weight], axis=1
    )
    chips = lax.axis_size(CHIPS)
    copies = jnp.broadcast_to(local_in, (chips, *local_in.shape))
    weight_own = lax.all_to_all(copies, CHIPS, 0, 0, tiled=True)
    local_out = jnp.concatenate([pooling_output_weight, attention_output_weight], axis=0).T
    outs = [local_out] + [shifted(local_out, "tp", k) for k in range(1, groups)]
    normed = normalize(tokens)
    half = normed.shape[0] // 2
    before = shifted(normed, "tp", 1)
    after = shifted(normed, "tp", -1)
    top, end = (before[:half], after[half:])
    far_top = shifted(top, "tp", 1)
    far_end = shifted(end, "tp", -1)
    weight_other = shifted(weight_own, "sp_2", 1)
    whole_out = lax.all_gather(jnp.concatenate(outs, axis=1), SP, axis=0, tiled=True)

    all_tokens, logs = call(
        decay_kernel,
        (shape_of(rows, model), shape_of(2, rows, LANES, kind=f32)),
        (
            place,
            normed,
            before,
            after,
            far_top,
            far_end,
            decay_inner_weight.T,
            decay_outer_weight,
            channel_decay_bias,
            spike_log_decay,
        ),
        flops=2 * rows * model * 4 * LANES,
        moved=5_000_000,
    )
    qkv, pool_input, packed = call(
        project_kernel,
        (
            shape_of(rows, 4 * LANES),
            shape_of(rows, 2 * LANES),
            shape_of(LANES, 3 * LANES),
        ),
        (place, weight_own, weight_other, all_tokens, logs),
        far=3,
        scratch=(
            pltpu.VMEM((rows, model), bf16),
            pltpu.VMEM((chips, 2, model // (2 * chips), 6 * LANES), bf16),
            pltpu.SemaphoreType.DMA((3,)),
        ),
        flops=2 * rows * model * 7 * LANES,
        moved=8_000_000,
    )
    packed = packed.reshape(members, LANES // members, 3 * LANES)
    received = lax.all_to_all(packed, GROUP, 0, 0, tiled=True)
    totals = call(
        total_kernel, shape_of(*packed.shape[1:]), (received,), scalars=0, flops=1_000_000
    )
    copies = jnp.broadcast_to(totals, (layers, *totals.shape))
    totals = lax.all_to_all(copies, "sp_0", 0, 0, tiled=True)
    states = call(
        scan_kernel,
        shape_of(members, LANES // members, 2 * LANES),
        (place, received, totals, starting_state.reshape(2, -1, DV)),
        flops=1_000_000,
    )
    entering = lax.all_to_all(states, GROUP, 0, 0, tiled=True).reshape(LANES, 2 * LANES)
    last, leading = (pool_input[rows - rim_width :], pool_input[:rim_width])
    rim_before = neighbours(last, SP, 1)
    rim_after = neighbours(leading, SP, -1)
    part, query = call(
        inner_kernel,
        (shape_of(rows, 2 * DV, kind=f32), shape_of(rows, 2 * LANES)),
        (qkv, logs),
        scalars=0,
        flops=2 * rows * model * 2 * LANES,
        moved=3_000_000,
    )
    pooled = call(
        pool_kernel,
        shape_of(rows, 2 * LANES),
        (place, pool_input, rim_before, rim_after, pooling_group_map),
        flops=2 * rows * 4 * LANES * LANES,
        moved=1_000_000,
    )
    activations = call(
        finish_kernel,
        shape_of(groups, rows // groups, 4 * LANES),
        (part, query, entering, pooled),
        scalars=0,
        flops=100_000_000,
        moved=2_000_000,
    )
    gathered = lax.all_to_all(activations, "tp", 0, 0, tiled=True)
    return output_projection(place, gathered, whole_out)


def solution(mesh):
    split = Mesh(mesh.devices.reshape(8, 8, 2, mesh.shape["tp"]), ("sp_0", "sp_1", "sp_2", "tp"))
    in_specs = (
        P(SP_TP, None),
        P(SP, "tp"),
        P(SP, "tp"),
        P(SP, "tp"),
        P(SP, "tp"),
        P(),
        P(),
        P(),
        P("tp", SP),
        P(None, "tp", None, None),
        P(),
        P("tp", SP),
        P("tp", SP),
    )
    out_specs = P(SP_TP, None)
    return jax.shard_map(
        shards, mesh=split, in_specs=in_specs, out_specs=out_specs, check_vma=False
    )
```

```python
import jax
import jax.numpy as jnp
from jax import lax
from jax.experimental import pallas as pl
from jax.experimental.pallas import tpu as pltpu
from jax.sharding import Mesh
from jax.sharding import PartitionSpec as P


KEY_CHANNELS = 64
DV = 128
RANK = 32
BLOCK = 64
LANES = 128
SP = ("sp_0", "sp_1", "sp_2")
CHIPS = ("sp_0", "sp_1")
SP_TP = ("sp_0", "sp_1", "sp_2", "tp")

eps_value = 1e-06
gate_norm_factor = 16.0
rim_width = 8
interpreted = False

bf16 = jnp.bfloat16
f32 = jnp.float32
exact = lax.Precision.HIGHEST


def matmul(a, b, dims=((1,), (0,)), precision=None):
    return lax.dot_general(a, b, (dims, ((), ())), precision=precision, preferred_element_type=f32)


def call(kernel, out_shapes, operands, scalars=1, far=0, scratch=(), flops=0, moved=0):
    smem = pl.BlockSpec(memory_space=pltpu.SMEM)
    vmem = pl.BlockSpec(memory_space=pltpu.VMEM)
    anywhere = pl.BlockSpec(memory_space=pl.ANY)
    near = len(operands) - scalars - far
    return pl.pallas_call(
        kernel,
        in_specs=[smem] * scalars + [anywhere] * far + [vmem] * near,
        out_specs=jax.tree.map(lambda _: vmem, out_shapes),
        out_shape=out_shapes,
        scratch_shapes=list(scratch),
        cost_estimate=pl.CostEstimate(flops=flops, bytes_accessed=moved, transcendentals=0),
        interpret=interpreted,
    )(*operands)


def shifted(value, axis, step):
    devices = lax.axis_size(axis)
    return lax.ppermute(value, axis, [(i, (i + step) % devices) for i in range(devices)])


def neighbours(value, axes, step):
    devices = lax.axis_size(axes)
    pairs = [(i, i + step) for i in range(devices) if 0 <= i + step < devices]
    return lax.ppermute(value, axes, pairs)


def normalize(token_rows):
    floats = token_rows.astype(f32)
    scaled = floats * lax.rsqrt(jnp.mean(floats * floats, axis=-1, keepdims=True) + eps_value)
    return scaled.astype(bf16)


def place_tokens(tp, pieces, whole_ref, first):
    own, before, after, far_top, far_end = pieces
    rows = own.shape[0]
    half = rows // 2

    def at(step):
        return pl.multiple_of(first + lax.rem(tp + step, 4) * rows, 8)

    whole_ref[pl.ds(at(0), rows), :] = own[...]
    whole_ref[pl.ds(at(3), rows), :] = before[...]
    whole_ref[pl.ds(at(1), rows), :] = after[...]
    far = at(2)
    whole_ref[pl.ds(far, half), :] = far_top[...]
    whole_ref[pl.ds(pl.multiple_of(far + half, 8), half), :] = far_end[...]


def split_dot(ones, values):
    high = values.astype(bf16)
    low = (values - high.astype(f32)).astype(bf16)
    return matmul(ones, high) + matmul(ones, low)


def project_kernel(
    place,
    own,
    before,
    after,
    far_top,
    far_end,
    weight_own,
    weight_other,
    inner,
    outer,
    bias,
    spike,
    qkv_out,
    pool_out,
    logs_out,
    packed_out,
    tokens_ref,
    weight_ref,
):
    tp, core = (place[0], place[1])
    place_tokens(tp, (own, before, after, far_top, far_end), tokens_ref, 0)
    weight_ref[:, pl.ds(core, 1)] = weight_own[...][:, None]
    weight_ref[:, pl.ds(1 - core, 1)] = weight_other[...][:, None]
    rows, width = tokens_ref.shape
    tokens = tokens_ref[...]
    low_rank = matmul(tokens, inner[...]).astype(bf16)
    projected = matmul(tokens, weight_ref[...].reshape(width, -1)).astype(bf16)
    qkv = projected[:, : 4 * LANES]
    qkv_out[...] = qkv
    pool_out[...] = projected[:, 4 * LANES :]
    here = pl.ds(pl.multiple_of(tp * LANES, LANES), LANES)
    blank = jnp.zeros((RANK, LANES), bf16)
    outer_both = jnp.concatenate(
        [
            jnp.concatenate([outer[0, :, here], blank], axis=1),
            jnp.concatenate([blank, outer[1, :, here]], axis=1),
        ],
        axis=0,
    )
    bias_both = jnp.concatenate([bias[0:1, here], bias[1:2, here]], axis=1)
    pre = matmul(low_rank, outer_both) + bias_both
    gate = jnp.minimum(pre, 0.0) - jnp.log1p(jnp.exp(-jnp.abs(pre)))
    lane = lax.broadcasted_iota(jnp.int32, (rows, LANES), 1)
    spikes = jnp.where(lane < KEY_CHANNELS, spike[:, 0:1], spike[:, 1:2])
    decay = gate * (1.0 / gate_norm_factor) + jnp.concatenate([spikes, spikes], axis=1)
    size = LANES
    row_ids = lax.broadcasted_iota(jnp.int32, (size, size), 0)
    col_ids = lax.broadcasted_iota(jnp.int32, (size, size), 1)
    upto = (col_ids <= row_ids).astype(bf16)
    onward = (col_ids >= row_ids).astype(bf16)
    tiles = rows // size
    carry = jnp.zeros((1, LANES), f32)
    for n in range(tiles):
        found = split_dot(upto, decay[n * size : (n + 1) * size, :LANES]) + carry
        logs_out[0, n * size : (n + 1) * size, :] = found
        carry = found[size - 1 : size, :]
    total_fwd = carry
    carry = jnp.zeros((1, LANES), f32)
    for n in reversed(range(tiles)):
        found = split_dot(onward, decay[n * size : (n + 1) * size, LANES:]) + carry
        logs_out[1, n * size : (n + 1) * size, :] = found
        carry = found[0:1, :]
    total_bwd = carry
    keys = qkv[:, LANES : 2 * LANES].astype(f32)
    weighted = jnp.concatenate(
        [
            (keys * jnp.exp(total_fwd - logs_out[0])).astype(bf16),
            (keys * jnp.exp(total_bwd - logs_out[1])).astype(bf16),
        ],
        axis=1,
    )
    updates = matmul(weighted, qkv[:, 2 * LANES :], ((0,), (0,)))
    first = lax.broadcasted_iota(jnp.int32, (LANES, LANES), 0) < KEY_CHANNELS
    for d in range(2):
        mine = updates[d * LANES : (d + 1) * LANES]
        packed_out[:, 0, d * LANES : (d + 1) * LANES] = jnp.where(
            first, mine[:, :LANES], mine[:, LANES:]
        )
    totals = jnp.concatenate([total_fwd, total_bwd], axis=0)
    stacked = jnp.concatenate([totals, jnp.zeros((LANES - 2, LANES), f32)], axis=0)
    packed_out[:, 0, 2 * LANES :] = stacked.T


def scan_kernel(place, received, start, out):
    devices = received.shape[0]
    here = place[0]
    logs = received[:, 0, 2 * LANES :]
    row = lax.broadcasted_iota(jnp.int32, (devices, devices), 0)
    col = lax.broadcasted_iota(jnp.int32, (devices, devices), 1)
    earlier = (col < row).astype(f32)
    upto = (row <= col).astype(f32)
    strictly = (row < col).astype(f32)
    before_col = matmul(earlier, logs, precision=exact)
    before_row = matmul(logs, strictly, ((0,), (0,)), precision=exact)
    past_row = matmul(logs, upto, ((0,), (0,)), precision=exact)
    past_col = before_col + logs
    total = jnp.sum(logs, axis=0, keepdims=True)
    for r in range(2):
        if r == 0:
            between = before_col[:, 0:1] - past_row[0:1, :]
            allowed = col < row
            outside = before_col[:, 0:1]
        else:
            between = before_row[1:2, :] - past_col[:, 1:2]
            allowed = col > row
            outside = total[:, 1:2] - past_col[:, 1:2]
        weights = jnp.where(allowed, jnp.exp(jnp.minimum(between, 0.0)), 0.0)
        high = weights.astype(bf16)
        low = (weights - high.astype(f32)).astype(bf16)
        updates = received[:, 0, r * LANES : (r + 1) * LANES].astype(bf16)
        first = start[r, pl.ds(here, 1), :]
        entering = matmul(high, updates) + matmul(low, updates)
        entering = entering + jnp.exp(jnp.minimum(outside, 0.0)) * first
        out[:, 0, r * LANES : (r + 1) * LANES] = entering


def inner_kernel(qkv, logs, part_out, query_out):
    rows = qkv.shape[0]
    blocks = rows // BLOCK
    lane = lax.broadcasted_iota(jnp.int32, (BLOCK, LANES), 1)
    row = lax.broadcasted_iota(jnp.int32, (BLOCK, LANES), 0)
    head_one = lane < KEY_CHANNELS
    lower = lax.rem(lane, KEY_CHANNELS) <= row
    value_lane = lax.broadcasted_iota(jnp.int32, (BLOCK, 2 * DV), 1)
    value_one = value_lane < DV
    diagonal = (
        lax.rem(lax.broadcasted_iota(jnp.int32, (4 * KEY_CHANNELS, 2 * DV), 0), LANES)
        < KEY_CHANNELS
    ) == (lax.broadcasted_iota(jnp.int32, (4 * KEY_CHANNELS, 2 * DV), 1) < DV)
    zero = jnp.zeros((), bf16)
    scale = KEY_CHANNELS ** (-0.5)
    edges, updates, scaled, scored = [], [], [], []
    nothing = jnp.zeros((1, LANES), f32)
    for n in range(blocks):
        at = slice(n * BLOCK, (n + 1) * BLOCK)
        base_fwd = logs[0, n * BLOCK - 1 : n * BLOCK, :] if n else nothing
        base_bwd = logs[1, (n + 1) * BLOCK : (n + 1) * BLOCK + 1, :] if n + 1 < blocks else nothing
        cum_fwd = logs[0, at, :] - base_fwd
        cum_bwd = logs[1, at, :] - base_bwd
        edge_fwd = cum_fwd[BLOCK - 1 : BLOCK, :]
        edge_bwd = cum_bwd[0:1, :]
        queries = qkv[at, :LANES].astype(f32) * scale
        keys = qkv[at, LANES : 2 * LANES].astype(f32)
        values = qkv[at, 2 * LANES :]
        query_out[at, :LANES] = (queries * jnp.exp(logs[0, at, :])).astype(bf16)
        query_out[at, LANES:] = (queries * jnp.exp(logs[1, at, :])).astype(bf16)
        query_fwd = (queries * jnp.exp(cum_fwd)).astype(bf16)
        query_bwd = (queries * jnp.exp(cum_bwd)).astype(bf16)
        key_fwd = (keys * jnp.exp(-cum_fwd)).astype(bf16)
        key_bwd = (keys * jnp.exp(-cum_bwd)).astype(bf16)

        def by_head(key):
            return jnp.concatenate(
                [jnp.where(head_one, key, zero), jnp.where(head_one, zero, key)], axis=0
            )

        across = ((1,), (1,))
        scores = jnp.where(
            lower,
            matmul(query_fwd, by_head(key_fwd), across),
            matmul(query_bwd, by_head(key_bwd), across),
        ).astype(bf16)
        spread = jnp.concatenate(
            [jnp.where(value_one, values, zero), jnp.where(value_one, zero, values)], axis=0
        )
        scored.append(matmul(scores, spread))
        scaled.append(jnp.concatenate([query_fwd, query_bwd], axis=1))
        weighted = jnp.concatenate(
            [
                (keys * jnp.exp(edge_fwd - cum_fwd)).astype(bf16),
                (keys * jnp.exp(edge_bwd - cum_bwd)).astype(bf16),
            ],
            axis=1,
        )
        update = matmul(weighted, values, ((0,), (0,)))
        updates.append(jnp.where(diagonal, update, 0.0))
        edges.append((edge_fwd, edge_bwd))
    stacked = jnp.concatenate(
        [e[0] for e in edges]
        + [e[1] for e in edges]
        + [jnp.zeros((LANES - 2 * blocks, LANES), f32)],
        axis=0,
    )
    factors = jnp.exp(stacked.T)
    start_fwd, start_bwd = [None] * blocks, [None] * blocks
    memory = jnp.zeros((LANES, 2 * DV), f32)
    for n in range(blocks):
        start_fwd[n] = memory.astype(bf16)
        memory = factors[:, n : n + 1] * memory + updates[n][:LANES]
    memory = jnp.zeros((LANES, 2 * DV), f32)
    for n in reversed(range(blocks)):
        start_bwd[n] = memory.astype(bf16)
        memory = factors[:, blocks + n : blocks + n + 1] * memory + updates[n][LANES:]
    for n in range(blocks):
        entering = jnp.concatenate([start_fwd[n], start_bwd[n]], axis=0)
        part_out[n * BLOCK : (n + 1) * BLOCK, :] = scored[n] + matmul(scaled[n], entering)


def pool_kernel(place, pool_input, rim_before, rim_after, group_map, out):
    tp, here = (place[0], place[2])
    rows = out.shape[0]
    padded = rows + 2 * rim_width
    values = jnp.concatenate([rim_before[...], pool_input[...], rim_after[...]], axis=0).astype(f32)
    sums = values + pltpu.roll(values, 1, 0)
    chosen = sums
    for level in (1, 2, 3):
        step = 2 ** (level - 1)
        sums = pltpu.roll(sums, step, 0) + pltpu.roll(sums, padded - step, 0)
        chosen = jnp.where(tp >= level, sums, chosen)
    half = jnp.left_shift(1, tp)
    position = here * rows + lax.broadcasted_iota(jnp.int32, (rows, LANES), 0)
    last = place[3] * rows - 1
    low_end = jnp.maximum(position - half, 0)
    high_end = jnp.minimum(position + half - 1, last)
    counted = (high_end - low_end + 1).astype(f32)[:, 0:1]
    inside = slice(rim_width, rim_width + rows)
    pooled = (chosen[inside] / counted - values[inside]).astype(bf16)
    out[...] = matmul(pooled, group_map[tp]).astype(bf16)


def finish_kernel(place, part, query, entering, pooled, *outs_and_scratch):
    *outs, ready = outs_and_scratch
    channel_one = lax.broadcasted_iota(jnp.int32, (LANES, DV), 0) < KEY_CHANNELS
    zero = jnp.zeros((), bf16)
    sides = []
    for d in range(2):
        state = entering[:, 0, d * LANES : (d + 1) * LANES].astype(bf16)
        sides.append(
            jnp.concatenate(
                [jnp.where(channel_one, state, zero), jnp.where(channel_one, zero, state)], axis=1
            )
        )
    joined = part[...] + matmul(query[...], jnp.concatenate(sides, axis=0))
    rows = joined.shape[0]
    width = pooled.shape[1]
    ready[:, :width] = pooled[...]
    for h in range(2):
        mine = joined[:, h * DV : (h + 1) * DV]
        scale = lax.rsqrt(jnp.mean(mine * mine, axis=1, keepdims=True) + eps_value)
        ready[:, width + h * DV : width + (h + 1) * DV] = (mine * scale).astype(bf16)
    owners = len(outs)
    share = rows // owners
    for step, out in enumerate(outs):
        first = pl.multiple_of(lax.rem(place[0] + step, owners) * share, share)
        out[...] = ready[pl.ds(first, share), :]


def start_loads(weights, start, weight_ref, sems):
    pieces = sems.shape[0]
    tile = weights.shape[0] // pieces
    columns = slice(start, start + weight_ref.shape[1])
    loads = []
    for n in range(pieces):
        here = slice(n * tile, (n + 1) * tile)
        load = pltpu.make_async_copy(weights.at[here, columns], weight_ref.at[here], sems.at[n])
        load.start()
        loads.append((here, load))
    return loads


def own_kernel(weights, mine, out, weight_ref, sems):
    for here, load in start_loads(weights, 0, weight_ref, sems):
        load.wait()
        out[:, here] = matmul(mine[...], weight_ref[here, :], ((1,), (1,))).astype(bf16)


def output_kernel(weights, own_part, *rest):
    *others, out, weight_ref, sems = rest
    width = others[0].shape[1]
    for here, load in start_loads(weights, width, weight_ref, sems):
        load.wait()
        total = own_part[:, here].astype(f32)
        for s, other in enumerate(others):
            block = weight_ref[here, s * width : (s + 1) * width]
            total = total + matmul(other[...], block, ((1,), (1,))).astype(bf16).astype(f32)
        out[:, here] = total.astype(bf16)


def shape_of(*lengths, kind=bf16):
    return jax.ShapeDtypeStruct(lengths, kind)


def shards(
    tokens,
    pooling_input_weight,
    query_matrix,
    key_matrix,
    value_matrix,
    decay_inner_weight,
    decay_outer_weight,
    channel_decay_bias,
    spike_log_decay,
    starting_state,
    pooling_group_map,
    pooling_output_weight,
    attention_output_weight,
):
    sp_index = lax.axis_index(SP)
    tp_index = lax.axis_index("tp")
    core = lax.axis_index("sp_2")
    positions = lax.axis_size(SP)
    place = jnp.stack([tp_index, core, sp_index, jnp.int32(positions)]).astype(jnp.int32)
    groups = lax.axis_size("tp")
    rows = tokens.shape[0] * groups
    model = tokens.shape[1]

    local_in = jnp.concatenate(
        [query_matrix, key_matrix, value_matrix, pooling_input_weight], axis=1
    )
    chips = lax.axis_size(CHIPS)
    copies = jnp.broadcast_to(local_in, (chips, *local_in.shape))
    weight_own = lax.all_to_all(copies, CHIPS, 0, 0, tiled=True)
    local_out = jnp.concatenate([pooling_output_weight, attention_output_weight], axis=0).T
    outs = [local_out] + [shifted(local_out, "tp", k) for k in range(1, groups)]
    normed = normalize(tokens)
    half = normed.shape[0] // 2
    before = shifted(normed, "tp", 1)
    after = shifted(normed, "tp", -1)
    top, end = (before[:half], after[half:])
    far_top = shifted(top, "tp", 1)
    far_end = shifted(end, "tp", -1)
    weight_other = shifted(weight_own, "sp_2", 1)
    whole_out = lax.all_gather(jnp.concatenate(outs, axis=1), SP, axis=0, tiled=True)

    qkv, pool_input, logs, packed = call(
        project_kernel,
        (
            shape_of(rows, 4 * LANES),
            shape_of(rows, 2 * LANES),
            shape_of(2, rows, LANES, kind=f32),
            shape_of(LANES, 1, 3 * LANES, kind=f32),
        ),
        (
            place,
            normed,
            before,
            after,
            far_top,
            far_end,
            weight_own,
            weight_other,
            decay_inner_weight,
            decay_outer_weight,
            channel_decay_bias,
            spike_log_decay.T,
        ),
        scratch=(
            pltpu.VMEM((rows, model), bf16),
            pltpu.VMEM((chips, 2, model // (2 * chips), 6 * LANES), bf16),
        ),
        flops=2 * rows * model * 7 * LANES,
        moved=10_000_000,
    )
    received = lax.all_to_all(packed, SP, 0, 0, tiled=True)
    rim_before = neighbours(pool_input[rows - rim_width :], SP, 1)
    rim_after = neighbours(pool_input[:rim_width], SP, -1)
    part, query = call(
        inner_kernel,
        (shape_of(rows, 2 * DV, kind=f32), shape_of(rows, 2 * LANES)),
        (qkv, logs),
        scalars=0,
        flops=2 * rows * model * 2 * LANES,
        moved=3_000_000,
    )
    states = call(
        scan_kernel,
        shape_of(positions, 1, 2 * LANES, kind=f32),
        (place[2:3], received, starting_state.reshape(2, -1, DV)),
        flops=40_000_000,
    )
    entering = lax.all_to_all(states, SP, 0, 0, tiled=True)
    pooled = call(
        pool_kernel,
        shape_of(rows, 2 * LANES),
        (place, pool_input, rim_before, rim_after, pooling_group_map),
        flops=2 * rows * 4 * LANES * LANES,
        moved=1_000_000,
    )
    share = rows // groups
    width = 4 * LANES
    mine, for_next, for_far, for_last = call(
        finish_kernel,
        (shape_of(share, width),) * groups,
        (place, part, query, entering, pooled),
        scratch=(pltpu.VMEM((rows, width), bf16),),
        flops=100_000_000,
        moved=2_000_000,
    )
    first = shifted(for_next, "tp", 1)
    third = shifted(for_last, "tp", -1)
    second = shifted(for_far, "tp", 2)
    own_part = call(
        own_kernel,
        shape_of(share, model),
        (whole_out, mine),
        scalars=0,
        far=1,
        scratch=(pltpu.VMEM((model, width), bf16), pltpu.SemaphoreType.DMA((4,))),
        flops=2 * share * model * width,
        moved=2 * model * width,
    )
    return call(
        output_kernel,
        shape_of(share, model),
        (whole_out, own_part, first, second, third),
        scalars=0,
        far=1,
        scratch=(
            pltpu.VMEM((model, (groups - 1) * width), bf16),
            pltpu.SemaphoreType.DMA((8,)),
        ),
        flops=2 * share * model * (groups - 1) * width,
        moved=2 * model * (groups - 1) * width,
    )


def solution(mesh):
    split = Mesh(mesh.devices.reshape(8, 8, 2, mesh.shape["tp"]), ("sp_0", "sp_1", "sp_2", "tp"))
    in_specs = (
        P(SP_TP, None),
        P(SP, "tp"),
        P(SP, "tp"),
        P(SP, "tp"),
        P(SP, "tp"),
        P(),
        P(),
        P(),
        P("tp", SP),
        P(None, "tp", None, None),
        P(),
        P("tp", SP),
        P("tp", SP),
    )
    out_specs = P(SP_TP, None)
    return jax.shard_map(
        shards, mesh=split, in_specs=in_specs, out_specs=out_specs, check_vma=False
    )
```

```python
import jax
import jax.numpy as jnp
from jax import lax
from jax.experimental import pallas as pl
from jax.experimental.pallas import tpu as pltpu
from jax.sharding import Mesh
from jax.sharding import PartitionSpec as P


KEY_CHANNELS = 64
DV = 128
RANK = 32
BLOCK = 64
LANES = 128
SP = ("sp_0", "sp_1", "sp_2")
CHIPS = ("sp_0", "sp_1")
SP_TP = ("sp_0", "sp_1", "sp_2", "tp")

eps_value = 1e-06
gate_norm_factor = 16.0
rim_width = 8
interpreted = False

bf16 = jnp.bfloat16
f32 = jnp.float32
exact = lax.Precision.HIGHEST


def matmul(a, b, dims=((1,), (0,)), precision=None):
    return lax.dot_general(a, b, (dims, ((), ())), precision=precision, preferred_element_type=f32)


def call(kernel, out_shapes, operands, scalars=1, far=0, scratch=(), flops=0, moved=0):
    smem = pl.BlockSpec(memory_space=pltpu.SMEM)
    vmem = pl.BlockSpec(memory_space=pltpu.VMEM)
    anywhere = pl.BlockSpec(memory_space=pl.ANY)
    near = len(operands) - scalars - far
    return pl.pallas_call(
        kernel,
        in_specs=[smem] * scalars + [anywhere] * far + [vmem] * near,
        out_specs=jax.tree.map(lambda _: vmem, out_shapes),
        out_shape=out_shapes,
        scratch_shapes=list(scratch),
        cost_estimate=pl.CostEstimate(flops=flops, bytes_accessed=moved, transcendentals=0),
        interpret=interpreted,
    )(*operands)


def shifted(value, axis, step):
    devices = lax.axis_size(axis)
    return lax.ppermute(value, axis, [(i, (i + step) % devices) for i in range(devices)])


def neighbours(value, axes, step):
    devices = lax.axis_size(axes)
    pairs = [(i, i + step) for i in range(devices) if 0 <= i + step < devices]
    return lax.ppermute(value, axes, pairs)


def normalize(token_rows):
    floats = token_rows.astype(f32)
    scaled = floats * lax.rsqrt(jnp.mean(floats * floats, axis=-1, keepdims=True) + eps_value)
    return scaled.astype(bf16)


def place_tokens(tp, pieces, whole_ref, first):
    own, before, after, far_top, far_end = pieces
    rows = own.shape[0]
    half = rows // 2

    def at(step):
        return pl.multiple_of(first + lax.rem(tp + step, 4) * rows, 8)

    whole_ref[pl.ds(at(0), rows), :] = own[...]
    whole_ref[pl.ds(at(3), rows), :] = before[...]
    whole_ref[pl.ds(at(1), rows), :] = after[...]
    far = at(2)
    whole_ref[pl.ds(far, half), :] = far_top[...]
    whole_ref[pl.ds(pl.multiple_of(far + half, 8), half), :] = far_end[...]


def split_dot(ones, values):
    high = values.astype(bf16)
    low = (values - high.astype(f32)).astype(bf16)
    return matmul(ones, high) + matmul(ones, low)


def project_kernel(
    place,
    own,
    before,
    after,
    far_top,
    far_end,
    weight_own,
    weight_other,
    inner,
    outer,
    bias,
    spike,
    qkv_out,
    pool_out,
    logs_out,
    packed_out,
    tokens_ref,
    weight_ref,
):
    tp, core = (place[0], place[1])
    place_tokens(tp, (own, before, after, far_top, far_end), tokens_ref, 0)
    weight_ref[:, pl.ds(core, 1)] = weight_own[...][:, None]
    weight_ref[:, pl.ds(1 - core, 1)] = weight_other[...][:, None]
    rows, width = tokens_ref.shape
    tokens = tokens_ref[...]
    low_rank = matmul(tokens, inner[...]).astype(bf16)
    projected = matmul(tokens, weight_ref[...].reshape(width, -1)).astype(bf16)
    qkv = projected[:, : 4 * LANES]
    qkv_out[...] = qkv
    pool_out[...] = projected[:, 4 * LANES :]
    here = pl.ds(pl.multiple_of(tp * LANES, LANES), LANES)
    blank = jnp.zeros((RANK, LANES), bf16)
    outer_both = jnp.concatenate(
        [
            jnp.concatenate([outer[0, :, here], blank], axis=1),
            jnp.concatenate([blank, outer[1, :, here]], axis=1),
        ],
        axis=0,
    )
    bias_both = jnp.concatenate([bias[0:1, here], bias[1:2, here]], axis=1)
    pre = matmul(low_rank, outer_both) + bias_both
    gate = jnp.minimum(pre, 0.0) - jnp.log1p(jnp.exp(-jnp.abs(pre)))
    lane = lax.broadcasted_iota(jnp.int32, (rows, LANES), 1)
    spikes = jnp.where(lane < KEY_CHANNELS, spike[:, 0:1], spike[:, 1:2])
    decay = gate * (1.0 / gate_norm_factor) + jnp.concatenate([spikes, spikes], axis=1)
    size = LANES
    row_ids = lax.broadcasted_iota(jnp.int32, (size, size), 0)
    col_ids = lax.broadcasted_iota(jnp.int32, (size, size), 1)
    upto = (col_ids <= row_ids).astype(bf16)
    onward = (col_ids >= row_ids).astype(bf16)
    tiles = rows // size
    carry = jnp.zeros((1, LANES), f32)
    for n in range(tiles):
        found = split_dot(upto, decay[n * size : (n + 1) * size, :LANES]) + carry
        logs_out[0, n * size : (n + 1) * size, :] = found
        carry = found[size - 1 : size, :]
    total_fwd = carry
    carry = jnp.zeros((1, LANES), f32)
    for n in reversed(range(tiles)):
        found = split_dot(onward, decay[n * size : (n + 1) * size, LANES:]) + carry
        logs_out[1, n * size : (n + 1) * size, :] = found
        carry = found[0:1, :]
    total_bwd = carry
    keys = qkv[:, LANES : 2 * LANES].astype(f32)
    weighted = jnp.concatenate(
        [
            (keys * jnp.exp(total_fwd - logs_out[0])).astype(bf16),
            (keys * jnp.exp(total_bwd - logs_out[1])).astype(bf16),
        ],
        axis=1,
    )
    updates = matmul(weighted, qkv[:, 2 * LANES :], ((0,), (0,)))
    first = lax.broadcasted_iota(jnp.int32, (LANES, LANES), 0) < KEY_CHANNELS
    for d in range(2):
        mine = updates[d * LANES : (d + 1) * LANES]
        packed_out[:, d, :] = jnp.where(first, mine[:, :LANES], mine[:, LANES:]).astype(bf16)
    totals = jnp.concatenate([total_fwd, total_bwd], axis=0)
    high = totals.astype(bf16).astype(f32)
    stacked = jnp.concatenate([high, totals - high, jnp.zeros((LANES - 4, LANES), f32)], axis=0)
    packed_out[:, 2, :] = stacked.T.astype(bf16)


def scan_kernel(place, received, start, out):
    devices = received.shape[0]
    here = place[0]
    parts = received[:, 2, :].astype(f32)
    logs = parts + pltpu.roll(parts, LANES - 2, 1)
    row = lax.broadcasted_iota(jnp.int32, (devices, devices), 0)
    col = lax.broadcasted_iota(jnp.int32, (devices, devices), 1)
    earlier = (col < row).astype(f32)
    upto = (row <= col).astype(f32)
    strictly = (row < col).astype(f32)
    before_col = matmul(earlier, logs, precision=exact)
    before_row = matmul(logs, strictly, ((0,), (0,)), precision=exact)
    past_row = matmul(logs, upto, ((0,), (0,)), precision=exact)
    past_col = before_col + logs
    total = jnp.sum(logs, axis=0, keepdims=True)
    for r in range(2):
        if r == 0:
            between = before_col[:, 0:1] - past_row[0:1, :]
            allowed = col < row
            outside = before_col[:, 0:1]
        else:
            between = before_row[1:2, :] - past_col[:, 1:2]
            allowed = col > row
            outside = total[:, 1:2] - past_col[:, 1:2]
        weights = jnp.where(allowed, jnp.exp(jnp.minimum(between, 0.0)), 0.0)
        high = weights.astype(bf16)
        low = (weights - high.astype(f32)).astype(bf16)
        updates = received[:, r, :]
        first = start[r, pl.ds(here, 1), :]
        entering = matmul(high, updates) + matmul(low, updates)
        entering = entering + jnp.exp(jnp.minimum(outside, 0.0)) * first
        out[:, r, :] = entering.astype(bf16)


def inner_kernel(qkv, logs, part_out, query_out):
    rows = qkv.shape[0]
    blocks = rows // BLOCK
    lane = lax.broadcasted_iota(jnp.int32, (BLOCK, LANES), 1)
    row = lax.broadcasted_iota(jnp.int32, (BLOCK, LANES), 0)
    head_one = lane < KEY_CHANNELS
    lower = lax.rem(lane, KEY_CHANNELS) <= row
    value_lane = lax.broadcasted_iota(jnp.int32, (BLOCK, 2 * DV), 1)
    value_one = value_lane < DV
    diagonal = (
        lax.rem(lax.broadcasted_iota(jnp.int32, (4 * KEY_CHANNELS, 2 * DV), 0), LANES)
        < KEY_CHANNELS
    ) == (lax.broadcasted_iota(jnp.int32, (4 * KEY_CHANNELS, 2 * DV), 1) < DV)
    zero = jnp.zeros((), bf16)
    scale = KEY_CHANNELS ** (-0.5)
    edges, updates, scaled, scored = [], [], [], []
    nothing = jnp.zeros((1, LANES), f32)
    for n in range(blocks):
        at = slice(n * BLOCK, (n + 1) * BLOCK)
        base_fwd = logs[0, n * BLOCK - 1 : n * BLOCK, :] if n else nothing
        base_bwd = logs[1, (n + 1) * BLOCK : (n + 1) * BLOCK + 1, :] if n + 1 < blocks else nothing
        cum_fwd = logs[0, at, :] - base_fwd
        cum_bwd = logs[1, at, :] - base_bwd
        edge_fwd = cum_fwd[BLOCK - 1 : BLOCK, :]
        edge_bwd = cum_bwd[0:1, :]
        queries = qkv[at, :LANES].astype(f32) * scale
        keys = qkv[at, LANES : 2 * LANES].astype(f32)
        values = qkv[at, 2 * LANES :]
        query_out[at, :LANES] = (queries * jnp.exp(logs[0, at, :])).astype(bf16)
        query_out[at, LANES:] = (queries * jnp.exp(logs[1, at, :])).astype(bf16)
        query_fwd = (queries * jnp.exp(cum_fwd)).astype(bf16)
        query_bwd = (queries * jnp.exp(cum_bwd)).astype(bf16)
        key_fwd = (keys * jnp.exp(-cum_fwd)).astype(bf16)
        key_bwd = (keys * jnp.exp(-cum_bwd)).astype(bf16)

        def by_head(key):
            return jnp.concatenate(
                [jnp.where(head_one, key, zero), jnp.where(head_one, zero, key)], axis=0
            )

        across = ((1,), (1,))
        scores = jnp.where(
            lower,
            matmul(query_fwd, by_head(key_fwd), across),
            matmul(query_bwd, by_head(key_bwd), across),
        ).astype(bf16)
        spread = jnp.concatenate(
            [jnp.where(value_one, values, zero), jnp.where(value_one, zero, values)], axis=0
        )
        scored.append(matmul(scores, spread))
        scaled.append(jnp.concatenate([query_fwd, query_bwd], axis=1))
        weighted = jnp.concatenate(
            [
                (keys * jnp.exp(edge_fwd - cum_fwd)).astype(bf16),
                (keys * jnp.exp(edge_bwd - cum_bwd)).astype(bf16),
            ],
            axis=1,
        )
        update = matmul(weighted, values, ((0,), (0,)))
        updates.append(jnp.where(diagonal, update, 0.0))
        edges.append((edge_fwd, edge_bwd))
    stacked = jnp.concatenate(
        [e[0] for e in edges]
        + [e[1] for e in edges]
        + [jnp.zeros((LANES - 2 * blocks, LANES), f32)],
        axis=0,
    )
    factors = jnp.exp(stacked.T)
    start_fwd, start_bwd = [None] * blocks, [None] * blocks
    memory = jnp.zeros((LANES, 2 * DV), f32)
    for n in range(blocks):
        start_fwd[n] = memory.astype(bf16)
        memory = factors[:, n : n + 1] * memory + updates[n][:LANES]
    memory = jnp.zeros((LANES, 2 * DV), f32)
    for n in reversed(range(blocks)):
        start_bwd[n] = memory.astype(bf16)
        memory = factors[:, blocks + n : blocks + n + 1] * memory + updates[n][LANES:]
    for n in range(blocks):
        entering = jnp.concatenate([start_fwd[n], start_bwd[n]], axis=0)
        part_out[n * BLOCK : (n + 1) * BLOCK, :] = scored[n] + matmul(scaled[n], entering)


def pool_kernel(place, pool_input, rim_before, rim_after, group_map, out):
    tp, here = (place[0], place[2])
    rows = out.shape[0]
    padded = rows + 2 * rim_width
    values = jnp.concatenate([rim_before[...], pool_input[...], rim_after[...]], axis=0).astype(f32)
    sums = values + pltpu.roll(values, 1, 0)
    chosen = sums
    for level in (1, 2, 3):
        step = 2 ** (level - 1)
        sums = pltpu.roll(sums, step, 0) + pltpu.roll(sums, padded - step, 0)
        chosen = jnp.where(tp >= level, sums, chosen)
    half = jnp.left_shift(1, tp)
    position = here * rows + lax.broadcasted_iota(jnp.int32, (rows, LANES), 0)
    last = place[3] * rows - 1
    low_end = jnp.maximum(position - half, 0)
    high_end = jnp.minimum(position + half - 1, last)
    counted = (high_end - low_end + 1).astype(f32)[:, 0:1]
    inside = slice(rim_width, rim_width + rows)
    pooled = (chosen[inside] / counted - values[inside]).astype(bf16)
    out[...] = matmul(pooled, group_map[tp]).astype(bf16)


def finish_kernel(place, part, query, entering, pooled, *outs_and_scratch):
    *outs, ready = outs_and_scratch
    channel_one = lax.broadcasted_iota(jnp.int32, (LANES, DV), 0) < KEY_CHANNELS
    zero = jnp.zeros((), bf16)
    sides = []
    for d in range(2):
        state = entering[:, d, :]
        sides.append(
            jnp.concatenate(
                [jnp.where(channel_one, state, zero), jnp.where(channel_one, zero, state)], axis=1
            )
        )
    joined = part[...] + matmul(query[...], jnp.concatenate(sides, axis=0))
    rows = joined.shape[0]
    width = pooled.shape[1]
    ready[:, :width] = pooled[...]
    for h in range(2):
        mine = joined[:, h * DV : (h + 1) * DV]
        scale = lax.rsqrt(jnp.mean(mine * mine, axis=1, keepdims=True) + eps_value)
        ready[:, width + h * DV : width + (h + 1) * DV] = (mine * scale).astype(bf16)
    owners = len(outs)
    share = rows // owners
    for step, out in enumerate(outs):
        first = pl.multiple_of(lax.rem(place[0] + step, owners) * share, share)
        out[...] = ready[pl.ds(first, share), :]


def start_loads(weights, start, weight_ref, sems):
    pieces = sems.shape[0]
    tile = weights.shape[0] // pieces
    columns = slice(start, start + weight_ref.shape[1])
    loads = []
    for n in range(pieces):
        here = slice(n * tile, (n + 1) * tile)
        load = pltpu.make_async_copy(weights.at[here, columns], weight_ref.at[here], sems.at[n])
        load.start()
        loads.append((here, load))
    return loads


def own_kernel(weights, mine, out, weight_ref, sems):
    for here, load in start_loads(weights, 0, weight_ref, sems):
        load.wait()
        out[:, here] = matmul(mine[...], weight_ref[here, :], ((1,), (1,))).astype(bf16)


def output_kernel(weights, own_part, *rest):
    *others, out, weight_ref, sems = rest
    width = others[0].shape[1]
    for here, load in start_loads(weights, width, weight_ref, sems):
        load.wait()
        total = own_part[:, here].astype(f32)
        for s, other in enumerate(others):
            block = weight_ref[here, s * width : (s + 1) * width]
            total = total + matmul(other[...], block, ((1,), (1,))).astype(bf16).astype(f32)
        out[:, here] = total.astype(bf16)


def shape_of(*lengths, kind=bf16):
    return jax.ShapeDtypeStruct(lengths, kind)


def shards(
    tokens,
    pooling_input_weight,
    query_matrix,
    key_matrix,
    value_matrix,
    decay_inner_weight,
    decay_outer_weight,
    channel_decay_bias,
    spike_log_decay,
    starting_state,
    pooling_group_map,
    pooling_output_weight,
    attention_output_weight,
):
    sp_index = lax.axis_index(SP)
    tp_index = lax.axis_index("tp")
    core = lax.axis_index("sp_2")
    positions = lax.axis_size(SP)
    place = jnp.stack([tp_index, core, sp_index, jnp.int32(positions)]).astype(jnp.int32)
    groups = lax.axis_size("tp")
    rows = tokens.shape[0] * groups
    model = tokens.shape[1]

    local_in = jnp.concatenate(
        [query_matrix, key_matrix, value_matrix, pooling_input_weight], axis=1
    )
    chips = lax.axis_size(CHIPS)
    copies = jnp.broadcast_to(local_in, (chips, *local_in.shape))
    weight_own = lax.all_to_all(copies, CHIPS, 0, 0, tiled=True)
    local_out = jnp.concatenate([pooling_output_weight, attention_output_weight], axis=0).T
    outs = [local_out] + [shifted(local_out, "tp", k) for k in range(1, groups)]
    normed = normalize(tokens)
    half = normed.shape[0] // 2
    before = shifted(normed, "tp", 1)
    after = shifted(normed, "tp", -1)
    top, end = (before[:half], after[half:])
    far_top = shifted(top, "tp", 1)
    far_end = shifted(end, "tp", -1)
    weight_other = shifted(weight_own, "sp_2", 1)
    whole_out = lax.all_gather(jnp.concatenate(outs, axis=1), SP, axis=0, tiled=True)

    qkv, pool_input, logs, packed = call(
        project_kernel,
        (
            shape_of(rows, 4 * LANES),
            shape_of(rows, 2 * LANES),
            shape_of(2, rows, LANES, kind=f32),
            shape_of(LANES, 3, LANES),
        ),
        (
            place,
            normed,
            before,
            after,
            far_top,
            far_end,
            weight_own,
            weight_other,
            decay_inner_weight,
            decay_outer_weight,
            channel_decay_bias,
            spike_log_decay.T,
        ),
        scratch=(
            pltpu.VMEM((rows, model), bf16),
            pltpu.VMEM((chips, 2, model // (2 * chips), 6 * LANES), bf16),
        ),
        flops=2 * rows * model * 7 * LANES,
        moved=10_000_000,
    )
    received = lax.all_to_all(packed, SP, 0, 0, tiled=True)
    part, query = call(
        inner_kernel,
        (shape_of(rows, 2 * DV, kind=f32), shape_of(rows, 2 * LANES)),
        (qkv, logs),
        scalars=0,
        flops=2 * rows * model * 2 * LANES,
        moved=3_000_000,
    )
    rim_before = neighbours(pool_input[rows - rim_width :], SP, 1)
    rim_after = neighbours(pool_input[:rim_width], SP, -1)
    states = call(
        scan_kernel,
        shape_of(positions, 2, LANES),
        (place[2:3], received, starting_state.reshape(2, -1, DV)),
        flops=40_000_000,
    )
    entering = lax.all_to_all(states, SP, 0, 0, tiled=True)
    pooled = call(
        pool_kernel,
        shape_of(rows, 2 * LANES),
        (place, pool_input, rim_before, rim_after, pooling_group_map),
        flops=2 * rows * 4 * LANES * LANES,
        moved=1_000_000,
    )
    share = rows // groups
    width = 4 * LANES
    mine, for_next, for_far, for_last = call(
        finish_kernel,
        (shape_of(share, width),) * groups,
        (place, part, query, entering, pooled),
        scratch=(pltpu.VMEM((rows, width), bf16),),
        flops=100_000_000,
        moved=2_000_000,
    )
    first = shifted(for_next, "tp", 1)
    third = shifted(for_last, "tp", -1)
    second = shifted(for_far, "tp", 2)
    own_part = call(
        own_kernel,
        shape_of(share, model),
        (whole_out, mine),
        scalars=0,
        far=1,
        scratch=(pltpu.VMEM((model, width), bf16), pltpu.SemaphoreType.DMA((4,))),
        flops=2 * share * model * width,
        moved=2 * model * width,
    )
    return call(
        output_kernel,
        shape_of(share, model),
        (whole_out, own_part, first, second, third),
        scalars=0,
        far=1,
        scratch=(
            pltpu.VMEM((model, (groups - 1) * width), bf16),
            pltpu.SemaphoreType.DMA((8,)),
        ),
        flops=2 * share * model * (groups - 1) * width,
        moved=2 * model * (groups - 1) * width,
    )


def solution(mesh):
    split = Mesh(mesh.devices.reshape(8, 8, 2, mesh.shape["tp"]), ("sp_0", "sp_1", "sp_2", "tp"))
    in_specs = (
        P(SP_TP, None),
        P(SP, "tp"),
        P(SP, "tp"),
        P(SP, "tp"),
        P(SP, "tp"),
        P(),
        P(),
        P(),
        P("tp", SP),
        P(None, "tp", None, None),
        P(),
        P("tp", SP),
        P("tp", SP),
    )
    out_specs = P(SP_TP, None)
    return jax.shard_map(
        shards, mesh=split, in_specs=in_specs, out_specs=out_specs, check_vma=False
    )
```

```python
import jax
import jax.numpy as jnp
from jax import lax
from jax.experimental import pallas as pl
from jax.experimental.pallas import tpu as pltpu
from jax.sharding import Mesh
from jax.sharding import PartitionSpec as P


KEY_CHANNELS = 64
DV = 128
RANK = 32
BLOCK = 64
LANES = 128
SP = ("sp_0", "sp_1", "sp_2")
CHIPS = ("sp_0", "sp_1")
SP_TP = ("sp_0", "sp_1", "sp_2", "tp")

eps_value = 1e-06
gate_norm_factor = 16.0
rim_width = 8
interpreted = False

bf16 = jnp.bfloat16
f32 = jnp.float32
exact = lax.Precision.HIGHEST


def matmul(a, b, dims=((1,), (0,)), precision=None):
    return lax.dot_general(a, b, (dims, ((), ())), precision=precision, preferred_element_type=f32)


def call(kernel, out_shapes, operands, scalars=1, far=0, scratch=(), flops=0, moved=0):
    smem = pl.BlockSpec(memory_space=pltpu.SMEM)
    vmem = pl.BlockSpec(memory_space=pltpu.VMEM)
    anywhere = pl.BlockSpec(memory_space=pl.ANY)
    near = len(operands) - scalars - far
    return pl.pallas_call(
        kernel,
        in_specs=[smem] * scalars + [anywhere] * far + [vmem] * near,
        out_specs=jax.tree.map(lambda _: vmem, out_shapes),
        out_shape=out_shapes,
        scratch_shapes=list(scratch),
        cost_estimate=pl.CostEstimate(flops=flops, bytes_accessed=moved, transcendentals=0),
        interpret=interpreted,
    )(*operands)


def shifted(value, axis, step):
    devices = lax.axis_size(axis)
    return lax.ppermute(value, axis, [(i, (i + step) % devices) for i in range(devices)])


def neighbours(value, axes, step):
    devices = lax.axis_size(axes)
    pairs = [(i, i + step) for i in range(devices) if 0 <= i + step < devices]
    return lax.ppermute(value, axes, pairs)


def normalize(token_rows):
    floats = token_rows.astype(f32)
    scaled = floats * lax.rsqrt(jnp.mean(floats * floats, axis=-1, keepdims=True) + eps_value)
    return scaled.astype(bf16)


def place_tokens(tp, pieces, whole_ref, first):
    own, before, after, far_top, far_end = pieces
    rows = own.shape[0]
    half = rows // 2

    def at(step):
        return pl.multiple_of(first + lax.rem(tp + step, 4) * rows, 8)

    whole_ref[pl.ds(at(0), rows), :] = own[...]
    whole_ref[pl.ds(at(3), rows), :] = before[...]
    whole_ref[pl.ds(at(1), rows), :] = after[...]
    far = at(2)
    whole_ref[pl.ds(far, half), :] = far_top[...]
    whole_ref[pl.ds(pl.multiple_of(far + half, 8), half), :] = far_end[...]


def split_dot(ones, values):
    high = values.astype(bf16)
    low = (values - high.astype(f32)).astype(bf16)
    return matmul(ones, high) + matmul(ones, low)


def project_kernel(
    place,
    own,
    before,
    after,
    far_top,
    far_end,
    weight_own,
    weight_other,
    inner,
    outer,
    bias,
    spike,
    qkv_out,
    pool_out,
    logs_out,
    packed_out,
    tokens_ref,
    weight_ref,
):
    tp, core = (place[0], place[1])
    place_tokens(tp, (own, before, after, far_top, far_end), tokens_ref, 0)
    weight_ref[:, pl.ds(core, 1)] = weight_own[...][:, None]
    weight_ref[:, pl.ds(1 - core, 1)] = weight_other[...][:, None]
    rows, width = tokens_ref.shape
    tokens = tokens_ref[...]
    low_rank = matmul(tokens, inner[...]).astype(bf16)
    projected = matmul(tokens, weight_ref[...].reshape(width, -1)).astype(bf16)
    qkv = projected[:, : 4 * LANES]
    qkv_out[...] = qkv
    pool_out[...] = projected[:, 4 * LANES :]
    here = pl.ds(pl.multiple_of(tp * LANES, LANES), LANES)
    blank = jnp.zeros((RANK, LANES), bf16)
    outer_both = jnp.concatenate(
        [
            jnp.concatenate([outer[0, :, here], blank], axis=1),
            jnp.concatenate([blank, outer[1, :, here]], axis=1),
        ],
        axis=0,
    )
    bias_both = jnp.concatenate([bias[0:1, here], bias[1:2, here]], axis=1)
    pre = matmul(low_rank, outer_both) + bias_both
    gate = jnp.minimum(pre, 0.0) - jnp.log1p(jnp.exp(-jnp.abs(pre)))
    lane = lax.broadcasted_iota(jnp.int32, (rows, LANES), 1)
    spikes = jnp.where(lane < KEY_CHANNELS, spike[:, 0:1], spike[:, 1:2])
    decay = gate * (1.0 / gate_norm_factor) + jnp.concatenate([spikes, spikes], axis=1)
    size = LANES
    row_ids = lax.broadcasted_iota(jnp.int32, (size, size), 0)
    col_ids = lax.broadcasted_iota(jnp.int32, (size, size), 1)
    upto = (col_ids <= row_ids).astype(bf16)
    onward = (col_ids >= row_ids).astype(bf16)
    tiles = rows // size
    carry = jnp.zeros((1, LANES), f32)
    for n in range(tiles):
        found = split_dot(upto, decay[n * size : (n + 1) * size, :LANES]) + carry
        logs_out[0, n * size : (n + 1) * size, :] = found
        carry = found[size - 1 : size, :]
    total_fwd = carry
    carry = jnp.zeros((1, LANES), f32)
    for n in reversed(range(tiles)):
        found = split_dot(onward, decay[n * size : (n + 1) * size, LANES:]) + carry
        logs_out[1, n * size : (n + 1) * size, :] = found
        carry = found[0:1, :]
    total_bwd = carry
    keys = qkv[:, LANES : 2 * LANES].astype(f32)
    weighted = jnp.concatenate(
        [
            (keys * jnp.exp(total_fwd - logs_out[0])).astype(bf16),
            (keys * jnp.exp(total_bwd - logs_out[1])).astype(bf16),
        ],
        axis=1,
    )
    updates = matmul(weighted, qkv[:, 2 * LANES :], ((0,), (0,)))
    first = lax.broadcasted_iota(jnp.int32, (LANES, LANES), 0) < KEY_CHANNELS
    for d in range(2):
        mine = updates[d * LANES : (d + 1) * LANES]
        packed_out[:, d, :] = jnp.where(first, mine[:, :LANES], mine[:, LANES:]).astype(bf16)
    totals = jnp.concatenate([total_fwd, total_bwd], axis=0)
    high = totals.astype(bf16).astype(f32)
    stacked = jnp.concatenate([high, totals - high, jnp.zeros((LANES - 4, LANES), f32)], axis=0)
    packed_out[:, 2, :] = stacked.T.astype(bf16)


def scan_kernel(place, received, start, out):
    devices = received.shape[0]
    here = place[0]
    parts = received[:, 2, :].astype(f32)
    logs = parts + pltpu.roll(parts, LANES - 2, 1)
    row = lax.broadcasted_iota(jnp.int32, (devices, devices), 0)
    col = lax.broadcasted_iota(jnp.int32, (devices, devices), 1)
    earlier = (col < row).astype(f32)
    upto = (row <= col).astype(f32)
    strictly = (row < col).astype(f32)
    before_col = matmul(earlier, logs, precision=exact)
    before_row = matmul(logs, strictly, ((0,), (0,)), precision=exact)
    past_row = matmul(logs, upto, ((0,), (0,)), precision=exact)
    past_col = before_col + logs
    total = jnp.sum(logs, axis=0, keepdims=True)
    for r in range(2):
        if r == 0:
            between = before_col[:, 0:1] - past_row[0:1, :]
            allowed = col < row
            outside = before_col[:, 0:1]
        else:
            between = before_row[1:2, :] - past_col[:, 1:2]
            allowed = col > row
            outside = total[:, 1:2] - past_col[:, 1:2]
        weights = jnp.where(allowed, jnp.exp(jnp.minimum(between, 0.0)), 0.0)
        high = weights.astype(bf16)
        low = (weights - high.astype(f32)).astype(bf16)
        updates = received[:, r, :]
        first = start[r, pl.ds(here, 1), :]
        entering = matmul(high, updates) + matmul(low, updates)
        entering = entering + jnp.exp(jnp.minimum(outside, 0.0)) * first
        out[:, r, :] = entering.astype(bf16)


def inner_kernel(qkv, logs, part_out, query_out):
    rows = qkv.shape[0]
    blocks = rows // BLOCK
    lane = lax.broadcasted_iota(jnp.int32, (BLOCK, LANES), 1)
    row = lax.broadcasted_iota(jnp.int32, (BLOCK, LANES), 0)
    head_one = lane < KEY_CHANNELS
    lower = lax.rem(lane, KEY_CHANNELS) <= row
    value_lane = lax.broadcasted_iota(jnp.int32, (BLOCK, 2 * DV), 1)
    value_one = value_lane < DV
    diagonal = (
        lax.rem(lax.broadcasted_iota(jnp.int32, (4 * KEY_CHANNELS, 2 * DV), 0), LANES)
        < KEY_CHANNELS
    ) == (lax.broadcasted_iota(jnp.int32, (4 * KEY_CHANNELS, 2 * DV), 1) < DV)
    zero = jnp.zeros((), bf16)
    scale = KEY_CHANNELS ** (-0.5)
    edges, updates, scaled, scored = [], [], [], []
    nothing = jnp.zeros((1, LANES), f32)
    for n in range(blocks):
        at = slice(n * BLOCK, (n + 1) * BLOCK)
        base_fwd = logs[0, n * BLOCK - 1 : n * BLOCK, :] if n else nothing
        base_bwd = logs[1, (n + 1) * BLOCK : (n + 1) * BLOCK + 1, :] if n + 1 < blocks else nothing
        cum_fwd = logs[0, at, :] - base_fwd
        cum_bwd = logs[1, at, :] - base_bwd
        edge_fwd = cum_fwd[BLOCK - 1 : BLOCK, :]
        edge_bwd = cum_bwd[0:1, :]
        queries = qkv[at, :LANES].astype(f32) * scale
        keys = qkv[at, LANES : 2 * LANES].astype(f32)
        values = qkv[at, 2 * LANES :]
        query_out[at, :LANES] = (queries * jnp.exp(logs[0, at, :])).astype(bf16)
        query_out[at, LANES:] = (queries * jnp.exp(logs[1, at, :])).astype(bf16)
        query_fwd = (queries * jnp.exp(cum_fwd)).astype(bf16)
        query_bwd = (queries * jnp.exp(cum_bwd)).astype(bf16)
        key_fwd = (keys * jnp.exp(-cum_fwd)).astype(bf16)
        key_bwd = (keys * jnp.exp(-cum_bwd)).astype(bf16)

        def by_head(key):
            return jnp.concatenate(
                [jnp.where(head_one, key, zero), jnp.where(head_one, zero, key)], axis=0
            )

        across = ((1,), (1,))
        scores = jnp.where(
            lower,
            matmul(query_fwd, by_head(key_fwd), across),
            matmul(query_bwd, by_head(key_bwd), across),
        ).astype(bf16)
        spread = jnp.concatenate(
            [jnp.where(value_one, values, zero), jnp.where(value_one, zero, values)], axis=0
        )
        scored.append(matmul(scores, spread))
        scaled.append(jnp.concatenate([query_fwd, query_bwd], axis=1))
        weighted = jnp.concatenate(
            [
                (keys * jnp.exp(edge_fwd - cum_fwd)).astype(bf16),
                (keys * jnp.exp(edge_bwd - cum_bwd)).astype(bf16),
            ],
            axis=1,
        )
        update = matmul(weighted, values, ((0,), (0,)))
        updates.append(jnp.where(diagonal, update, 0.0))
        edges.append((edge_fwd, edge_bwd))
    stacked = jnp.concatenate(
        [e[0] for e in edges]
        + [e[1] for e in edges]
        + [jnp.zeros((LANES - 2 * blocks, LANES), f32)],
        axis=0,
    )
    factors = jnp.exp(stacked.T)
    start_fwd, start_bwd = [None] * blocks, [None] * blocks
    memory = jnp.zeros((LANES, 2 * DV), f32)
    for n in range(blocks):
        start_fwd[n] = memory.astype(bf16)
        memory = factors[:, n : n + 1] * memory + updates[n][:LANES]
    memory = jnp.zeros((LANES, 2 * DV), f32)
    for n in reversed(range(blocks)):
        start_bwd[n] = memory.astype(bf16)
        memory = factors[:, blocks + n : blocks + n + 1] * memory + updates[n][LANES:]
    for n in range(blocks):
        entering = jnp.concatenate([start_fwd[n], start_bwd[n]], axis=0)
        part_out[n * BLOCK : (n + 1) * BLOCK, :] = scored[n] + matmul(scaled[n], entering)


def pool_kernel(place, pool_input, rim_before, rim_after, group_map, out):
    tp, here = (place[0], place[2])
    rows = out.shape[0]
    padded = rows + 2 * rim_width
    values = jnp.concatenate([rim_before[...], pool_input[...], rim_after[...]], axis=0).astype(f32)
    sums = values + pltpu.roll(values, 1, 0)
    chosen = sums
    for level in (1, 2, 3):
        step = 2 ** (level - 1)
        sums = pltpu.roll(sums, step, 0) + pltpu.roll(sums, padded - step, 0)
        chosen = jnp.where(tp >= level, sums, chosen)
    half = jnp.left_shift(1, tp)
    position = here * rows + lax.broadcasted_iota(jnp.int32, (rows, LANES), 0)
    last = place[3] * rows - 1
    low_end = jnp.maximum(position - half, 0)
    high_end = jnp.minimum(position + half - 1, last)
    counted = (high_end - low_end + 1).astype(f32)[:, 0:1]
    inside = slice(rim_width, rim_width + rows)
    pooled = (chosen[inside] / counted - values[inside]).astype(bf16)
    out[...] = matmul(pooled, group_map[tp]).astype(bf16)


def finish_kernel(place, part, query, entering, pooled, *outs_and_scratch):
    *outs, ready = outs_and_scratch
    channel_one = lax.broadcasted_iota(jnp.int32, (LANES, DV), 0) < KEY_CHANNELS
    zero = jnp.zeros((), bf16)
    sides = []
    for d in range(2):
        state = entering[:, d, :]
        sides.append(
            jnp.concatenate(
                [jnp.where(channel_one, state, zero), jnp.where(channel_one, zero, state)], axis=1
            )
        )
    joined = part[...] + matmul(query[...], jnp.concatenate(sides, axis=0))
    rows = joined.shape[0]
    width = pooled.shape[1]
    ready[:, :width] = pooled[...]
    for h in range(2):
        mine = joined[:, h * DV : (h + 1) * DV]
        scale = lax.rsqrt(jnp.mean(mine * mine, axis=1, keepdims=True) + eps_value)
        ready[:, width + h * DV : width + (h + 1) * DV] = (mine * scale).astype(bf16)
    owners = len(outs)
    share = rows // owners
    for step, out in enumerate(outs):
        first = pl.multiple_of(lax.rem(place[0] + step, owners) * share, share)
        out[...] = ready[pl.ds(first, share), :]


def start_loads(weights, start, weight_ref, sems):
    pieces = sems.shape[0]
    tile = weights.shape[0] // pieces
    columns = slice(start, start + weight_ref.shape[1])
    loads = []
    for n in range(pieces):
        here = slice(n * tile, (n + 1) * tile)
        load = pltpu.make_async_copy(weights.at[here, columns], weight_ref.at[here], sems.at[n])
        load.start()
        loads.append((here, load))
    return loads


def own_kernel(weights, mine, out, weight_ref, sems):
    for here, load in start_loads(weights, 0, weight_ref, sems):
        load.wait()
        out[:, here] = matmul(mine[...], weight_ref[here, :], ((1,), (1,))).astype(bf16)


def output_kernel(weights, own_part, *rest):
    *others, out, weight_ref, sems = rest
    width = others[0].shape[1]
    for here, load in start_loads(weights, width, weight_ref, sems):
        load.wait()
        total = own_part[:, here].astype(f32)
        for s, other in enumerate(others):
            block = weight_ref[here, s * width : (s + 1) * width]
            total = total + matmul(other[...], block, ((1,), (1,))).astype(bf16).astype(f32)
        out[:, here] = total.astype(bf16)


def shape_of(*lengths, kind=bf16):
    return jax.ShapeDtypeStruct(lengths, kind)


def shards(
    tokens,
    pooling_input_weight,
    query_matrix,
    key_matrix,
    value_matrix,
    decay_inner_weight,
    decay_outer_weight,
    channel_decay_bias,
    spike_log_decay,
    starting_state,
    pooling_group_map,
    pooling_output_weight,
    attention_output_weight,
):
    sp_index = lax.axis_index(SP)
    tp_index = lax.axis_index("tp")
    core = lax.axis_index("sp_2")
    positions = lax.axis_size(SP)
    place = jnp.stack([tp_index, core, sp_index, jnp.int32(positions)]).astype(jnp.int32)
    groups = lax.axis_size("tp")
    rows = tokens.shape[0] * groups
    model = tokens.shape[1]

    local_in = jnp.concatenate(
        [query_matrix, key_matrix, value_matrix, pooling_input_weight], axis=1
    )
    chips = lax.axis_size(CHIPS)
    copies = jnp.broadcast_to(local_in, (chips, *local_in.shape))
    weight_own = lax.all_to_all(copies, CHIPS, 0, 0, tiled=True)
    local_out = jnp.concatenate([pooling_output_weight, attention_output_weight], axis=0).T
    outs = [local_out] + [shifted(local_out, "tp", k) for k in range(1, groups)]
    normed = normalize(tokens)
    half = normed.shape[0] // 2
    before = shifted(normed, "tp", 1)
    after = shifted(normed, "tp", -1)
    top, end = (before[:half], after[half:])
    far_top = shifted(top, "tp", 1)
    far_end = shifted(end, "tp", -1)
    weight_other = shifted(weight_own, "sp_2", 1)
    whole_out = lax.all_gather(jnp.concatenate(outs, axis=1), SP, axis=0, tiled=True)

    qkv, pool_input, logs, packed = call(
        project_kernel,
        (
            shape_of(rows, 4 * LANES),
            shape_of(rows, 2 * LANES),
            shape_of(2, rows, LANES, kind=f32),
            shape_of(LANES, 3, LANES),
        ),
        (
            place,
            normed,
            before,
            after,
            far_top,
            far_end,
            weight_own,
            weight_other,
            decay_inner_weight,
            decay_outer_weight,
            channel_decay_bias,
            spike_log_decay.T,
        ),
        scratch=(
            pltpu.VMEM((rows, model), bf16),
            pltpu.VMEM((chips, 2, model // (2 * chips), 6 * LANES), bf16),
        ),
        flops=2 * rows * model * 7 * LANES,
        moved=10_000_000,
    )
    received = lax.all_to_all(packed, SP, 0, 0, tiled=True)
    part, query = call(
        inner_kernel,
        (shape_of(rows, 2 * DV, kind=f32), shape_of(rows, 2 * LANES)),
        (qkv, logs),
        scalars=0,
        flops=2 * rows * model * 2 * LANES,
        moved=3_000_000,
    )
    last, leading = (pool_input[rows - rim_width :], pool_input[:rim_width])
    rim_before = neighbours(last, SP, 1)
    rim_after = neighbours(leading, SP, -1)
    states = call(
        scan_kernel,
        shape_of(positions, 2, LANES),
        (place[2:3], received, starting_state.reshape(2, -1, DV)),
        flops=40_000_000,
    )
    entering = lax.all_to_all(states, SP, 0, 0, tiled=True)
    pooled = call(
        pool_kernel,
        shape_of(rows, 2 * LANES),
        (place, pool_input, rim_before, rim_after, pooling_group_map),
        flops=2 * rows * 4 * LANES * LANES,
        moved=1_000_000,
    )
    share = rows // groups
    width = 4 * LANES
    mine, for_next, for_far, for_last = call(
        finish_kernel,
        (shape_of(share, width),) * groups,
        (place, part, query, entering, pooled),
        scratch=(pltpu.VMEM((rows, width), bf16),),
        flops=100_000_000,
        moved=2_000_000,
    )
    first = shifted(for_next, "tp", 1)
    third = shifted(for_last, "tp", -1)
    second = shifted(for_far, "tp", 2)
    own_part = call(
        own_kernel,
        shape_of(share, model),
        (whole_out, mine),
        scalars=0,
        far=1,
        scratch=(pltpu.VMEM((model, width), bf16), pltpu.SemaphoreType.DMA((4,))),
        flops=2 * share * model * width,
        moved=2 * model * width,
    )
    return call(
        output_kernel,
        shape_of(share, model),
        (whole_out, own_part, first, second, third),
        scalars=0,
        far=1,
        scratch=(
            pltpu.VMEM((model, (groups - 1) * width), bf16),
            pltpu.SemaphoreType.DMA((8,)),
        ),
        flops=2 * share * model * (groups - 1) * width,
        moved=2 * model * (groups - 1) * width,
    )


def solution(mesh):
    split = Mesh(mesh.devices.reshape(8, 8, 2, mesh.shape["tp"]), ("sp_0", "sp_1", "sp_2", "tp"))
    in_specs = (
        P(SP_TP, None),
        P(SP, "tp"),
        P(SP, "tp"),
        P(SP, "tp"),
        P(SP, "tp"),
        P(),
        P(),
        P(),
        P("tp", SP),
        P(None, "tp", None, None),
        P(),
        P("tp", SP),
        P("tp", SP),
    )
    out_specs = P(SP_TP, None)
    return jax.shard_map(
        shards, mesh=split, in_specs=in_specs, out_specs=out_specs, check_vma=False
    )
```

```python
import jax
import jax.numpy as jnp
from jax import lax
from jax.experimental import pallas as pl
from jax.experimental.pallas import tpu as pltpu
from jax.sharding import Mesh
from jax.sharding import PartitionSpec as P


KEY_CHANNELS = 64
DV = 128
RANK = 32
BLOCK = 64
LANES = 128
SP = ("sp_0", "sp_1", "sp_2")
CHIPS = ("sp_0", "sp_1")
SP_TP = ("sp_0", "sp_1", "sp_2", "tp")

eps_value = 1e-06
gate_norm_factor = 16.0
rim_width = 8
interpreted = False

bf16 = jnp.bfloat16
f32 = jnp.float32
exact = lax.Precision.HIGHEST


def matmul(a, b, dims=((1,), (0,)), precision=None):
    return lax.dot_general(a, b, (dims, ((), ())), precision=precision, preferred_element_type=f32)


def call(kernel, out_shapes, operands, scalars=1, far=0, scratch=(), flops=0, moved=0):
    smem = pl.BlockSpec(memory_space=pltpu.SMEM)
    vmem = pl.BlockSpec(memory_space=pltpu.VMEM)
    anywhere = pl.BlockSpec(memory_space=pl.ANY)
    near = len(operands) - scalars - far
    return pl.pallas_call(
        kernel,
        in_specs=[smem] * scalars + [anywhere] * far + [vmem] * near,
        out_specs=jax.tree.map(lambda _: vmem, out_shapes),
        out_shape=out_shapes,
        scratch_shapes=list(scratch),
        cost_estimate=pl.CostEstimate(flops=flops, bytes_accessed=moved, transcendentals=0),
        interpret=interpreted,
    )(*operands)


def shifted(value, axis, step):
    devices = lax.axis_size(axis)
    return lax.ppermute(value, axis, [(i, (i + step) % devices) for i in range(devices)])


def neighbours(value, axes, step):
    devices = lax.axis_size(axes)
    pairs = [(i, i + step) for i in range(devices) if 0 <= i + step < devices]
    return lax.ppermute(value, axes, pairs)


def normalize(token_rows):
    floats = token_rows.astype(f32)
    scaled = floats * lax.rsqrt(jnp.mean(floats * floats, axis=-1, keepdims=True) + eps_value)
    return scaled.astype(bf16)


def place_tokens(tp, pieces, whole_ref, first):
    own, before, after, far_top, far_end = pieces
    rows = own.shape[0]
    half = rows // 2

    def at(step):
        return pl.multiple_of(first + lax.rem(tp + step, 4) * rows, 8)

    whole_ref[pl.ds(at(0), rows), :] = own[...]
    whole_ref[pl.ds(at(3), rows), :] = before[...]
    whole_ref[pl.ds(at(1), rows), :] = after[...]
    far = at(2)
    whole_ref[pl.ds(far, half), :] = far_top[...]
    whole_ref[pl.ds(pl.multiple_of(far + half, 8), half), :] = far_end[...]


def split_dot(ones, values):
    high = values.astype(bf16)
    low = (values - high.astype(f32)).astype(bf16)
    return matmul(ones, high) + matmul(ones, low)


def project_kernel(
    place,
    own,
    before,
    after,
    far_top,
    far_end,
    weight_own,
    weight_other,
    inner,
    outer,
    bias,
    spike,
    qkv_out,
    pool_out,
    logs_out,
    packed_out,
    tokens_ref,
    weight_ref,
):
    tp, core = (place[0], place[1])
    place_tokens(tp, (own, before, after, far_top, far_end), tokens_ref, 0)
    weight_ref[:, pl.ds(core, 1)] = weight_own[...][:, None]
    weight_ref[:, pl.ds(1 - core, 1)] = weight_other[...][:, None]
    rows, width = tokens_ref.shape
    tokens = tokens_ref[...]
    low_rank = matmul(tokens, inner[...], ((1,), (1,))).astype(bf16)
    projected = matmul(tokens, weight_ref[...].reshape(width, -1)).astype(bf16)
    qkv = projected[:, : 4 * LANES]
    qkv_out[...] = qkv
    pool_out[...] = projected[:, 4 * LANES :]
    here = pl.ds(pl.multiple_of(tp * LANES, LANES), LANES)
    blank = jnp.zeros((RANK, LANES), bf16)
    outer_both = jnp.concatenate(
        [
            jnp.concatenate([outer[0, :, here], blank], axis=1),
            jnp.concatenate([blank, outer[1, :, here]], axis=1),
        ],
        axis=0,
    )
    bias_both = jnp.concatenate([bias[0:1, here], bias[1:2, here]], axis=1)
    pre = matmul(low_rank, outer_both) + bias_both
    gate = jnp.minimum(pre, 0.0) - jnp.log1p(jnp.exp(-jnp.abs(pre)))
    lane = lax.broadcasted_iota(jnp.int32, (rows, LANES), 1)
    spike_rows = jnp.concatenate([spike[...], jnp.zeros((6, rows), f32)], axis=0).T
    spikes = jnp.where(lane < KEY_CHANNELS, spike_rows[:, 0:1], spike_rows[:, 1:2])
    decay = gate * (1.0 / gate_norm_factor) + jnp.concatenate([spikes, spikes], axis=1)
    size = LANES
    row_ids = lax.broadcasted_iota(jnp.int32, (size, size), 0)
    col_ids = lax.broadcasted_iota(jnp.int32, (size, size), 1)
    upto = (col_ids <= row_ids).astype(bf16)
    onward = (col_ids >= row_ids).astype(bf16)
    tiles = rows // size
    carry = jnp.zeros((1, LANES), f32)
    for n in range(tiles):
        found = split_dot(upto, decay[n * size : (n + 1) * size, :LANES]) + carry
        logs_out[0, n * size : (n + 1) * size, :] = found
        carry = found[size - 1 : size, :]
    total_fwd = carry
    carry = jnp.zeros((1, LANES), f32)
    for n in reversed(range(tiles)):
        found = split_dot(onward, decay[n * size : (n + 1) * size, LANES:]) + carry
        logs_out[1, n * size : (n + 1) * size, :] = found
        carry = found[0:1, :]
    total_bwd = carry
    keys = qkv[:, LANES : 2 * LANES].astype(f32)
    weighted = jnp.concatenate(
        [
            (keys * jnp.exp(total_fwd - logs_out[0])).astype(bf16),
            (keys * jnp.exp(total_bwd - logs_out[1])).astype(bf16),
        ],
        axis=1,
    )
    updates = matmul(weighted, qkv[:, 2 * LANES :], ((0,), (0,)))
    first = lax.broadcasted_iota(jnp.int32, (LANES, LANES), 0) < KEY_CHANNELS
    for d in range(2):
        mine = updates[d * LANES : (d + 1) * LANES]
        packed_out[:, d, :] = jnp.where(first, mine[:, :LANES], mine[:, LANES:]).astype(bf16)
    totals = jnp.concatenate([total_fwd, total_bwd], axis=0)
    high = totals.astype(bf16).astype(f32)
    stacked = jnp.concatenate([high, totals - high, jnp.zeros((LANES - 4, LANES), f32)], axis=0)
    packed_out[:, 2, :] = stacked.T.astype(bf16)


def scan_kernel(place, received, start, out):
    devices = received.shape[0]
    here = place[0]
    parts = received[:, 2, :].astype(f32)
    logs = parts + pltpu.roll(parts, LANES - 2, 1)
    row = lax.broadcasted_iota(jnp.int32, (devices, devices), 0)
    col = lax.broadcasted_iota(jnp.int32, (devices, devices), 1)
    earlier = (col < row).astype(f32)
    upto = (row <= col).astype(f32)
    strictly = (row < col).astype(f32)
    before_col = matmul(earlier, logs, precision=exact)
    before_row = matmul(logs, strictly, ((0,), (0,)), precision=exact)
    past_row = matmul(logs, upto, ((0,), (0,)), precision=exact)
    past_col = before_col + logs
    total = jnp.sum(logs, axis=0, keepdims=True)
    for r in range(2):
        if r == 0:
            between = before_col[:, 0:1] - past_row[0:1, :]
            allowed = col < row
            outside = before_col[:, 0:1]
        else:
            between = before_row[1:2, :] - past_col[:, 1:2]
            allowed = col > row
            outside = total[:, 1:2] - past_col[:, 1:2]
        weights = jnp.where(allowed, jnp.exp(jnp.minimum(between, 0.0)), 0.0)
        high = weights.astype(bf16)
        low = (weights - high.astype(f32)).astype(bf16)
        updates = received[:, r, :]
        first = start[r, pl.ds(here, 1), :]
        entering = matmul(high, updates) + matmul(low, updates)
        entering = entering + jnp.exp(jnp.minimum(outside, 0.0)) * first
        out[:, r, :] = entering.astype(bf16)


def inner_kernel(qkv, logs, part_out, query_out):
    rows = qkv.shape[0]
    blocks = rows // BLOCK
    lane = lax.broadcasted_iota(jnp.int32, (BLOCK, LANES), 1)
    row = lax.broadcasted_iota(jnp.int32, (BLOCK, LANES), 0)
    head_one = lane < KEY_CHANNELS
    lower = lax.rem(lane, KEY_CHANNELS) <= row
    value_lane = lax.broadcasted_iota(jnp.int32, (BLOCK, 2 * DV), 1)
    value_one = value_lane < DV
    diagonal = (
        lax.rem(lax.broadcasted_iota(jnp.int32, (4 * KEY_CHANNELS, 2 * DV), 0), LANES)
        < KEY_CHANNELS
    ) == (lax.broadcasted_iota(jnp.int32, (4 * KEY_CHANNELS, 2 * DV), 1) < DV)
    zero = jnp.zeros((), bf16)
    scale = KEY_CHANNELS ** (-0.5)
    edges, updates, scaled, scored = [], [], [], []
    nothing = jnp.zeros((1, LANES), f32)
    for n in range(blocks):
        at = slice(n * BLOCK, (n + 1) * BLOCK)
        base_fwd = logs[0, n * BLOCK - 1 : n * BLOCK, :] if n else nothing
        base_bwd = logs[1, (n + 1) * BLOCK : (n + 1) * BLOCK + 1, :] if n + 1 < blocks else nothing
        cum_fwd = logs[0, at, :] - base_fwd
        cum_bwd = logs[1, at, :] - base_bwd
        edge_fwd = cum_fwd[BLOCK - 1 : BLOCK, :]
        edge_bwd = cum_bwd[0:1, :]
        queries = qkv[at, :LANES].astype(f32) * scale
        keys = qkv[at, LANES : 2 * LANES].astype(f32)
        values = qkv[at, 2 * LANES :]
        query_out[at, :LANES] = (queries * jnp.exp(logs[0, at, :])).astype(bf16)
        query_out[at, LANES:] = (queries * jnp.exp(logs[1, at, :])).astype(bf16)
        query_fwd = (queries * jnp.exp(cum_fwd)).astype(bf16)
        query_bwd = (queries * jnp.exp(cum_bwd)).astype(bf16)
        key_fwd = (keys * jnp.exp(-cum_fwd)).astype(bf16)
        key_bwd = (keys * jnp.exp(-cum_bwd)).astype(bf16)

        def by_head(key):
            return jnp.concatenate(
                [jnp.where(head_one, key, zero), jnp.where(head_one, zero, key)], axis=0
            )

        across = ((1,), (1,))
        scores = jnp.where(
            lower,
            matmul(query_fwd, by_head(key_fwd), across),
            matmul(query_bwd, by_head(key_bwd), across),
        ).astype(bf16)
        spread = jnp.concatenate(
            [jnp.where(value_one, values, zero), jnp.where(value_one, zero, values)], axis=0
        )
        scored.append(matmul(scores, spread))
        scaled.append(jnp.concatenate([query_fwd, query_bwd], axis=1))
        weighted = jnp.concatenate(
            [
                (keys * jnp.exp(edge_fwd - cum_fwd)).astype(bf16),
                (keys * jnp.exp(edge_bwd - cum_bwd)).astype(bf16),
            ],
            axis=1,
        )
        update = matmul(weighted, values, ((0,), (0,)))
        updates.append(jnp.where(diagonal, update, 0.0))
        edges.append((edge_fwd, edge_bwd))
    stacked = jnp.concatenate(
        [e[0] for e in edges]
        + [e[1] for e in edges]
        + [jnp.zeros((LANES - 2 * blocks, LANES), f32)],
        axis=0,
    )
    factors = jnp.exp(stacked.T)
    start_fwd, start_bwd = [None] * blocks, [None] * blocks
    memory = jnp.zeros((LANES, 2 * DV), f32)
    for n in range(blocks):
        start_fwd[n] = memory.astype(bf16)
        memory = factors[:, n : n + 1] * memory + updates[n][:LANES]
    memory = jnp.zeros((LANES, 2 * DV), f32)
    for n in reversed(range(blocks)):
        start_bwd[n] = memory.astype(bf16)
        memory = factors[:, blocks + n : blocks + n + 1] * memory + updates[n][LANES:]
    for n in range(blocks):
        entering = jnp.concatenate([start_fwd[n], start_bwd[n]], axis=0)
        part_out[n * BLOCK : (n + 1) * BLOCK, :] = scored[n] + matmul(scaled[n], entering)


def pool_kernel(place, pool_input, rim_before, rim_after, group_map, out):
    tp, here = (place[0], place[2])
    rows = out.shape[0]
    padded = rows + 2 * rim_width
    values = jnp.concatenate([rim_before[...], pool_input[...], rim_after[...]], axis=0).astype(f32)
    sums = values + pltpu.roll(values, 1, 0)
    chosen = sums
    for level in (1, 2, 3):
        step = 2 ** (level - 1)
        sums = pltpu.roll(sums, step, 0) + pltpu.roll(sums, padded - step, 0)
        chosen = jnp.where(tp >= level, sums, chosen)
    half = jnp.left_shift(1, tp)
    position = here * rows + lax.broadcasted_iota(jnp.int32, (rows, LANES), 0)
    last = place[3] * rows - 1
    low_end = jnp.maximum(position - half, 0)
    high_end = jnp.minimum(position + half - 1, last)
    counted = (high_end - low_end + 1).astype(f32)[:, 0:1]
    inside = slice(rim_width, rim_width + rows)
    pooled = (chosen[inside] / counted - values[inside]).astype(bf16)
    out[...] = matmul(pooled, group_map[tp]).astype(bf16)


def finish_kernel(place, part, query, entering, pooled, *outs_and_scratch):
    *outs, ready = outs_and_scratch
    channel_one = lax.broadcasted_iota(jnp.int32, (LANES, DV), 0) < KEY_CHANNELS
    zero = jnp.zeros((), bf16)
    sides = []
    for d in range(2):
        state = entering[:, d, :]
        sides.append(
            jnp.concatenate(
                [jnp.where(channel_one, state, zero), jnp.where(channel_one, zero, state)], axis=1
            )
        )
    joined = part[...] + matmul(query[...], jnp.concatenate(sides, axis=0))
    rows = joined.shape[0]
    width = pooled.shape[1]
    ready[:, :width] = pooled[...]
    for h in range(2):
        mine = joined[:, h * DV : (h + 1) * DV]
        scale = lax.rsqrt(jnp.mean(mine * mine, axis=1, keepdims=True) + eps_value)
        ready[:, width + h * DV : width + (h + 1) * DV] = (mine * scale).astype(bf16)
    owners = len(outs)
    share = rows // owners
    for step, out in enumerate(outs):
        first = pl.multiple_of(lax.rem(place[0] + step, owners) * share, share)
        out[...] = ready[pl.ds(first, share), :]


def start_loads(weights, start, weight_ref, sems):
    pieces = sems.shape[0]
    tile = weights.shape[0] // pieces
    columns = slice(start, start + weight_ref.shape[1])
    loads = []
    for n in range(pieces):
        here = slice(n * tile, (n + 1) * tile)
        load = pltpu.make_async_copy(weights.at[here, columns], weight_ref.at[here], sems.at[n])
        load.start()
        loads.append((here, load))
    return loads


def own_kernel(weights, mine, out, weight_ref, sems):
    for here, load in start_loads(weights, 0, weight_ref, sems):
        load.wait()
        out[:, here] = matmul(mine[...], weight_ref[here, :], ((1,), (1,))).astype(bf16)


def output_kernel(weights, own_part, *rest):
    *others, out, weight_ref, sems = rest
    width = others[0].shape[1]
    for here, load in start_loads(weights, width, weight_ref, sems):
        load.wait()
        total = own_part[:, here].astype(f32)
        for s, other in enumerate(others):
            block = weight_ref[here, s * width : (s + 1) * width]
            total = total + matmul(other[...], block, ((1,), (1,))).astype(bf16).astype(f32)
        out[:, here] = total.astype(bf16)


def shape_of(*lengths, kind=bf16):
    return jax.ShapeDtypeStruct(lengths, kind)


def shards(
    tokens,
    pooling_input_weight,
    query_matrix,
    key_matrix,
    value_matrix,
    decay_inner_weight,
    decay_outer_weight,
    channel_decay_bias,
    spike_log_decay,
    starting_state,
    pooling_group_map,
    pooling_output_weight,
    attention_output_weight,
):
    sp_index = lax.axis_index(SP)
    tp_index = lax.axis_index("tp")
    core = lax.axis_index("sp_2")
    positions = lax.axis_size(SP)
    place = jnp.stack([tp_index, core, sp_index, jnp.int32(positions)]).astype(jnp.int32)
    groups = lax.axis_size("tp")
    rows = tokens.shape[0] * groups
    model = tokens.shape[1]

    local_in = jnp.concatenate(
        [query_matrix, key_matrix, value_matrix, pooling_input_weight], axis=1
    )
    chips = lax.axis_size(CHIPS)
    copies = jnp.broadcast_to(local_in, (chips, *local_in.shape))
    weight_own = lax.all_to_all(copies, CHIPS, 0, 0, tiled=True)
    local_out = jnp.concatenate([pooling_output_weight, attention_output_weight], axis=0).T
    outs = [local_out] + [shifted(local_out, "tp", k) for k in range(1, groups)]
    normed = normalize(tokens)
    half = normed.shape[0] // 2
    before = shifted(normed, "tp", 1)
    after = shifted(normed, "tp", -1)
    top, end = (before[:half], after[half:])
    far_top = shifted(top, "tp", 1)
    far_end = shifted(end, "tp", -1)
    weight_other = shifted(weight_own, "sp_2", 1)
    whole_out = lax.all_gather(jnp.concatenate(outs, axis=1), SP, axis=0, tiled=True)

    qkv, pool_input, logs, packed = call(
        project_kernel,
        (
            shape_of(rows, 4 * LANES),
            shape_of(rows, 2 * LANES),
            shape_of(2, rows, LANES, kind=f32),
            shape_of(LANES, 3, LANES),
        ),
        (
            place,
            normed,
            before,
            after,
            far_top,
            far_end,
            weight_own,
            weight_other,
            decay_inner_weight.T,
            decay_outer_weight,
            channel_decay_bias,
            spike_log_decay,
        ),
        scratch=(
            pltpu.VMEM((rows, model), bf16),
            pltpu.VMEM((chips, 2, model // (2 * chips), 6 * LANES), bf16),
        ),
        flops=2 * rows * model * 7 * LANES,
        moved=10_000_000,
    )
    received = lax.all_to_all(packed, SP, 0, 0, tiled=True)
    part, query = call(
        inner_kernel,
        (shape_of(rows, 2 * DV, kind=f32), shape_of(rows, 2 * LANES)),
        (qkv, logs),
        scalars=0,
        flops=2 * rows * model * 2 * LANES,
        moved=3_000_000,
    )
    rim_before = neighbours(pool_input[rows - rim_width :], SP, 1)
    rim_after = neighbours(pool_input[:rim_width], SP, -1)
    states = call(
        scan_kernel,
        shape_of(positions, 2, LANES),
        (place[2:3], received, starting_state.reshape(2, -1, DV)),
        flops=40_000_000,
    )
    entering = lax.all_to_all(states, SP, 0, 0, tiled=True)
    pooled = call(
        pool_kernel,
        shape_of(rows, 2 * LANES),
        (place, pool_input, rim_before, rim_after, pooling_group_map),
        flops=2 * rows * 4 * LANES * LANES,
        moved=1_000_000,
    )
    share = rows // groups
    width = 4 * LANES
    mine, for_next, for_far, for_last = call(
        finish_kernel,
        (shape_of(share, width),) * groups,
        (place, part, query, entering, pooled),
        scratch=(pltpu.VMEM((rows, width), bf16),),
        flops=100_000_000,
        moved=2_000_000,
    )
    first = shifted(for_next, "tp", 1)
    third = shifted(for_last, "tp", -1)
    second = shifted(for_far, "tp", 2)
    own_part = call(
        own_kernel,
        shape_of(share, model),
        (whole_out, mine),
        scalars=0,
        far=1,
        scratch=(pltpu.VMEM((model, width), bf16), pltpu.SemaphoreType.DMA((4,))),
        flops=2 * share * model * width,
        moved=2 * model * width,
    )
    return call(
        output_kernel,
        shape_of(share, model),
        (whole_out, own_part, first, second, third),
        scalars=0,
        far=1,
        scratch=(
            pltpu.VMEM((model, (groups - 1) * width), bf16),
            pltpu.SemaphoreType.DMA((8,)),
        ),
        flops=2 * share * model * (groups - 1) * width,
        moved=2 * model * (groups - 1) * width,
    )


def solution(mesh):
    split = Mesh(mesh.devices.reshape(8, 8, 2, mesh.shape["tp"]), ("sp_0", "sp_1", "sp_2", "tp"))
    in_specs = (
        P(SP_TP, None),
        P(SP, "tp"),
        P(SP, "tp"),
        P(SP, "tp"),
        P(SP, "tp"),
        P(),
        P(),
        P(),
        P("tp", SP),
        P(None, "tp", None, None),
        P(),
        P("tp", SP),
        P("tp", SP),
    )
    out_specs = P(SP_TP, None)
    return jax.shard_map(
        shards, mesh=split, in_specs=in_specs, out_specs=out_specs, check_vma=False
    )
```
